32 devices in a mesh: kv: 8 (over z, y), tp: 4 (over x, core).
Axes of the slice: x: 2, y: 2, z: 4, core: 2. Of those that a mesh axis runs over, the one named last changes fastest.
Arguments:
- tokens: bfloat16 [16, 16, 4096], replicated, may hold values from -6 to 6
- gain_pre: float32 [4096], replicated, may hold values from 0.1 to 1.9
- w_query: bfloat16 [4096, 2048], P('kv', 'tp'), may hold values from -0.09375 to 0.09375
- w_key: bfloat16 [4096, 2048], P('kv', 'tp'), may hold values from -0.09375 to 0.09375
- w_value: bfloat16 [4096, 2048], P('kv', 'tp'), may hold values from -0.09375 to 0.09375
- w_forget: bfloat16 [4096, 16], replicated, may hold values from -0.09375 to 0.09375
- b_forget: float32 [16], replicated
- w_out: bfloat16 [2048, 4096], P('tp', 'kv'), may hold values from -0.125 to 0.125
- gain_post: float32 [4096], P(('kv', 'tp')), may hold values from 0.1 to 1.9
- key_cache: bfloat16 [16, 1024, 16, 128], P(None, 'kv', 'tp'), may hold values from -6 to 6
- value_cache: bfloat16 [16, 1024, 16, 128], P(None, 'kv', 'tp'), may hold values from -6 to 6
- cum_cache: float32 [16, 1024, 16], P(None, 'kv', 'tp'), may hold values from -402 to 0, as said below
- lengths: int32 [16], replicated, may hold values from 512 to 992
- accepted: int32 [16], replicated, may hold values from 0 to 16
- parent: int32 [16, 16], replicated, may hold values from -1 to 14, as said below
Outputs:
- mixed: bfloat16 [16, 16, 4096], P(None, None, ('kv', 'tp'))
- key_out: bfloat16 [16, 1024, 16, 128], P(None, 'kv', 'tp')
- value_out: bfloat16 [16, 1024, 16, 128], P(None, 'kv', 'tp')
- cum_out: float32 [16, 1024, 16], P(None, 'kv', 'tp')
The draws below stay inside these ranges and needn't reach their ends.
Inputs may be any that keep to these rules, and one draw needn't show every extreme that they name: parent[s, 0] is -1 and parent[s, i] lies between -1 and i - 1. `cum_cache`: along the positions of each sequence and head the values never rise. lengths + accepted + 16 never exceeds 1024.
All inputs are finite; a program needn't handle non-finite values.
Results may differ from the reference program's by a relative error of at most 0.03.
Values may be sent and summed in bfloat16 or wider, within the bound.
A program may use at most 64 MiB of HBM per device.

```python
import jax
import jax.numpy as jnp
from jax import lax

D = 4096
HEADS = 16
HD = 128
PROP = 16
SEQS = 16
POS_DEV = 128
HW = 2048
CACHE_LEN = 1024
SHARDS = 8
GROUPS = 4


def fast_heads(key):
    share = 0.5
    return jax.random.bernoulli(jax.random.fold_in(key, 11), share, (HEADS,))


def draw_b_forget(key, part):
    fast = fast_heads(key)
    spread = jax.random.uniform(jax.random.fold_in(key, 12), (HEADS,), jnp.float32)
    return jnp.where(fast, 0.5 + 1.5 * spread, 2.5 + 1.5 * spread).astype(jnp.float32)


def draw_cum_cache(key, part):
    fast = fast_heads(key)
    slow_rate = jax.random.uniform(jax.random.fold_in(key, 21), (SEQS, HEADS), jnp.float32, 0.3, 1.2) / CACHE_LEN
    fast_rate = 1.0 / jax.random.uniform(jax.random.fold_in(key, 22), (SEQS, HEADS), jnp.float32, 40.0, 100.0)
    rates = jnp.where(fast[None, :], fast_rate, slow_rate)
    factor_pos = jnp.exp(jax.random.uniform(jax.random.fold_in(key, 23), (SEQS, CACHE_LEN, HEADS), jnp.float32, jnp.log(0.6), jnp.log(1.6)))
    factor_block = jnp.exp(jax.random.uniform(jax.random.fold_in(key, 24), (SEQS, CACHE_LEN // POS_DEV, HEADS), jnp.float32, jnp.log(0.5), jnp.log(2.0)))
    factor_block = jnp.repeat(factor_block, POS_DEV, axis=1)
    decrements = -rates[:, None, :] * factor_pos * factor_block
    offsets = jax.random.uniform(jax.random.fold_in(key, 25), (SEQS, 1, HEADS), jnp.float32, -300.0, 0.0)
    return (offsets + jnp.cumsum(decrements, axis=1)).astype(jnp.float32)


def draw_parent(key, part):
    limits = jnp.arange(PROP, dtype=jnp.int32)[None, :]
    return jax.random.randint(key, (SEQS, PROP), -1, limits, dtype=jnp.int32)


def place_ends(entries, stream_key, least, largest):
    longest = entries.shape.index(max(entries.shape))
    spots = []
    for shift in (0, 1):
        where = [jax.random.randint(jax.random.fold_in(stream_key, axis), (), 0, length) for axis, length in enumerate(entries.shape)]
        where[longest] = (where[longest] + shift) % entries.shape[longest]
        spots.append(tuple(where))
    return entries.at[spots[0]].set(least).at[spots[1]].set(largest)


def shard_levels(key, extent, split, low, largest):
    def one(position, blocks):
        draws = jax.random.uniform(jax.random.fold_in(jax.random.fold_in(key, 6), position), (blocks,), jnp.float32, low / len(split), largest / len(split))
        return jnp.repeat(jnp.exp(draws), extent[position] // blocks).reshape((-1,) + (1,) * (len(extent) - position - 1))

    factor_of = one(*split[0])
    for cut in split[1:]:
        factor_of = factor_of * one(*cut)
    return factor_of


def normal_values(key, shape, width, most, split=(), kind=jnp.bfloat16):
    gain = shard_levels(key, shape, split, -0.22, 0.18) if split else 1.0
    drawn = jax.random.normal(key, shape, jnp.float32) * width * gain
    return jnp.minimum(jnp.maximum(drawn, -most), most).astype(kind)


def setup_inputs(seed: int = 0) -> dict:
    key_of = jax.random.split(jax.random.key(seed), 16)
    tokens = normal_values(key_of[0], (SEQS, PROP, D), 1.0, 6.0)
    gain_pre = jnp.clip(1.0 + 0.18 * jax.random.normal(key_of[1], (D,), jnp.float32), 0.1, 1.9)
    w_query = normal_values(key_of[2], (D, HW), D ** -0.5, 0.09375, ((0, 8), (1, 4)))
    w_key = normal_values(key_of[3], (D, HW), D ** -0.5, 0.09375, ((0, 8), (1, 4)))
    w_value = normal_values(key_of[4], (D, HW), D ** -0.5, 0.09375, ((0, 8), (1, 4)))
    w_forget = normal_values(key_of[5], (D, HEADS), D ** -0.5, 0.09375)
    b_forget = draw_b_forget(jax.random.fold_in(key_of[15], 71), 0)
    w_out = normal_values(key_of[7], (HW, D), HW ** -0.5, 0.125, ((0, 4), (1, 8)))
    gain_post = jnp.clip(1.0 + 0.18 * jax.random.normal(key_of[8], (D,), jnp.float32), 0.1, 1.9)
    key_cache = normal_values(key_of[9], (SEQS, CACHE_LEN, HEADS, HD), 1.0, 6.0, ((1, 8), (2, 4)))
    value_cache = normal_values(key_of[10], (SEQS, CACHE_LEN, HEADS, HD), 1.0, 6.0, ((1, 8), (2, 4)))
    cum_cache = draw_cum_cache(jax.random.fold_in(key_of[15], 71), 0)
    lengths = place_ends(jax.random.randint(key_of[12], (SEQS,), CACHE_LEN // 2, CACHE_LEN - 2 * PROP + 1), jax.random.fold_in(key_of[12], 1), CACHE_LEN // 2, CACHE_LEN - 2 * PROP).astype(jnp.int32)
    accepted = place_ends(jax.random.randint(key_of[13], (SEQS,), 0, PROP + 1), jax.random.fold_in(key_of[13], 1), 0, PROP).astype(jnp.int32)
    parent = draw_parent(jax.random.fold_in(key_of[15], 71), 0)
    return {"tokens": tokens, "gain_pre": gain_pre, "w_query": w_query, "w_key": w_key, "w_value": w_value, "w_forget": w_forget, "b_forget": b_forget, "w_out": w_out, "gain_post": gain_post, "key_cache": key_cache, "value_cache": value_cache, "cum_cache": cum_cache, "lengths": lengths, "accepted": accepted, "parent": parent}


epsilon = 1e-06
floor_value = -1e+30

def ancestry(parent_ids, members):
    identity = jnp.eye(members, dtype=jnp.float32)
    parent_hot = (parent_ids[:, :, None] == jnp.arange(members, dtype=jnp.int32)[None, None, :]).astype(jnp.float32)
    ancestors = jnp.minimum(identity[None] + parent_hot, 1.0)
    for sweep in range(max(1, (members - 1).bit_length())):
        ancestors = jnp.minimum(jnp.einsum('bij,bjk->bik', ancestors, ancestors, precision=lax.Precision.HIGHEST), 1.0)
    return ancestors

def reference(tokens, gain_pre, w_query, w_key, w_value, w_forget, b_forget, w_out, gain_post, key_cache, value_cache, cum_cache, lengths, accepted, parent):
    num_seqs = tokens.shape[0]
    scale = HD ** (-0.5)
    tok_float = tokens.astype(jnp.float32)
    normed = (tok_float * lax.rsqrt(lax.optimization_barrier(jnp.mean(tok_float * tok_float, -1, keepdims=True)) + epsilon) * gain_pre.astype(jnp.float32)).astype(jnp.bfloat16)
    flat = normed.reshape(num_seqs * PROP, D)
    query = jnp.dot(flat, w_query, preferred_element_type=jnp.float32).astype(jnp.bfloat16).reshape(num_seqs, PROP, HEADS, HD)
    key_new = jnp.dot(flat, w_key, preferred_element_type=jnp.float32).astype(jnp.bfloat16).reshape(num_seqs, PROP, HEADS, HD)
    value_new = jnp.dot(flat, w_value, preferred_element_type=jnp.float32).astype(jnp.bfloat16).reshape(num_seqs, PROP, HEADS, HD)
    log_forget = jax.nn.log_sigmoid(jnp.dot(flat, w_forget, preferred_element_type=jnp.float32) + b_forget.astype(jnp.float32)).reshape(num_seqs, PROP, HEADS)
    ancestors = ancestry(parent, PROP)
    path = jnp.einsum('bij,bjh->bih', ancestors, log_forget, precision=lax.Precision.HIGHEST)
    valid = (lengths + accepted).astype(jnp.int32)
    last_index = jnp.broadcast_to((valid - 1).astype(jnp.int32)[:, None, None], (num_seqs, 1, HEADS))
    last_cum = jnp.take_along_axis(cum_cache, last_index, axis=1)[:, 0, :]
    query_float = query.astype(jnp.float32)
    key_blocks = jnp.swapaxes(key_cache.reshape(num_seqs, SHARDS, POS_DEV, HEADS, HD), 0, 1)
    value_blocks = jnp.swapaxes(value_cache.reshape(num_seqs, SHARDS, POS_DEV, HEADS, HD), 0, 1)
    cum_blocks = jnp.swapaxes(cum_cache.reshape(num_seqs, SHARDS, POS_DEV, HEADS), 0, 1)
    starts = (jnp.arange(SHARDS, dtype=jnp.int32) * POS_DEV).astype(jnp.int32)

    def add_block(carry, item):
        run_max, run_total, run_values = carry
        block_keys, block_vals, block_cum, start = item
        positions = start + jnp.arange(POS_DEV, dtype=jnp.int32)
        live = (positions[None, :] < valid[:, None])[:, None, None, :]
        score = jnp.einsum('bihd,bkhd->bihk', query_float, block_keys.astype(jnp.float32)) * scale + path[..., None] - jnp.swapaxes(block_cum, 1, 2)[:, None]
        block_max = lax.optimization_barrier(jnp.max(jnp.where(live, score, floor_value), axis=-1))
        weight = jnp.exp(jnp.where(live, score - block_max[..., None], floor_value))
        block_total = lax.optimization_barrier(jnp.sum(weight, axis=-1))
        weight_low = lax.optimization_barrier(weight.astype(jnp.bfloat16)).astype(jnp.float32)
        block_values = jnp.einsum('bihk,bkhd->bihd', weight_low, block_vals.astype(jnp.float32))
        new_max = jnp.maximum(run_max, block_max)
        old_scale = jnp.exp(run_max - new_max)
        new_scale = jnp.exp(block_max - new_max)
        return ((new_max, run_total * old_scale + block_total * new_scale, run_values * old_scale[..., None] + block_values * new_scale[..., None]), None)
    init = (jnp.full((num_seqs, PROP, HEADS), floor_value, jnp.float32), jnp.zeros((num_seqs, PROP, HEADS), jnp.float32), jnp.zeros((num_seqs, PROP, HEADS, HD), jnp.float32))
    (cache_max, cache_total, cache_values), unused = lax.scan(add_block, init, (key_blocks, value_blocks, cum_blocks, starts))
    tree_mask = (ancestors > 0.5)[:, :, None, :]
    tree_score = jnp.einsum('bihd,bjhd->bihj', query_float, key_new.astype(jnp.float32)) * scale + path[..., None] - jnp.swapaxes(path, 1, 2)[:, None]
    tree_max = lax.optimization_barrier(jnp.max(jnp.where(tree_mask, tree_score, floor_value), axis=-1))
    tree_weight = jnp.exp(jnp.where(tree_mask, tree_score - tree_max[..., None], floor_value))
    tree_total = lax.optimization_barrier(jnp.sum(tree_weight, axis=-1))
    tree_low = lax.optimization_barrier(tree_weight.astype(jnp.bfloat16)).astype(jnp.float32)
    tree_values = jnp.einsum('bihj,bjhd->bihd', tree_low, value_new.astype(jnp.float32))
    shifted = cache_max + last_cum[:, None, :]
    top = jnp.maximum(shifted, tree_max)
    cache_scale = jnp.exp(shifted - top)
    tree_scale = jnp.exp(tree_max - top)
    attended = ((cache_values * cache_scale[..., None] + tree_values * tree_scale[..., None]) / (cache_total * cache_scale + tree_total * tree_scale)[..., None]).astype(jnp.bfloat16)
    attended = attended.reshape(num_seqs * PROP, GROUPS, HW // GROUPS).astype(jnp.float32)
    group_out = jnp.einsum('tgc,gcd->gtd', attended, w_out.reshape(GROUPS, HW // GROUPS, D).astype(jnp.float32))
    group_out = lax.optimization_barrier(group_out.astype(jnp.bfloat16)).astype(jnp.float32)
    mixed_sum = lax.optimization_barrier(jnp.sum(group_out, axis=0))
    mixed = (mixed_sum * lax.rsqrt(lax.optimization_barrier(jnp.mean(mixed_sum * mixed_sum, -1, keepdims=True)) + epsilon) * gain_post.astype(jnp.float32)).astype(jnp.bfloat16).reshape(num_seqs, PROP, D)
    zero_index = jnp.zeros((), jnp.int32)

    def write_rows(cache_rows, new_rows, start):
        return lax.dynamic_update_slice(cache_rows, new_rows, (start.astype(jnp.int32), zero_index, zero_index))
    key_out = jax.vmap(write_rows)(key_cache, key_new, valid)
    value_out = jax.vmap(write_rows)(value_cache, value_new, valid)
    cum_new = last_cum[:, None, :] + path

    def write_cum(cache_rows, new_rows, start):
        return lax.dynamic_update_slice(cache_rows, new_rows, (start.astype(jnp.int32), zero_index))
    cum_out = jax.vmap(write_cum)(cum_cache, cum_new, valid)
    return (mixed, key_out, value_out, cum_out)
```

```python
import functools

import jax
import jax.numpy as jnp
from jax import lax
from jax.experimental import pallas as pl
from jax.experimental.pallas import tpu as pltpu
from jax.sharding import PartitionSpec as P

epsilon = 1e-06
floor_value = -1e30


def merged(part, axis, combine):
    gathered = jax.tree.map(lambda a: lax.all_gather(a, axis), part)

    def take(source):
        return jax.tree.map(lambda a: lax.dynamic_index_in_dim(a, source, 0, False), gathered)

    return lax.fori_loop(
        1, lax.axis_size(axis), lambda source, state: combine(state, take(source)), take(0)
    )


def ancestry(parent_ids, members):
    identity = jnp.eye(members, dtype=jnp.float32)
    parent_hot = (
        parent_ids[:, :, None] == jnp.arange(members, dtype=jnp.int32)[None, None, :]
    ).astype(jnp.float32)
    ancestors = jnp.minimum(identity[None] + parent_hot, 1.0)
    for sweep in range(max(1, (members - 1).bit_length())):
        ancestors = jnp.minimum(
            jnp.einsum("bij,bjk->bik", ancestors, ancestors, precision=lax.Precision.HIGHEST), 1.0
        )
    return ancestors


def combine_parts(first, second):
    new_max = jnp.maximum(first[0], second[0])
    first_scale = jnp.exp(first[0] - new_max)
    second_scale = jnp.exp(second[0] - new_max)
    return (
        new_max,
        first[1] * first_scale + second[1] * second_scale,
        first[2] * first_scale[..., None] + second[2] * second_scale[..., None],
        jnp.maximum(first[3], second[3]),
    )


def finish_rows(cache_max, cache_total, cache_values, last_rows, tree_max, tree_total, tree_values):
    shifted = cache_max + last_rows
    top = jnp.maximum(shifted, tree_max)
    cache_scale = jnp.exp(shifted - top)
    tree_scale = jnp.exp(tree_max - top)
    attended = (
        (cache_values * cache_scale[..., None] + tree_values * tree_scale[..., None])
        / (cache_total * cache_scale + tree_total * tree_scale)[..., None]
    ).astype(jnp.bfloat16)
    return attended.reshape(attended.shape[0], attended.shape[1] * attended.shape[2])


def per_device(
    tokens,
    gain_pre,
    w_query,
    w_key,
    w_value,
    w_forget,
    b_forget,
    w_out,
    gain_post,
    key_cache,
    value_cache,
    cum_cache,
    lengths,
    accepted,
    parent,
):
    num_seqs, proposals, model_width = tokens.shape
    kv_rank = lax.axis_index("kv")
    tp_rank = lax.axis_index("tp")
    span = key_cache.shape[1]
    heads_local = key_cache.shape[2]
    head_dim = key_cache.shape[3]
    scale = head_dim ** (-0.5)
    all_rows = num_seqs * proposals
    tok_float = tokens.astype(jnp.float32)
    normed = (
        tok_float
        * lax.rsqrt(jnp.mean(tok_float * tok_float, -1, keepdims=True) + epsilon)
        * gain_pre
    ).astype(jnp.bfloat16)
    flat = normed.reshape(all_rows, model_width)
    weight_rows = w_query.shape[0]
    local_rows = lax.dynamic_slice_in_dim(flat, kv_rank * weight_rows, weight_rows, 1)
    query_part = jnp.dot(local_rows, w_query, preferred_element_type=jnp.float32)
    key_part = jnp.dot(local_rows, w_key, preferred_element_type=jnp.float32)
    value_part = jnp.dot(local_rows, w_value, preferred_element_type=jnp.float32)
    summed = (
        lax.psum(query_part.astype(jnp.bfloat16), "kv").astype(jnp.float32),
        lax.psum(key_part.astype(jnp.bfloat16), "kv").astype(jnp.float32),
        lax.psum(value_part.astype(jnp.bfloat16), "kv").astype(jnp.float32),
    )
    query_flat = summed[0].astype(jnp.bfloat16)
    key_flat = summed[1].astype(jnp.bfloat16)
    value_flat = summed[2].astype(jnp.bfloat16)
    query = query_flat.reshape(num_seqs, proposals, heads_local, head_dim)
    key_new = key_flat.reshape(num_seqs, proposals, heads_local, head_dim)
    value_new = value_flat.reshape(num_seqs, proposals, heads_local, head_dim)
    forget_cols = lax.dynamic_slice_in_dim(w_forget, tp_rank * heads_local, heads_local, 1)
    forget_bias = lax.dynamic_slice_in_dim(b_forget, tp_rank * heads_local, heads_local, 0)
    log_forget = jax.nn.log_sigmoid(
        jnp.dot(flat, forget_cols, preferred_element_type=jnp.float32) + forget_bias
    ).reshape(num_seqs, proposals, heads_local)
    ancestors = ancestry(parent, proposals)
    path = jnp.einsum("bij,bjh->bih", ancestors, log_forget, precision=lax.Precision.HIGHEST)
    valid = lengths + accepted
    positions = kv_rank * span + jnp.arange(span, dtype=jnp.int32)
    live = (positions[None, :] < valid[:, None])[:, None, None, :]
    score = (
        jnp.einsum("bihd,bkhd->bihk", query, key_cache, preferred_element_type=jnp.float32) * scale
        + path[..., None]
        - jnp.swapaxes(cum_cache, 1, 2)[:, None]
    )
    block_max = jnp.max(jnp.where(live, score, floor_value), axis=-1)
    weight = jnp.exp(jnp.where(live, score - block_max[..., None], floor_value))
    block_total = jnp.sum(weight, axis=-1)
    block_values = jnp.einsum(
        "bihk,bkhd->bihd",
        weight.astype(jnp.bfloat16),
        value_cache,
        preferred_element_type=jnp.float32,
    )
    owner = positions[None, :] == (valid - 1)[:, None]
    candidate = jnp.max(jnp.where(owner[:, :, None], cum_cache, floor_value), axis=1)
    tree_mask = (ancestors > 0.5)[:, :, None, :]
    tree_score = (
        jnp.einsum("bihd,bjhd->bihj", query, key_new, preferred_element_type=jnp.float32) * scale
        + path[..., None]
        - jnp.swapaxes(path, 1, 2)[:, None]
    )
    tree_max = jnp.max(jnp.where(tree_mask, tree_score, floor_value), axis=-1)
    tree_weight = jnp.exp(jnp.where(tree_mask, tree_score - tree_max[..., None], floor_value))
    tree_total = jnp.sum(tree_weight, axis=-1)
    tree_values = jnp.einsum(
        "bihj,bjhd->bihd",
        tree_weight.astype(jnp.bfloat16),
        value_new,
        preferred_element_type=jnp.float32,
    )
    tree_max_rows = tree_max.reshape(all_rows, heads_local)
    tree_total_rows = tree_total.reshape(all_rows, heads_local)
    tree_values_rows = tree_values.reshape(all_rows, heads_local, head_dim)
    cache_max, cache_total, cache_values, last_cum = merged(
        (block_max, block_total, block_values, candidate), "kv", combine_parts
    )
    last_rows = jnp.broadcast_to(last_cum[:, None, :], (num_seqs, proposals, heads_local)).reshape(
        all_rows, heads_local
    )
    attended = finish_rows(
        cache_max.reshape(all_rows, heads_local),
        cache_total.reshape(all_rows, heads_local),
        cache_values.reshape(all_rows, heads_local, head_dim),
        last_rows,
        tree_max_rows,
        tree_total_rows,
        tree_values_rows,
    )
    mixed_part = jnp.dot(attended, w_out, preferred_element_type=jnp.float32)
    mixed_sum = lax.psum_scatter(
        mixed_part.astype(jnp.bfloat16), "tp", scatter_dimension=1, tiled=True
    ).astype(jnp.float32)
    squares = lax.psum(jnp.sum(mixed_sum * mixed_sum, axis=1), ("kv", "tp"))
    mixed = (mixed_sum * lax.rsqrt(squares / model_width + epsilon)[:, None] * gain_post).astype(
        jnp.bfloat16
    )
    mixed = mixed.reshape(num_seqs, proposals, mixed_sum.shape[1])
    relative = positions[None, :] - valid[:, None]
    select = relative[:, :, None] == jnp.arange(proposals, dtype=jnp.int32)[None, None, :]
    written = (relative >= 0) & (relative < proposals)
    placed_keys = jnp.einsum(
        "bkj,bjhd->bkhd", select.astype(jnp.bfloat16), key_new, preferred_element_type=jnp.float32
    ).astype(jnp.bfloat16)
    placed_values = jnp.einsum(
        "bkj,bjhd->bkhd", select.astype(jnp.bfloat16), value_new, preferred_element_type=jnp.float32
    ).astype(jnp.bfloat16)
    key_out = jnp.where(written[:, :, None, None], placed_keys, key_cache)
    value_out = jnp.where(written[:, :, None, None], placed_values, value_cache)
    cum_new = last_cum[:, None, :] + path
    placed_cum = jnp.einsum(
        "bkj,bjh->bkh", select.astype(jnp.float32), cum_new, precision=lax.Precision.HIGHEST
    )
    cum_out = jnp.where(written[:, :, None], placed_cum, cum_cache)
    return (mixed, key_out, value_out, cum_out)


MESH = pl.DeviceIdType.MESH
HI = lax.Precision.HIGHEST
F32 = jnp.float32
BF = jnp.bfloat16


def iota(shape, dim):
    return lax.broadcasted_iota(jnp.int32, shape, dim)


def hot(mask):
    return jnp.where(mask, 1.0, 0.0).astype(F32)


def dot_hi(a, b, dims=(((1,), (0,)), ((), ()))):
    return lax.dot_general(a, b, dims, precision=HI, preferred_element_type=F32)


NT = (((1,), (1,)), ((), ()))


def flip(value, mask):
    total = 0
    bit = 1
    while bit < 64:
        total = total + ((value // bit + mask // bit) % 2) * bit
        bit *= 2
    return total


def layer_kernel(
    n,
    nt,
    num_seqs,
    prop,
    heads,
    hd,
    span,
    tok_h,
    gain_h,
    wq_h,
    wk_h,
    wv_h,
    wft_h,
    bias_h,
    wo_h,
    gpost_h,
    kc_h,
    vc_h,
    cum_h,
    lens_h,
    accs_h,
    parent_h,
    mixed_out,
    cum_out,
    knew_out,
    vnew_out,
    tokv,
    gain,
    wqkv,
    wft,
    bias,
    wov,
    gpost,
    kcv,
    vcv,
    cum,
    lens,
    accs,
    parent,
    ssq,
    invv,
    xloc,
    part_q,
    q_recv,
    q_full,
    part_kv,
    kv_y,
    kv_zs,
    kv_zr,
    kv_full,
    st_send,
    val_send,
    st_recv,
    val_recv,
    cand_send,
    cand_recv,
    brow,
    anc,
    tpath,
    ptile,
    att,
    o_send,
    o_recv,
    sq_send,
    sq_recv,
    loc,
    ssem,
    rsem,
    tssem,
    trsem,
    qssem,
    qrsem,
):
    me = lax.axis_index("kv")
    mt = lax.axis_index("tp")
    rows, width = tokv.shape
    hw = heads * hd
    kdim = wq_h.shape[0]
    cols = heads * span
    sp = num_seqs // n
    R = sp * prop
    hp = heads * prop
    L = sp * hp
    scale = hd ** (-0.5)
    base = me * span
    heads_all = wft.shape[0]
    half = n // 2
    everyone = n * nt

    barrier = pltpu.get_barrier_semaphore()

    def greet(e, c):
        pl.semaphore_signal(
            barrier,
            inc=1,
            device_id={"kv": flip(me, e // nt), "tp": flip(mt, e % nt)},
            device_id_type=MESH,
        )
        return c

    chunks = 4
    crow = rows // chunks
    in_tok = [
        pltpu.make_async_copy(
            tok_h.at[pl.ds(i * crow, crow)], tokv.at[pl.ds(i * crow, crow)], loc.at[i]
        )
        for i in range(chunks)
    ]
    later = [
        (gain_h, gain),
        (wq_h, wqkv.at[0]),
        (wk_h, wqkv.at[1]),
        (wv_h, wqkv.at[2]),
        (wft_h, wft),
        (bias_h, bias),
        (lens_h, lens),
        (accs_h, accs),
        (parent_h, parent),
        (cum_h, cum),
        (gpost_h, gpost),
        (kc_h, kcv),
        (vc_h, vcv),
        (wo_h, wov),
    ]
    copies = [
        pltpu.make_async_copy(src, dst, loc.at[chunks + i]) for i, (src, dst) in enumerate(later)
    ]
    (
        in_gain,
        in_wq,
        in_wk,
        in_wv,
        in_wft,
        in_bias,
        in_lens,
        in_accs,
        in_parent,
        in_cum,
        in_gpost,
        in_kc,
        in_vc,
        in_wo,
    ) = copies
    for c in in_tok:
        c.start()
    for c in copies:
        c.start()
    lax.fori_loop(1, everyone, greet, 0)

    def to_kv(ph, slot, mask, src, dst):
        return pltpu.make_async_remote_copy(
            src_ref=src,
            dst_ref=dst,
            send_sem=ssem.at[ph, slot],
            recv_sem=rsem.at[ph, slot],
            device_id={"kv": flip(me, mask)},
            device_id_type=MESH,
        )

    def rrow(i):
        return pl.ds(pl.multiple_of(i * R, R), R)

    def q_rs(m):
        return to_kv(0, m, m, part_q.at[rrow(flip(me, m))], q_recv.at[m])

    def q_ag(m):
        return to_kv(1, m, m, q_full.at[rrow(me)], q_full.at[rrow(me)])

    def kv_yrs(m):
        return to_kv(2, m, 1, part_kv.at[rrow(flip(me, m + 1))], kv_y.at[m // 2])

    def kv_zrs(m):
        return to_kv(2, m + 1, m, kv_zs.at[m // 2], kv_zr.at[m // 2])

    def cand_copy(m):
        return to_kv(3, m, m, cand_send, cand_recv.at[m])

    def stat_copy(m):
        return to_kv(4, m, m, st_send.at[m], st_recv.at[m])

    def val_copy(m):
        return to_kv(5, m, m, val_send.at[m], val_recv.at[m])

    def att_copy(m):
        return to_kv(6, m, m, att.at[rrow(me)], att.at[rrow(me)])

    def kv_zag(m):
        return to_kv(7, m, m, kv_full.at[rrow(me)], kv_full.at[rrow(me)])

    def kv_yag(m):
        return to_kv(7, m + 1, 1, kv_full.at[rrow(flip(me, m))], kv_full.at[rrow(flip(me, m))])

    def each(count, fn):
        def body(d, c):
            fn(d)
            return c

        lax.fori_loop(1, count, body, 0)

    def each_far(count, fn):
        each(count, lambda d: fn(count - d))

    zmasks = list(range(2, n, 2))
    nb = prop
    lanes = 128

    def sum_rows(i, c):
        sl = pl.ds(pl.multiple_of(i * nb, nb), nb)
        accs4 = [None] * 4
        for j in range(width // lanes):
            t = tokv[sl, j * lanes : (j + 1) * lanes].astype(F32)
            p = t * t
            accs4[j % 4] = p if accs4[j % 4] is None else accs4[j % 4] + p
        ssq[sl, :] = (accs4[0] + accs4[1]) + (accs4[2] + accs4[3])
        return c

    for i in range(chunks):
        in_tok[i].wait()
        lax.fori_loop(i * crow // nb, (i + 1) * crow // nb, sum_rows, 0)
    total = dot_hi(ssq[...], jnp.ones((lanes, lanes), F32))
    inv = lax.rsqrt(total / width + epsilon)
    invv[...] = inv
    in_gain.wait()
    for j in range(kdim // lanes):
        at = pl.ds(pl.multiple_of(me * kdim + j * lanes, lanes), lanes)
        xloc[:, j * lanes : (j + 1) * lanes] = (
            tokv[:, at].astype(F32) * inv * gain[:, at]
        ).astype(BF)
    in_wq.wait()
    part_q[...] = jnp.dot(xloc[...], wqkv[0], preferred_element_type=F32).astype(BF)
    pl.semaphore_wait(barrier, everyone - 1)
    each_far(n, lambda m: q_rs(m).start())
    in_wk.wait()
    in_wv.wait()
    part_kv[:, 0:hw] = jnp.dot(xloc[...], wqkv[1], preferred_element_type=F32).astype(BF)
    part_kv[:, hw : 2 * hw] = jnp.dot(xloc[...], wqkv[2], preferred_element_type=F32).astype(BF)
    for m in zmasks[::-1] + [0]:
        kv_yrs(m).start()

    in_lens.wait()
    in_accs.wait()
    in_cum.wait()
    r64 = num_seqs * heads
    c64 = cum[...]
    srow = iota((r64, span), 0) // heads
    lane = iota((r64, span), 1)
    rel64 = jnp.zeros((r64, span), jnp.int32)
    rel16 = jnp.zeros((num_seqs, cols), jnp.int32)
    s16 = iota((num_seqs, cols), 0)
    for s in range(num_seqs):
        rel_s = lens[s] + accs[s] - base
        rel64 = jnp.where(srow == s, rel_s, rel64)
        rel16 = jnp.where(s16 == s, rel_s, rel16)
    cand = jnp.max(jnp.where(lane == rel64 - 1, c64, floor_value), axis=1, keepdims=True)
    diag = iota((r64, 128), 0) == iota((r64, 128), 1)
    cand_send[...] = jnp.sum(jnp.where(diag, cand, 0.0), axis=0, keepdims=True)
    each_far(n, lambda m: cand_copy(m).start())

    spread = hot(iota((span, cols), 1) // heads == iota((span, cols), 0))
    e1 = dot_hi(c64, spread)
    e1 = jnp.where(iota((r64, cols), 0) % heads == iota((r64, cols), 1) % heads, e1, 0.0)
    take = hot(iota((num_seqs, r64), 1) // heads == iota((num_seqs, r64), 0))
    cflat = dot_hi(take, e1)
    brow[...] = jnp.where(iota((num_seqs, cols), 1) // heads < rel16, -cflat, floor_value)

    in_parent.wait()
    ri = iota((rows, rows), 0)
    ci = iota((rows, rows), 1)
    pick = hot(iota((rows, num_seqs), 0) // prop == iota((rows, num_seqs), 1))
    pb = dot_hi(pick, parent[...].astype(F32))
    pcol = jnp.sum(
        jnp.where(iota((rows, prop), 1) == iota((rows, prop), 0) % prop, pb, 0.0),
        axis=1,
        keepdims=True,
    )
    target = jnp.where(pcol >= 0.0, (ri // prop * prop).astype(F32) + pcol, -1.0)
    a = jnp.where((ri == ci) | (ci.astype(F32) == target), 1.0, 0.0)
    for sweep in range(max(1, (prop - 1).bit_length())):
        low = a.astype(BF)
        a = jnp.minimum(jnp.dot(low, low, preferred_element_type=F32), 1.0)
    anc[...] = a
    in_wft.wait()
    in_bias.wait()
    wscaled = wft[...].astype(F32) * gain[...]
    whigh = wscaled.astype(BF)
    wlow = (wscaled - whigh.astype(F32)).astype(BF)
    lf = lax.dot_general(
        jnp.concatenate([whigh, wlow], axis=0), tokv[...], NT, preferred_element_type=F32
    )
    lf = lf[0:heads_all] + lf[heads_all : 2 * heads_all]
    inv_lane = dot_hi(jnp.full((8, lanes), 1.0 / lanes, F32), invv[...], NT)[0:1]
    bcol = jnp.zeros((heads_all, rows), F32)
    for h in range(heads_all):
        bcol = jnp.where(iota((heads_all, rows), 0) == h, bias[h], bcol)
    z = lf * inv_lane + bcol
    lf = jnp.minimum(z, 0.0) - jnp.log1p(jnp.exp(-jnp.abs(z)))
    path_t = dot_hi(lf, a, NT)
    rep = hot(iota((r64, heads_all), 1) == mt * heads + iota((r64, heads_all), 0) % heads)
    pm = dot_hi(rep, path_t)
    pm = jnp.where(iota((r64, rows), 1) // prop == iota((r64, rows), 0) // heads, pm, 0.0)
    fold = hot(iota((rows, 128), 0) % prop == iota((rows, 128), 1) % prop)
    pt = dot_hi(pm, fold)
    ptile[...] = pt
    ptm = jnp.where((iota((r64, 128), 1) // prop) % heads == iota((r64, 128), 0) % heads, pt, 0.0)
    tpath[...] = dot_hi(take, ptm)
    in_kc.wait()
    in_vc.wait()

    own = part_q[rrow(me)].astype(F32)
    for m in range(1, n):
        q_rs(m).wait_recv()
        own = own + q_recv[m].astype(F32)
    q_full[rrow(me)] = own.astype(BF)
    each_far(n, lambda m: q_ag(m).start())

    for m in zmasks[::-1]:
        kv_yrs(m).wait_recv()
        kv_zs[m // 2] = (
            part_kv[rrow(flip(me, m))].astype(F32) + kv_y[m // 2].astype(F32)
        ).astype(BF)
        kv_zrs(m).start()

    same_head = iota((hp, cols), 0) // prop == iota((hp, cols), 1) % heads
    diag_l = iota((L, L), 0) == iota((L, L), 1)

    def heads_of(ref, s, first):
        block = ref[pl.ds(pl.multiple_of(s * prop, prop), prop), first : first + hw]
        return jnp.concatenate([block[:, h * hd : (h + 1) * hd] for h in range(heads)], axis=0)

    def block_part(src):
        maxes, totals, values = [], [], []
        for j in range(sp):
            s = src * sp + j
            q = heads_of(q_full, s, 0)
            sc = lax.dot_general(q, kcv[s], NT, preferred_element_type=F32) * scale
            sc = jnp.where(same_head, sc + brow[pl.ds(s, 1), :], floor_value)
            m = jnp.max(sc, axis=1, keepdims=True)
            w = jnp.exp(sc - m)
            maxes.append(m)
            totals.append(jnp.sum(w, axis=1, keepdims=True))
            values.append(
                jnp.dot(w.astype(BF), vcv[s], preferred_element_type=F32).astype(BF)
            )
        m = jnp.concatenate(maxes, axis=0)
        t = jnp.concatenate(totals, axis=0)
        m_lane = jnp.sum(jnp.where(diag_l, m, 0.0), axis=0, keepdims=True)
        t_lane = jnp.sum(jnp.where(diag_l, t, 0.0), axis=0, keepdims=True)
        stats = jnp.where(iota((2, L), 0) == 0, m_lane, t_lane)
        return stats, jnp.concatenate(values, axis=0)

    def remote_block(m):
        q_ag(m).wait_recv()
        stats, values = block_part(flip(me, m))
        st_send[m] = stats
        val_send[m] = values
        stat_copy(m).start()
        val_copy(m).start()

    stats, values = block_part(me)
    st_recv[0] = stats
    val_recv[0] = values
    each(n, remote_block)

    kv_yrs(0).wait_recv()
    own = part_kv[rrow(me)].astype(F32) + kv_y[0].astype(F32)
    for m in zmasks:
        kv_zrs(m).wait_recv()
        own = own + kv_zr[m // 2].astype(F32)
    kv_full[rrow(me)] = own.astype(BF)

    fold_h = iota((rows, hp), 0)
    tmax, ttot, tval = [], [], []
    for j in range(sp):
        s = me * sp + j
        q = heads_of(q_full, s, 0)
        k = heads_of(kv_full, s, 0)
        v = heads_of(kv_full, s, hw)
        arows = anc[pl.ds(pl.multiple_of(s * prop, prop), prop), :]
        sel = hot(fold_h == s * prop + iota((rows, hp), 1) % prop).astype(BF)
        am = jnp.dot(arows.astype(BF), sel, preferred_element_type=F32)
        am = jnp.concatenate([am] * heads, axis=0)
        mask = (am > 0.5) & (iota((hp, hp), 0) // prop == iota((hp, hp), 1) // prop)
        sc = lax.dot_general(q, k, NT, preferred_element_type=F32) * scale
        sc = jnp.where(mask, sc - tpath[pl.ds(s, 1), 0:hp], floor_value)
        m = jnp.max(sc, axis=1, keepdims=True)
        w = jnp.where(mask, jnp.exp(sc - m), 0.0)
        tmax.append(m)
        ttot.append(jnp.sum(w, axis=1, keepdims=True))
        tval.append(jnp.dot(w.astype(BF), v, preferred_element_type=F32))
    tree_max = jnp.concatenate(tmax, axis=0)
    tree_tot = jnp.concatenate(ttot, axis=0)
    tree_val = jnp.concatenate(tval, axis=0)

    last_lane = cand_send[...]
    for m in range(1, n):
        cand_copy(m).wait_recv()
        last_lane = jnp.maximum(last_lane, cand_recv[m])
    last_col = jnp.sum(jnp.where(diag, last_lane, 0.0), axis=1, keepdims=True)
    own_rows = iota((L, 128), 0)
    own_pick = iota((L, 128), 1) == (me * sp + own_rows // hp) * heads + (own_rows % hp) // prop
    last_own = jnp.sum(jnp.where(own_pick, last_lane, 0.0), axis=1, keepdims=True)

    shifted_path = ptile[...]
    for b in range((span - 1).bit_length()):
        moved = pltpu.roll(shifted_path, 1 << b, 1)
        shifted_path = jnp.where((rel64 >> b) & 1 == 1, moved, shifted_path)
    off = lane - rel64
    cum_out[...] = jnp.where((off >= 0) & (off < prop), last_col + shifted_path, c64)

    for m in range(1, n):
        stat_copy(m).wait_recv()
    top = st_recv[0, 0:1]
    for m in range(1, n):
        top = jnp.maximum(top, st_recv[m, 0:1])

    def col(x):
        return jnp.sum(jnp.where(diag_l, x, 0.0), axis=1, keepdims=True)

    cache_tot = jnp.zeros((1, L), F32)
    scales = []
    for m in range(n):
        sd = jnp.exp(st_recv[m, 0:1] - top)
        scales.append(col(sd))
        cache_tot = cache_tot + st_recv[m, 1:2] * sd
    shifted = col(top) + last_own
    both = jnp.maximum(shifted, tree_max)
    cscale = jnp.exp(shifted - both)
    tscale = jnp.exp(tree_max - both)
    denom = col(cache_tot) * cscale + tree_tot * tscale
    vals = val_recv[0].astype(F32) * scales[0]
    for m in range(1, n):
        val_copy(m).wait_recv()
        vals = vals + val_recv[m].astype(F32) * scales[m]
    attended = ((vals * cscale + tree_val * tscale) / denom).astype(BF)
    for j in range(sp):
        for h in range(heads):
            att[pl.ds(pl.multiple_of(me * R + j * prop, prop), prop), h * hd : (h + 1) * hd] = (
                attended[j * hp + h * prop : j * hp + (h + 1) * prop]
            )
    each_far(n, lambda m: att_copy(m).start())

    upper = me >= half

    @pl.when(upper)
    def _():
        for m in [z for z in zmasks if z < half]:
            kv_zag(m).start()
        kv_yag(0).start()

    @pl.when(jnp.logical_not(upper))
    def _():
        for m in [z for z in zmasks if z >= half]:
            kv_zag(m).start()

    in_wo.wait()
    each(n, lambda m: to_kv(6, m, m, att.at[rrow(me)], att.at[rrow(flip(me, m))]).wait_recv())
    full = jnp.dot(att[...], wov[...], preferred_element_type=F32).astype(BF)
    oc = o_send.shape[2]
    for t in range(nt):
        o_send[t] = full[:, t * oc : (t + 1) * oc]

    def o_copy(d):
        return pltpu.make_async_remote_copy(
            src_ref=o_send.at[flip(mt, d)],
            dst_ref=o_recv.at[d],
            send_sem=tssem.at[d],
            recv_sem=trsem.at[d],
            device_id={"tp": flip(mt, d)},
            device_id_type=MESH,
        )

    each_far(nt, lambda d: o_copy(d).start())

    @pl.when(upper)
    def _():
        for m in zmasks:
            to_kv(7, m, m, kv_full.at[rrow(me)], kv_full.at[rrow(flip(me, m))]).wait_recv()
            kv_yag(m).start()

    mixed = o_send[mt].astype(F32)
    for d in range(1, nt):
        o_copy(d).wait_recv()
        mixed = mixed + o_recv[d].astype(F32)
    sq = dot_hi(jnp.ones((8, oc), F32), mixed * mixed, NT)[0:1]
    sq_send[...] = sq

    def sq_copy(e):
        return pltpu.make_async_remote_copy(
            src_ref=sq_send,
            dst_ref=sq_recv.at[e],
            send_sem=qssem.at[e],
            recv_sem=qrsem.at[e],
            device_id={"kv": flip(me, e // nt), "tp": flip(mt, e % nt)},
            device_id_type=MESH,
        )

    each_far(everyone, lambda e: sq_copy(e).start())

    order = hot(
        iota((hp, hp), 1) == iota((hp, hp), 0) % heads * prop + iota((hp, hp), 0) // heads
    ).astype(BF)

    unroll = 4

    @pl.when(upper)
    def _():
        for m in [0] + zmasks:
            to_kv(
                7, m + 1, 1, kv_full.at[rrow(me)], kv_full.at[rrow(flip(me, m + 1))]
            ).wait_recv()

        def some(i, c):
            fresh = [
                heads_of(kv_full, i * unroll + j, first) for j in range(unroll) for first in (0, hw)
            ]
            placed = jnp.dot(
                order, jnp.concatenate(fresh, axis=1), preferred_element_type=F32
            ).astype(BF)
            for j in range(unroll):
                at = 2 * j * hd
                knew_out[i * unroll + j] = placed[:, at : at + hd]
                vnew_out[i * unroll + j] = placed[:, at + hd : at + 2 * hd]
            return c

        lax.fori_loop(0, num_seqs // unroll, some, 0)

    for e in range(1, everyone):
        sq_copy(e).wait_recv()
        sq = sq + sq_recv[e]
    ssum = dot_hi(
        jnp.broadcast_to(sq, (8, rows)), jnp.full((8, oc), 0.125, F32), (((0,), (0,)), ((), ()))
    )
    in_gpost.wait()
    mixed_out[...] = (mixed * lax.rsqrt(ssum / width + epsilon) * gpost[...]).astype(BF)

    def drain(m):
        q_rs(m).wait_send()
        q_ag(m).wait_send()
        cand_copy(m).wait_send()
        stat_copy(m).wait_send()
        val_copy(m).wait_send()
        att_copy(m).wait_send()

    each(n, drain)
    for m in [0] + zmasks:
        kv_yrs(m).wait_send()
    for m in zmasks:
        kv_zrs(m).wait_send()

    @pl.when(upper)
    def _():
        for m in [z for z in zmasks if z < half]:
            kv_zag(m).wait_send()
        for m in [0] + zmasks:
            kv_yag(m).wait_send()

    @pl.when(jnp.logical_not(upper))
    def _():
        for m in [z for z in zmasks if z >= half]:
            kv_zag(m).wait_send()

    each(nt, lambda d: o_copy(d).wait_send())
    each(everyone, lambda e: sq_copy(e).wait_send())


def patch_kernel(
    n, prop, kc, vc, knew, vnew, mixed, cum, lens, accs, k_out, v_out, mixed_out, cum_out, sem, bsem, wsem
):
    me = lax.axis_index("kv")
    num_seqs, span = k_out.shape[:2]
    out_m = pltpu.make_async_copy(mixed, mixed_out, sem.at[0])
    out_c = pltpu.make_async_copy(cum, cum_out, sem.at[1])
    bulk = [
        [
            pltpu.make_async_copy(src.at[s], dst.at[s], bsem.at[i, s])
            for i, (src, dst) in enumerate(((kc, k_out), (vc, v_out)))
        ]
        for s in range(num_seqs)
    ]
    for row in bulk:
        for c in row:
            c.start()
    out_m.start()
    out_c.start()

    def moves(act, before=None):
        for s in range(num_seqs):
            if before is not None:
                before(s)
            at = lens[s] + accs[s] - me * span
            pairs = ((knew, k_out), (vnew, v_out))

            @pl.when((at >= 0) & (at <= span - prop))
            def _():
                for i, (src, dst) in enumerate(pairs):
                    act(
                        pltpu.make_async_copy(
                            src.at[s], dst.at[s, pl.ds(at, prop)], wsem.at[i, s]
                        )
                    )

            @pl.when(((at > -prop) & (at < 0)) | ((at > span - prop) & (at < span)))
            def _():
                def one(j, c):
                    @pl.when((at + j >= 0) & (at + j < span))
                    def _():
                        for i, (src, dst) in enumerate(pairs):
                            act(
                                pltpu.make_async_copy(
                                    src.at[s, j], dst.at[s, at + j], wsem.at[i, s]
                                )
                            )

                    return c

                lax.fori_loop(0, prop, one, 0)

    def settle(s):
        for c in bulk[s]:
            c.wait()

    @pl.when(me >= n // 2)
    def _():
        moves(lambda c: c.start(), settle)
        moves(lambda c: c.wait())

    @pl.when(me < n // 2)
    def _():
        for s in range(num_seqs):
            settle(s)

    out_m.wait()
    out_c.wait()


def fast_device(
    n,
    nt,
    tokens,
    gain_pre,
    w_query,
    w_key,
    w_value,
    w_forget,
    b_forget,
    w_out,
    gain_post,
    key_cache,
    value_cache,
    cum_cache,
    lengths,
    accepted,
    parent,
):
    num_seqs, prop, width = tokens.shape
    span, heads, hd = key_cache.shape[1:]
    rows = num_seqs * prop
    hw = heads * hd
    cols = heads * span
    sp = num_seqs // n
    R = sp * prop
    L = sp * heads * prop
    oc = gain_post.shape[0]
    half = n // 2
    everyone = n * nt
    kc = key_cache.reshape(num_seqs, cols, hd)
    vc = value_cache.reshape(num_seqs, cols, hd)
    cum = jnp.swapaxes(cum_cache, 1, 2).reshape(num_seqs * heads, span)
    hbm = pl.BlockSpec(memory_space=pltpu.HBM)
    vmem = pl.BlockSpec(memory_space=pltpu.VMEM)
    smem = pl.BlockSpec(memory_space=pltpu.SMEM)
    V = pltpu.VMEM
    S = pltpu.SMEM
    D = pltpu.SemaphoreType.DMA
    mixed, cum_new, knew, vnew = pl.pallas_call(
        functools.partial(layer_kernel, n, nt, num_seqs, prop, heads, hd, span),
        out_shape=(
            V((rows, oc), BF),
            V(cum.shape, F32),
            V((num_seqs, heads * prop, hd), BF),
            V((num_seqs, heads * prop, hd), BF),
        ),
        in_specs=[hbm] * 15,
        out_specs=(vmem, vmem, vmem, vmem),
        scratch_shapes=[
            V((rows, width), BF),
            V((1, width), F32),
            V((3,) + w_query.shape, BF),
            V(w_forget.shape[::-1], BF),
            S(b_forget.shape, F32),
            V(w_out.shape, BF),
            V((1, oc), F32),
            V(kc.shape, BF),
            V(vc.shape, BF),
            V(cum.shape, F32),
            S(lengths.shape, jnp.int32),
            S(accepted.shape, jnp.int32),
            V(parent.shape, jnp.int32),
            V((rows, 128), F32),
            V((rows, 128), F32),
            V((rows, w_query.shape[0]), BF),
            V((rows, hw), BF),
            V((n, R, hw), BF),
            V((rows, hw), BF),
            V((rows, 2 * hw), BF),
            V((half, R, 2 * hw), BF),
            V((half, R, 2 * hw), BF),
            V((half, R, 2 * hw), BF),
            V((rows, 2 * hw), BF),
            V((n, 2, L), F32),
            V((n, L, hd), BF),
            V((n, 2, L), F32),
            V((n, L, hd), BF),
            V((1, 128), F32),
            V((n, 1, 128), F32),
            V((num_seqs, cols), F32),
            V((rows, rows), F32),
            V((num_seqs, 128), F32),
            V((num_seqs * heads, 128), F32),
            V((rows, hw), BF),
            V((nt, rows, oc), BF),
            V((nt, rows, oc), BF),
            V((1, rows), F32),
            V((everyone, 1, rows), F32),
            D((18,)),
            D((8, n)),
            D((8, n)),
            D((nt,)),
            D((nt,)),
            D((everyone,)),
            D((everyone,)),
        ],
        compiler_params=pltpu.CompilerParams(
            collective_id=0, has_side_effects=True, vmem_limit_bytes=50 * 1024 * 1024
        ),
        name="layer",
    )(
        *[
            pltpu.with_memory_space_constraint(operand, pltpu.HBM)
            for operand in (
                tokens.reshape(rows, width),
                gain_pre.reshape(1, width),
                w_query,
                w_key,
                w_value,
                w_forget.T,
                b_forget,
                w_out,
                gain_post.reshape(1, oc),
                kc,
                vc,
                cum,
                lengths,
                accepted,
                parent,
            )
        ]
    )
    fresh = (num_seqs, prop, heads, hd)
    key_out, value_out, mixed, cum_new = pl.pallas_call(
        functools.partial(patch_kernel, n, prop),
        out_shape=(
            pltpu.HBM(key_cache.shape, BF),
            pltpu.HBM(value_cache.shape, BF),
            pltpu.HBM(mixed.shape, BF),
            pltpu.HBM(cum.shape, F32),
        ),
        in_specs=[vmem, vmem, vmem, vmem, vmem, vmem, smem, smem],
        out_specs=(hbm, hbm, hbm, hbm),
        scratch_shapes=[D((2,)), D((2, num_seqs)), D((2, num_seqs))],
        compiler_params=pltpu.CompilerParams(
            has_side_effects=True, vmem_limit_bytes=4 * 1024 * 1024
        ),
        name="patch",
    )(
        *[
            pltpu.with_memory_space_constraint(operand, V)
            for operand in (key_cache, value_cache, knew.reshape(fresh), vnew.reshape(fresh), mixed, cum_new)
        ],
        lengths,
        accepted,
    )
    cum_out = jnp.swapaxes(cum_new.reshape(num_seqs, heads, span), 1, 2)
    return (
        mixed.reshape(num_seqs, prop, oc),
        key_out.reshape(key_cache.shape),
        value_out.reshape(value_cache.shape),
        cum_out,
    )


def choose(mesh):
    n, nt = mesh.shape["kv"], mesh.shape["tp"]

    def body(*args):
        tokens, key_cache = args[0], args[9]
        num_seqs, prop = tokens.shape[:2]
        span, heads = key_cache.shape[1:3]
        fits = (
            num_seqs % n == 0
            and n >= 4
            and n & (n - 1) == 0
            and nt & (nt - 1) == 0
            and num_seqs % 4 == 0
            and (num_seqs // n) * heads * prop == 128
            and span == 128
            and num_seqs * heads <= 128
            and prop % 16 == 0
        )
        if fits:
            return fast_device(n, nt, *args)
        return per_device(*args)

    return body


def solution(mesh):
    return jax.shard_map(
        choose(mesh),
        mesh=mesh,
        in_specs=(
            P(),
            P(),
            P("kv", "tp"),
            P("kv", "tp"),
            P("kv", "tp"),
            P(),
            P(),
            P("tp", "kv"),
            P(("kv", "tp")),
            P(None, "kv", "tp", None),
            P(None, "kv", "tp", None),
            P(None, "kv", "tp"),
            P(),
            P(),
            P(),
        ),
        out_specs=(
            P(None, None, ("kv", "tp")),
            P(None, "kv", "tp", None),
            P(None, "kv", "tp", None),
            P(None, "kv", "tp"),
        ),
        check_vma=False,
    )
```

```python
import functools

import jax
import jax.numpy as jnp
from jax import lax
from jax.experimental import pallas as pl
from jax.experimental.pallas import tpu as pltpu
from jax.sharding import PartitionSpec as P

epsilon = 1e-06
floor_value = -1e30


def merged(part, axis, combine):
    gathered = jax.tree.map(lambda a: lax.all_gather(a, axis), part)

    def take(source):
        return jax.tree.map(lambda a: lax.dynamic_index_in_dim(a, source, 0, False), gathered)

    return lax.fori_loop(
        1, lax.axis_size(axis), lambda source, state: combine(state, take(source)), take(0)
    )


def ancestry(parent_ids, members):
    identity = jnp.eye(members, dtype=jnp.float32)
    parent_hot = (
        parent_ids[:, :, None] == jnp.arange(members, dtype=jnp.int32)[None, None, :]
    ).astype(jnp.float32)
    ancestors = jnp.minimum(identity[None] + parent_hot, 1.0)
    for sweep in range(max(1, (members - 1).bit_length())):
        ancestors = jnp.minimum(
            jnp.einsum("bij,bjk->bik", ancestors, ancestors, precision=lax.Precision.HIGHEST), 1.0
        )
    return ancestors


def combine_parts(first, second):
    new_max = jnp.maximum(first[0], second[0])
    first_scale = jnp.exp(first[0] - new_max)
    second_scale = jnp.exp(second[0] - new_max)
    return (
        new_max,
        first[1] * first_scale + second[1] * second_scale,
        first[2] * first_scale[..., None] + second[2] * second_scale[..., None],
        jnp.maximum(first[3], second[3]),
    )


def finish_rows(cache_max, cache_total, cache_values, last_rows, tree_max, tree_total, tree_values):
    shifted = cache_max + last_rows
    top = jnp.maximum(shifted, tree_max)
    cache_scale = jnp.exp(shifted - top)
    tree_scale = jnp.exp(tree_max - top)
    attended = (
        (cache_values * cache_scale[..., None] + tree_values * tree_scale[..., None])
        / (cache_total * cache_scale + tree_total * tree_scale)[..., None]
    ).astype(jnp.bfloat16)
    return attended.reshape(attended.shape[0], attended.shape[1] * attended.shape[2])


def per_device(
    tokens,
    gain_pre,
    w_query,
    w_key,
    w_value,
    w_forget,
    b_forget,
    w_out,
    gain_post,
    key_cache,
    value_cache,
    cum_cache,
    lengths,
    accepted,
    parent,
):
    num_seqs, proposals, model_width = tokens.shape
    kv_rank = lax.axis_index("kv")
    tp_rank = lax.axis_index("tp")
    span = key_cache.shape[1]
    heads_local = key_cache.shape[2]
    head_dim = key_cache.shape[3]
    scale = head_dim ** (-0.5)
    all_rows = num_seqs * proposals
    tok_float = tokens.astype(jnp.float32)
    normed = (
        tok_float
        * lax.rsqrt(jnp.mean(tok_float * tok_float, -1, keepdims=True) + epsilon)
        * gain_pre
    ).astype(jnp.bfloat16)
    flat = normed.reshape(all_rows, model_width)
    weight_rows = w_query.shape[0]
    local_rows = lax.dynamic_slice_in_dim(flat, kv_rank * weight_rows, weight_rows, 1)
    query_part = jnp.dot(local_rows, w_query, preferred_element_type=jnp.float32)
    key_part = jnp.dot(local_rows, w_key, preferred_element_type=jnp.float32)
    value_part = jnp.dot(local_rows, w_value, preferred_element_type=jnp.float32)
    summed = (
        lax.psum(query_part.astype(jnp.bfloat16), "kv").astype(jnp.float32),
        lax.psum(key_part.astype(jnp.bfloat16), "kv").astype(jnp.float32),
        lax.psum(value_part.astype(jnp.bfloat16), "kv").astype(jnp.float32),
    )
    query_flat = summed[0].astype(jnp.bfloat16)
    key_flat = summed[1].astype(jnp.bfloat16)
    value_flat = summed[2].astype(jnp.bfloat16)
    query = query_flat.reshape(num_seqs, proposals, heads_local, head_dim)
    key_new = key_flat.reshape(num_seqs, proposals, heads_local, head_dim)
    value_new = value_flat.reshape(num_seqs, proposals, heads_local, head_dim)
    forget_cols = lax.dynamic_slice_in_dim(w_forget, tp_rank * heads_local, heads_local, 1)
    forget_bias = lax.dynamic_slice_in_dim(b_forget, tp_rank * heads_local, heads_local, 0)
    log_forget = jax.nn.log_sigmoid(
        jnp.dot(flat, forget_cols, preferred_element_type=jnp.float32) + forget_bias
    ).reshape(num_seqs, proposals, heads_local)
    ancestors = ancestry(parent, proposals)
    path = jnp.einsum("bij,bjh->bih", ancestors, log_forget, precision=lax.Precision.HIGHEST)
    valid = lengths + accepted
    positions = kv_rank * span + jnp.arange(span, dtype=jnp.int32)
    live = (positions[None, :] < valid[:, None])[:, None, None, :]
    score = (
        jnp.einsum("bihd,bkhd->bihk", query, key_cache, preferred_element_type=jnp.float32) * scale
        + path[..., None]
        - jnp.swapaxes(cum_cache, 1, 2)[:, None]
    )
    block_max = jnp.max(jnp.where(live, score, floor_value), axis=-1)
    weight = jnp.exp(jnp.where(live, score - block_max[..., None], floor_value))
    block_total = jnp.sum(weight, axis=-1)
    block_values = jnp.einsum(
        "bihk,bkhd->bihd",
        weight.astype(jnp.bfloat16),
        value_cache,
        preferred_element_type=jnp.float32,
    )
    owner = positions[None, :] == (valid - 1)[:, None]
    candidate = jnp.max(jnp.where(owner[:, :, None], cum_cache, floor_value), axis=1)
    tree_mask = (ancestors > 0.5)[:, :, None, :]
    tree_score = (
        jnp.einsum("bihd,bjhd->bihj", query, key_new, preferred_element_type=jnp.float32) * scale
        + path[..., None]
        - jnp.swapaxes(path, 1, 2)[:, None]
    )
    tree_max = jnp.max(jnp.where(tree_mask, tree_score, floor_value), axis=-1)
    tree_weight = jnp.exp(jnp.where(tree_mask, tree_score - tree_max[..., None], floor_value))
    tree_total = jnp.sum(tree_weight, axis=-1)
    tree_values = jnp.einsum(
        "bihj,bjhd->bihd",
        tree_weight.astype(jnp.bfloat16),
        value_new,
        preferred_element_type=jnp.float32,
    )
    tree_max_rows = tree_max.reshape(all_rows, heads_local)
    tree_total_rows = tree_total.reshape(all_rows, heads_local)
    tree_values_rows = tree_values.reshape(all_rows, heads_local, head_dim)
    cache_max, cache_total, cache_values, last_cum = merged(
        (block_max, block_total, block_values, candidate), "kv", combine_parts
    )
    last_rows = jnp.broadcast_to(last_cum[:, None, :], (num_seqs, proposals, heads_local)).reshape(
        all_rows, heads_local
    )
    attended = finish_rows(
        cache_max.reshape(all_rows, heads_local),
        cache_total.reshape(all_rows, heads_local),
        cache_values.reshape(all_rows, heads_local, head_dim),
        last_rows,
        tree_max_rows,
        tree_total_rows,
        tree_values_rows,
    )
    mixed_part = jnp.dot(attended, w_out, preferred_element_type=jnp.float32)
    mixed_sum = lax.psum_scatter(
        mixed_part.astype(jnp.bfloat16), "tp", scatter_dimension=1, tiled=True
    ).astype(jnp.float32)
    squares = lax.psum(jnp.sum(mixed_sum * mixed_sum, axis=1), ("kv", "tp"))
    mixed = (mixed_sum * lax.rsqrt(squares / model_width + epsilon)[:, None] * gain_post).astype(
        jnp.bfloat16
    )
    mixed = mixed.reshape(num_seqs, proposals, mixed_sum.shape[1])
    relative = positions[None, :] - valid[:, None]
    select = relative[:, :, None] == jnp.arange(proposals, dtype=jnp.int32)[None, None, :]
    written = (relative >= 0) & (relative < proposals)
    placed_keys = jnp.einsum(
        "bkj,bjhd->bkhd", select.astype(jnp.bfloat16), key_new, preferred_element_type=jnp.float32
    ).astype(jnp.bfloat16)
    placed_values = jnp.einsum(
        "bkj,bjhd->bkhd", select.astype(jnp.bfloat16), value_new, preferred_element_type=jnp.float32
    ).astype(jnp.bfloat16)
    key_out = jnp.where(written[:, :, None, None], placed_keys, key_cache)
    value_out = jnp.where(written[:, :, None, None], placed_values, value_cache)
    cum_new = last_cum[:, None, :] + path
    placed_cum = jnp.einsum(
        "bkj,bjh->bkh", select.astype(jnp.float32), cum_new, precision=lax.Precision.HIGHEST
    )
    cum_out = jnp.where(written[:, :, None], placed_cum, cum_cache)
    return (mixed, key_out, value_out, cum_out)


MESH = pl.DeviceIdType.MESH
HI = lax.Precision.HIGHEST
F32 = jnp.float32
BF = jnp.bfloat16


def iota(shape, dim):
    return lax.broadcasted_iota(jnp.int32, shape, dim)


def hot(mask):
    return jnp.where(mask, 1.0, 0.0).astype(F32)


def dot_hi(a, b, dims=(((1,), (0,)), ((), ()))):
    return lax.dot_general(a, b, dims, precision=HI, preferred_element_type=F32)


NT = (((1,), (1,)), ((), ()))


def flips(value, count):
    bit = 1
    out = [value]
    while bit < count:
        step = bit * (1 - 2 * lax.rem(lax.div(value, bit), 2))
        out = out + [other + step for other in out]
        bit *= 2
    return out


def layer_kernel(
    n,
    nt,
    num_seqs,
    prop,
    heads,
    hd,
    span,
    tok_h,
    gain_h,
    wq_h,
    wk_h,
    wv_h,
    wft_h,
    bias_h,
    wo_h,
    gpost_h,
    kc_h,
    vc_h,
    cum_h,
    lens_h,
    accs_h,
    parent_h,
    mixed_out,
    cum_out,
    knew_out,
    vnew_out,
    tokv,
    gain,
    wqkv,
    wft,
    bias,
    wov,
    gpost,
    kcv,
    vcv,
    cum,
    lens,
    accs,
    parent,
    ssq,
    invv,
    xloc,
    part_q,
    q_recv,
    q_full,
    part_kv,
    kv_y,
    kv_zs,
    kv_zr,
    kv_full,
    st_send,
    val_send,
    st_recv,
    val_recv,
    cand_send,
    cand_recv,
    brow,
    anc,
    tpath,
    ptile,
    att,
    o_send,
    o_recv,
    sq_send,
    sq_recv,
    loc,
    ssem,
    rsem,
    tssem,
    trsem,
    qssem,
    qrsem,
):
    me = lax.axis_index("kv")
    mt = lax.axis_index("tp")
    rows, width = tokv.shape
    hw = heads * hd
    kdim = wq_h.shape[0]
    cols = heads * span
    sp = num_seqs // n
    R = sp * prop
    hp = heads * prop
    L = sp * hp
    scale = hd ** (-0.5)
    base = me * span
    heads_all = wft.shape[0]
    half = n // 2
    everyone = n * nt

    barrier = pltpu.get_barrier_semaphore()

    kvs = flips(me, n)
    tps = flips(mt, nt)

    chunks = 4
    crow = rows // chunks
    in_tok = [
        pltpu.make_async_copy(
            tok_h.at[pl.ds(i * crow, crow)], tokv.at[pl.ds(i * crow, crow)], loc.at[i]
        )
        for i in range(chunks)
    ]
    later = [
        (gain_h, gain),
        (wq_h, wqkv.at[0]),
        (wk_h, wqkv.at[1]),
        (wv_h, wqkv.at[2]),
        (wft_h, wft),
        (bias_h, bias),
        (lens_h, lens),
        (accs_h, accs),
        (parent_h, parent),
        (cum_h, cum),
        (gpost_h, gpost),
        (kc_h, kcv),
        (vc_h, vcv),
        (wo_h, wov),
    ]
    copies = [
        pltpu.make_async_copy(src, dst, loc.at[chunks + i]) for i, (src, dst) in enumerate(later)
    ]
    (
        in_gain,
        in_wq,
        in_wk,
        in_wv,
        in_wft,
        in_bias,
        in_lens,
        in_accs,
        in_parent,
        in_cum,
        in_gpost,
        in_kc,
        in_vc,
        in_wo,
    ) = copies
    for c in in_tok:
        c.start()
    for c in copies:
        c.start()
    for e in range(1, everyone):
        pl.semaphore_signal(
            barrier,
            inc=1,
            device_id={"kv": kvs[e // nt], "tp": tps[e % nt]},
            device_id_type=MESH,
        )

    def to_kv(ph, slot, mask, src, dst):
        return pltpu.make_async_remote_copy(
            src_ref=src,
            dst_ref=dst,
            send_sem=ssem.at[ph, slot],
            recv_sem=rsem.at[ph, slot],
            device_id={"kv": kvs[mask]},
            device_id_type=MESH,
        )

    def rrow(i):
        return pl.ds(pl.multiple_of(i * R, R), R)

    def q_rs(m):
        return to_kv(0, m, m, part_q.at[rrow(kvs[m])], q_recv.at[m])

    def q_ag(m):
        return to_kv(1, m, m, q_full.at[rrow(me)], q_full.at[rrow(me)])

    def kv_yrs(m):
        return to_kv(2, m, 1, part_kv.at[rrow(kvs[m + 1])], kv_y.at[m // 2])

    def kv_zrs(m):
        return to_kv(2, m + 1, m, kv_zs.at[m // 2], kv_zr.at[m // 2])

    def cand_copy(m):
        return to_kv(3, m, m, cand_send, cand_recv.at[m])

    def stat_copy(m):
        return to_kv(4, m, m, st_send.at[m], st_recv.at[m])

    def val_copy(m):
        return to_kv(5, m, m, val_send.at[m], val_recv.at[m])

    def att_copy(m):
        return to_kv(6, m, m, att.at[rrow(me)], att.at[rrow(me)])

    def kv_zag(m):
        return to_kv(7, m, m, kv_full.at[rrow(me)], kv_full.at[rrow(me)])

    def kv_yag(m):
        return to_kv(7, m + 1, 1, kv_full.at[rrow(kvs[m])], kv_full.at[rrow(kvs[m])])

    def each(count, fn):
        for d in range(1, count):
            fn(d)

    def each_far(count, fn):
        for d in range(count - 1, 0, -1):
            fn(d)

    zmasks = list(range(2, n, 2))
    nb = prop
    lanes = 128

    def sum_rows(i, c):
        sl = pl.ds(pl.multiple_of(i * nb, nb), nb)
        accs4 = [None] * 4
        for j in range(width // lanes):
            t = tokv[sl, j * lanes : (j + 1) * lanes].astype(F32)
            p = t * t
            accs4[j % 4] = p if accs4[j % 4] is None else accs4[j % 4] + p
        ssq[sl, :] = (accs4[0] + accs4[1]) + (accs4[2] + accs4[3])
        return c

    for i in range(chunks):
        in_tok[i].wait()
        lax.fori_loop(i * crow // nb, (i + 1) * crow // nb, sum_rows, 0)
    total = dot_hi(ssq[...], jnp.ones((lanes, lanes), F32))
    inv = lax.rsqrt(total / width + epsilon)
    invv[...] = inv
    in_gain.wait()
    for j in range(kdim // lanes):
        at = pl.ds(pl.multiple_of(me * kdim + j * lanes, lanes), lanes)
        xloc[:, j * lanes : (j + 1) * lanes] = (
            tokv[:, at].astype(F32) * inv * gain[:, at]
        ).astype(BF)
    in_wq.wait()
    part_q[...] = jnp.dot(xloc[...], wqkv[0], preferred_element_type=F32).astype(BF)
    pl.semaphore_wait(barrier, everyone - 1)
    each_far(n, lambda m: q_rs(m).start())
    in_wk.wait()
    in_wv.wait()
    part_kv[:, 0:hw] = jnp.dot(xloc[...], wqkv[1], preferred_element_type=F32).astype(BF)
    part_kv[:, hw : 2 * hw] = jnp.dot(xloc[...], wqkv[2], preferred_element_type=F32).astype(BF)
    for m in zmasks[::-1] + [0]:
        kv_yrs(m).start()

    in_lens.wait()
    in_accs.wait()
    in_cum.wait()
    r64 = num_seqs * heads
    c64 = cum[...]
    srow = iota((r64, span), 0) // heads
    lane = iota((r64, span), 1)
    rel64 = jnp.zeros((r64, span), jnp.int32)
    rel16 = jnp.zeros((num_seqs, cols), jnp.int32)
    s16 = iota((num_seqs, cols), 0)
    for s in range(num_seqs):
        rel_s = lens[s] + accs[s] - base
        rel64 = jnp.where(srow == s, rel_s, rel64)
        rel16 = jnp.where(s16 == s, rel_s, rel16)
    cand = jnp.max(jnp.where(lane == rel64 - 1, c64, floor_value), axis=1, keepdims=True)
    diag = iota((r64, 128), 0) == iota((r64, 128), 1)
    cand_send[...] = jnp.sum(jnp.where(diag, cand, 0.0), axis=0, keepdims=True)
    each_far(n, lambda m: cand_copy(m).start())

    spread = hot(iota((span, cols), 1) // heads == iota((span, cols), 0))
    e1 = dot_hi(c64, spread)
    e1 = jnp.where(iota((r64, cols), 0) % heads == iota((r64, cols), 1) % heads, e1, 0.0)
    take = hot(iota((num_seqs, r64), 1) // heads == iota((num_seqs, r64), 0))
    cflat = dot_hi(take, e1)
    brow[...] = jnp.where(iota((num_seqs, cols), 1) // heads < rel16, -cflat, floor_value)

    in_parent.wait()
    ri = iota((rows, rows), 0)
    ci = iota((rows, rows), 1)
    pick = hot(iota((rows, num_seqs), 0) // prop == iota((rows, num_seqs), 1))
    pb = dot_hi(pick, parent[...].astype(F32))
    pcol = jnp.sum(
        jnp.where(iota((rows, prop), 1) == iota((rows, prop), 0) % prop, pb, 0.0),
        axis=1,
        keepdims=True,
    )
    target = jnp.where(pcol >= 0.0, (ri // prop * prop).astype(F32) + pcol, -1.0)
    a = jnp.where((ri == ci) | (ci.astype(F32) == target), 1.0, 0.0)
    for sweep in range(max(1, (prop - 1).bit_length())):
        low = a.astype(BF)
        a = jnp.minimum(jnp.dot(low, low, preferred_element_type=F32), 1.0)
    anc[...] = a
    in_wft.wait()
    in_bias.wait()
    wscaled = wft[...].astype(F32) * gain[...]
    whigh = wscaled.astype(BF)
    wlow = (wscaled - whigh.astype(F32)).astype(BF)
    lf = lax.dot_general(
        jnp.concatenate([whigh, wlow], axis=0), tokv[...], NT, preferred_element_type=F32
    )
    lf = lf[0:heads_all] + lf[heads_all : 2 * heads_all]
    inv_lane = dot_hi(jnp.full((8, lanes), 1.0 / lanes, F32), invv[...], NT)[0:1]
    bcol = jnp.zeros((heads_all, rows), F32)
    for h in range(heads_all):
        bcol = jnp.where(iota((heads_all, rows), 0) == h, bias[h], bcol)
    z = lf * inv_lane + bcol
    lf = jnp.minimum(z, 0.0) - jnp.log1p(jnp.exp(-jnp.abs(z)))
    path_t = dot_hi(lf, a, NT)
    rep = hot(iota((r64, heads_all), 1) == mt * heads + iota((r64, heads_all), 0) % heads)
    pm = dot_hi(rep, path_t)
    pm = jnp.where(iota((r64, rows), 1) // prop == iota((r64, rows), 0) // heads, pm, 0.0)
    fold = hot(iota((rows, 128), 0) % prop == iota((rows, 128), 1) % prop)
    pt = dot_hi(pm, fold)
    ptile[...] = pt
    ptm = jnp.where((iota((r64, 128), 1) // prop) % heads == iota((r64, 128), 0) % heads, pt, 0.0)
    tpath[...] = dot_hi(take, ptm)
    in_kc.wait()
    in_vc.wait()

    own = part_q[rrow(me)].astype(F32)
    for m in range(1, n):
        q_rs(m).wait_recv()
        own = own + q_recv[m].astype(F32)
    q_full[rrow(me)] = own.astype(BF)
    each_far(n, lambda m: q_ag(m).start())

    for m in zmasks[::-1]:
        kv_yrs(m).wait_recv()
        kv_zs[m // 2] = (
            part_kv[rrow(kvs[m])].astype(F32) + kv_y[m // 2].astype(F32)
        ).astype(BF)
        kv_zrs(m).start()

    same_head = iota((hp, cols), 0) // prop == iota((hp, cols), 1) % heads
    diag_l = iota((L, L), 0) == iota((L, L), 1)

    def heads_of(ref, s, first):
        block = ref[pl.ds(pl.multiple_of(s * prop, prop), prop), first : first + hw]
        return jnp.concatenate([block[:, h * hd : (h + 1) * hd] for h in range(heads)], axis=0)

    def block_part(src):
        maxes, totals, values = [], [], []
        for j in range(sp):
            s = src * sp + j
            q = heads_of(q_full, s, 0)
            sc = lax.dot_general(q, kcv[s], NT, preferred_element_type=F32) * scale
            sc = jnp.where(same_head, sc + brow[pl.ds(s, 1), :], floor_value)
            m = jnp.max(sc, axis=1, keepdims=True)
            w = jnp.exp(sc - m)
            maxes.append(m)
            totals.append(jnp.sum(w, axis=1, keepdims=True))
            values.append(
                jnp.dot(w.astype(BF), vcv[s], preferred_element_type=F32).astype(BF)
            )
        m = jnp.concatenate(maxes, axis=0)
        t = jnp.concatenate(totals, axis=0)
        m_lane = jnp.sum(jnp.where(diag_l, m, 0.0), axis=0, keepdims=True)
        t_lane = jnp.sum(jnp.where(diag_l, t, 0.0), axis=0, keepdims=True)
        stats = jnp.where(iota((2, L), 0) == 0, m_lane, t_lane)
        return stats, jnp.concatenate(values, axis=0)

    def remote_blocks(masks):
        for m in masks:
            q_ag(m).wait_recv()
        parts = [block_part(kvs[m]) for m in masks]
        for m, (stats, values) in zip(masks, parts):
            st_send[m] = stats
            val_send[m] = values
        for m in masks:
            stat_copy(m).start()
            val_copy(m).start()

    stats, values = block_part(me)
    st_recv[0] = stats
    val_recv[0] = values
    remote_blocks([1])
    for m in zmasks:
        remote_blocks([m, m + 1])

    kv_yrs(0).wait_recv()
    own = part_kv[rrow(me)].astype(F32) + kv_y[0].astype(F32)
    for m in zmasks:
        kv_zrs(m).wait_recv()
        own = own + kv_zr[m // 2].astype(F32)
    kv_full[rrow(me)] = own.astype(BF)

    fold_h = iota((rows, hp), 0)
    tmax, ttot, tval = [], [], []
    for j in range(sp):
        s = me * sp + j
        q = heads_of(q_full, s, 0)
        k = heads_of(kv_full, s, 0)
        v = heads_of(kv_full, s, hw)
        arows = anc[pl.ds(pl.multiple_of(s * prop, prop), prop), :]
        sel = hot(fold_h == s * prop + iota((rows, hp), 1) % prop).astype(BF)
        am = jnp.dot(arows.astype(BF), sel, preferred_element_type=F32)
        am = jnp.concatenate([am] * heads, axis=0)
        mask = (am > 0.5) & (iota((hp, hp), 0) // prop == iota((hp, hp), 1) // prop)
        sc = lax.dot_general(q, k, NT, preferred_element_type=F32) * scale
        sc = jnp.where(mask, sc - tpath[pl.ds(s, 1), 0:hp], floor_value)
        m = jnp.max(sc, axis=1, keepdims=True)
        w = jnp.where(mask, jnp.exp(sc - m), 0.0)
        tmax.append(m)
        ttot.append(jnp.sum(w, axis=1, keepdims=True))
        tval.append(jnp.dot(w.astype(BF), v, preferred_element_type=F32))
    tree_max = jnp.concatenate(tmax, axis=0)
    tree_tot = jnp.concatenate(ttot, axis=0)
    tree_val = jnp.concatenate(tval, axis=0)

    last_lane = cand_send[...]
    for m in range(1, n):
        cand_copy(m).wait_recv()
        last_lane = jnp.maximum(last_lane, cand_recv[m])
    own_rows = iota((L, 128), 0)
    own_pick = iota((L, 128), 1) == (me * sp + own_rows // hp) * heads + (own_rows % hp) // prop
    last_own = jnp.sum(jnp.where(own_pick, last_lane, 0.0), axis=1, keepdims=True)

    for m in range(1, n):
        stat_copy(m).wait_recv()
    top = st_recv[0, 0:1]
    for m in range(1, n):
        top = jnp.maximum(top, st_recv[m, 0:1])

    def col(x):
        return jnp.sum(jnp.where(diag_l, x, 0.0), axis=1, keepdims=True)

    cache_tot = jnp.zeros((1, L), F32)
    scales = []
    for m in range(n):
        sd = jnp.exp(st_recv[m, 0:1] - top)
        scales.append(col(sd))
        cache_tot = cache_tot + st_recv[m, 1:2] * sd
    shifted = col(top) + last_own
    both = jnp.maximum(shifted, tree_max)
    cscale = jnp.exp(shifted - both)
    tscale = jnp.exp(tree_max - both)
    denom = col(cache_tot) * cscale + tree_tot * tscale
    vals = val_recv[0].astype(F32) * scales[0]
    for m in range(1, n):
        val_copy(m).wait_recv()
        vals = vals + val_recv[m].astype(F32) * scales[m]
    attended = ((vals * cscale + tree_val * tscale) / denom).astype(BF)
    for j in range(sp):
        for h in range(heads):
            att[pl.ds(pl.multiple_of(me * R + j * prop, prop), prop), h * hd : (h + 1) * hd] = (
                attended[j * hp + h * prop : j * hp + (h + 1) * prop]
            )
    each_far(n, lambda m: att_copy(m).start())

    upper = me >= half

    @pl.when(upper)
    def _():
        for m in [z for z in zmasks if z < half]:
            kv_zag(m).start()
        kv_yag(0).start()

    @pl.when(jnp.logical_not(upper))
    def _():
        for m in [z for z in zmasks if z >= half]:
            kv_zag(m).start()

    last_col = jnp.sum(jnp.where(diag, last_lane, 0.0), axis=1, keepdims=True)
    shifted_path = ptile[...]
    for b in range((span - 1).bit_length()):
        moved = pltpu.roll(shifted_path, 1 << b, 1)
        shifted_path = jnp.where((rel64 >> b) & 1 == 1, moved, shifted_path)
    off = lane - rel64
    cum_out[...] = jnp.where((off >= 0) & (off < prop), last_col + shifted_path, c64)

    in_wo.wait()
    oc = o_send.shape[2]
    near = lax.div(me, half) * (half * R)
    grows = [
        pl.ds(pl.multiple_of(first, half * R), half * R) for first in (near, half * R - near)
    ]

    def o_copy(g, d):
        return pltpu.make_async_remote_copy(
            src_ref=o_send.at[tps[d], grows[g]],
            dst_ref=o_recv.at[d, grows[g]],
            send_sem=tssem.at[g, d],
            recv_sem=trsem.at[g, d],
            device_id={"tp": tps[d]},
            device_id_type=MESH,
        )

    for g in range(2):
        for m in range(max(1, g * half), (g + 1) * half):
            to_kv(6, m, m, att.at[rrow(me)], att.at[rrow(kvs[m])]).wait_recv()
        full = jnp.dot(att[grows[g]], wov[...], preferred_element_type=F32).astype(BF)
        for t in range(nt):
            o_send[t, grows[g]] = full[:, t * oc : (t + 1) * oc]
        each_far(nt, lambda d: o_copy(g, d).start())

    @pl.when(upper)
    def _():
        for m in zmasks:
            to_kv(7, m, m, kv_full.at[rrow(me)], kv_full.at[rrow(kvs[m])]).wait_recv()
            kv_yag(m).start()

    mixed = o_send[mt].astype(F32)
    for d in range(1, nt):
        o_copy(0, d).wait_recv()
        o_copy(1, d).wait_recv()
        mixed = mixed + o_recv[d].astype(F32)
    sq = dot_hi(jnp.ones((8, oc), F32), mixed * mixed, NT)[0:1]
    sq_send[...] = sq

    def sq_copy(e):
        return pltpu.make_async_remote_copy(
            src_ref=sq_send,
            dst_ref=sq_recv.at[e],
            send_sem=qssem.at[e],
            recv_sem=qrsem.at[e],
            device_id={"kv": kvs[e // nt], "tp": tps[e % nt]},
            device_id_type=MESH,
        )

    each_far(everyone, lambda e: sq_copy(e).start())

    order = hot(
        iota((hp, hp), 1) == iota((hp, hp), 0) % heads * prop + iota((hp, hp), 0) // heads
    ).astype(BF)

    unroll = 4

    @pl.when(upper)
    def _():
        for m in [0] + zmasks:
            to_kv(
                7, m + 1, 1, kv_full.at[rrow(me)], kv_full.at[rrow(kvs[m + 1])]
            ).wait_recv()

        def some(i, c):
            fresh = [
                heads_of(kv_full, i * unroll + j, first) for j in range(unroll) for first in (0, hw)
            ]
            placed = jnp.dot(
                order, jnp.concatenate(fresh, axis=1), preferred_element_type=F32
            ).astype(BF)
            for j in range(unroll):
                at = 2 * j * hd
                knew_out[i * unroll + j] = placed[:, at : at + hd]
                vnew_out[i * unroll + j] = placed[:, at + hd : at + 2 * hd]
            return c

        lax.fori_loop(0, num_seqs // unroll, some, 0)

    for e in range(1, everyone):
        sq_copy(e).wait_recv()
        sq = sq + sq_recv[e]
    ssum = dot_hi(
        jnp.broadcast_to(sq, (8, rows)), jnp.full((8, oc), 0.125, F32), (((0,), (0,)), ((), ()))
    )
    in_gpost.wait()
    mixed_out[...] = (mixed * lax.rsqrt(ssum / width + epsilon) * gpost[...]).astype(BF)

    def drain(m):
        q_rs(m).wait_send()
        q_ag(m).wait_send()
        cand_copy(m).wait_send()
        stat_copy(m).wait_send()
        val_copy(m).wait_send()
        att_copy(m).wait_send()

    each(n, drain)
    for m in [0] + zmasks:
        kv_yrs(m).wait_send()
    for m in zmasks:
        kv_zrs(m).wait_send()

    @pl.when(upper)
    def _():
        for m in [z for z in zmasks if z < half]:
            kv_zag(m).wait_send()
        for m in [0] + zmasks:
            kv_yag(m).wait_send()

    @pl.when(jnp.logical_not(upper))
    def _():
        for m in [z for z in zmasks if z >= half]:
            kv_zag(m).wait_send()

    for g in range(2):
        each(nt, lambda d: o_copy(g, d).wait_send())
    each(everyone, lambda e: sq_copy(e).wait_send())


def patch_kernel(
    n, prop, kc, vc, knew, vnew, mixed, cum, lens, accs, k_out, v_out, mixed_out, cum_out, sem, bsem, wsem
):
    me = lax.axis_index("kv")
    num_seqs, span = k_out.shape[:2]
    out_m = pltpu.make_async_copy(mixed, mixed_out, sem.at[0])
    out_c = pltpu.make_async_copy(cum, cum_out, sem.at[1])
    bulk = [
        [
            pltpu.make_async_copy(src.at[s], dst.at[s], bsem.at[i, s])
            for i, (src, dst) in enumerate(((kc, k_out), (vc, v_out)))
        ]
        for s in range(num_seqs)
    ]
    for row in bulk:
        for c in row:
            c.start()
    out_m.start()
    out_c.start()

    def moves(act, before=None):
        for s in range(num_seqs):
            if before is not None:
                before(s)
            at = lens[s] + accs[s] - me * span
            pairs = ((knew, k_out), (vnew, v_out))

            @pl.when((at >= 0) & (at <= span - prop))
            def _():
                for i, (src, dst) in enumerate(pairs):
                    act(
                        pltpu.make_async_copy(
                            src.at[s], dst.at[s, pl.ds(at, prop)], wsem.at[i, s]
                        )
                    )

            @pl.when(((at > -prop) & (at < 0)) | ((at > span - prop) & (at < span)))
            def _():
                def one(j, c):
                    @pl.when((at + j >= 0) & (at + j < span))
                    def _():
                        for i, (src, dst) in enumerate(pairs):
                            act(
                                pltpu.make_async_copy(
                                    src.at[s, j], dst.at[s, at + j], wsem.at[i, s]
                                )
                            )

                    return c

                lax.fori_loop(0, prop, one, 0)

    def settle(s):
        for c in bulk[s]:
            c.wait()

    @pl.when(me >= n // 2)
    def _():
        moves(lambda c: c.start(), settle)
        moves(lambda c: c.wait())

    @pl.when(me < n // 2)
    def _():
        for s in range(num_seqs):
            settle(s)

    out_m.wait()
    out_c.wait()


def fast_device(
    n,
    nt,
    tokens,
    gain_pre,
    w_query,
    w_key,
    w_value,
    w_forget,
    b_forget,
    w_out,
    gain_post,
    key_cache,
    value_cache,
    cum_cache,
    lengths,
    accepted,
    parent,
):
    num_seqs, prop, width = tokens.shape
    span, heads, hd = key_cache.shape[1:]
    rows = num_seqs * prop
    hw = heads * hd
    cols = heads * span
    sp = num_seqs // n
    R = sp * prop
    L = sp * heads * prop
    oc = gain_post.shape[0]
    half = n // 2
    everyone = n * nt
    kc = key_cache.reshape(num_seqs, cols, hd)
    vc = value_cache.reshape(num_seqs, cols, hd)
    cum = jnp.swapaxes(cum_cache, 1, 2).reshape(num_seqs * heads, span)
    hbm = pl.BlockSpec(memory_space=pltpu.HBM)
    vmem = pl.BlockSpec(memory_space=pltpu.VMEM)
    smem = pl.BlockSpec(memory_space=pltpu.SMEM)
    V = pltpu.VMEM
    S = pltpu.SMEM
    D = pltpu.SemaphoreType.DMA
    mixed, cum_new, knew, vnew = pl.pallas_call(
        functools.partial(layer_kernel, n, nt, num_seqs, prop, heads, hd, span),
        out_shape=(
            V((rows, oc), BF),
            V(cum.shape, F32),
            V((num_seqs, heads * prop, hd), BF),
            V((num_seqs, heads * prop, hd), BF),
        ),
        in_specs=[hbm] * 15,
        out_specs=(vmem, vmem, vmem, vmem),
        scratch_shapes=[
            V((rows, width), BF),
            V((1, width), F32),
            V((3,) + w_query.shape, BF),
            V(w_forget.shape[::-1], BF),
            S(b_forget.shape, F32),
            V(w_out.shape, BF),
            V((1, oc), F32),
            V(kc.shape, BF),
            V(vc.shape, BF),
            V(cum.shape, F32),
            S(lengths.shape, jnp.int32),
            S(accepted.shape, jnp.int32),
            V(parent.shape, jnp.int32),
            V((rows, 128), F32),
            V((rows, 128), F32),
            V((rows, w_query.shape[0]), BF),
            V((rows, hw), BF),
            V((n, R, hw), BF),
            V((rows, hw), BF),
            V((rows, 2 * hw), BF),
            V((half, R, 2 * hw), BF),
            V((half, R, 2 * hw), BF),
            V((half, R, 2 * hw), BF),
            V((rows, 2 * hw), BF),
            V((n, 2, L), F32),
            V((n, L, hd), BF),
            V((n, 2, L), F32),
            V((n, L, hd), BF),
            V((1, 128), F32),
            V((n, 1, 128), F32),
            V((num_seqs, cols), F32),
            V((rows, rows), F32),
            V((num_seqs, 128), F32),
            V((num_seqs * heads, 128), F32),
            V((rows, hw), BF),
            V((nt, rows, oc), BF),
            V((nt, rows, oc), BF),
            V((1, rows), F32),
            V((everyone, 1, rows), F32),
            D((18,)),
            D((8, n)),
            D((8, n)),
            D((2, nt)),
            D((2, nt)),
            D((everyone,)),
            D((everyone,)),
        ],
        compiler_params=pltpu.CompilerParams(
            collective_id=0, has_side_effects=True, vmem_limit_bytes=50 * 1024 * 1024
        ),
        name="layer",
    )(
        *[
            pltpu.with_memory_space_constraint(operand, pltpu.HBM)
            for operand in (
                tokens.reshape(rows, width),
                gain_pre.reshape(1, width),
                w_query,
                w_key,
                w_value,
                w_forget.T,
                b_forget,
                w_out,
                gain_post.reshape(1, oc),
                kc,
                vc,
                cum,
                lengths,
                accepted,
                parent,
            )
        ]
    )
    fresh = (num_seqs, prop, heads, hd)
    key_out, value_out, mixed, cum_new = pl.pallas_call(
        functools.partial(patch_kernel, n, prop),
        out_shape=(
            pltpu.HBM(key_cache.shape, BF),
            pltpu.HBM(value_cache.shape, BF),
            pltpu.HBM(mixed.shape, BF),
            pltpu.HBM(cum.shape, F32),
        ),
        in_specs=[vmem, vmem, vmem, vmem, vmem, vmem, smem, smem],
        out_specs=(hbm, hbm, hbm, hbm),
        scratch_shapes=[D((2,)), D((2, num_seqs)), D((2, num_seqs))],
        compiler_params=pltpu.CompilerParams(
            has_side_effects=True, vmem_limit_bytes=4 * 1024 * 1024
        ),
        name="patch",
    )(
        *[
            pltpu.with_memory_space_constraint(operand, V)
            for operand in (key_cache, value_cache, knew.reshape(fresh), vnew.reshape(fresh), mixed, cum_new)
        ],
        lengths,
        accepted,
    )
    cum_out = jnp.swapaxes(cum_new.reshape(num_seqs, heads, span), 1, 2)
    return (
        mixed.reshape(num_seqs, prop, oc),
        key_out.reshape(key_cache.shape),
        value_out.reshape(value_cache.shape),
        cum_out,
    )


def choose(mesh):
    n, nt = mesh.shape["kv"], mesh.shape["tp"]

    def body(*args):
        tokens, key_cache = args[0], args[9]
        num_seqs, prop = tokens.shape[:2]
        span, heads = key_cache.shape[1:3]
        fits = (
            num_seqs % n == 0
            and n >= 4
            and n & (n - 1) == 0
            and nt & (nt - 1) == 0
            and num_seqs % 4 == 0
            and (num_seqs // n) * heads * prop == 128
            and span == 128
            and num_seqs * heads <= 128
            and prop % 16 == 0
        )
        if fits:
            return fast_device(n, nt, *args)
        return per_device(*args)

    return body


def solution(mesh):
    return jax.shard_map(
        choose(mesh),
        mesh=mesh,
        in_specs=(
            P(),
            P(),
            P("kv", "tp"),
            P("kv", "tp"),
            P("kv", "tp"),
            P(),
            P(),
            P("tp", "kv"),
            P(("kv", "tp")),
            P(None, "kv", "tp", None),
            P(None, "kv", "tp", None),
            P(None, "kv", "tp"),
            P(),
            P(),
            P(),
        ),
        out_specs=(
            P(None, None, ("kv", "tp")),
            P(None, "kv", "tp", None),
            P(None, "kv", "tp", None),
            P(None, "kv", "tp"),
        ),
        check_vma=False,
    )
```

```python
import functools

import jax
import jax.numpy as jnp
from jax import lax
from jax.experimental import pallas as pl
from jax.experimental.pallas import tpu as pltpu
from jax.sharding import PartitionSpec as P

epsilon = 1e-06
floor_value = -1e30


def merged(part, axis, combine):
    gathered = jax.tree.map(lambda a: lax.all_gather(a, axis), part)

    def take(source):
        return jax.tree.map(lambda a: lax.dynamic_index_in_dim(a, source, 0, False), gathered)

    return lax.fori_loop(
        1, lax.axis_size(axis), lambda source, state: combine(state, take(source)), take(0)
    )


def ancestry(parent_ids, members):
    identity = jnp.eye(members, dtype=jnp.float32)
    parent_hot = (
        parent_ids[:, :, None] == jnp.arange(members, dtype=jnp.int32)[None, None, :]
    ).astype(jnp.float32)
    ancestors = jnp.minimum(identity[None] + parent_hot, 1.0)
    for sweep in range(max(1, (members - 1).bit_length())):
        ancestors = jnp.minimum(
            jnp.einsum("bij,bjk->bik", ancestors, ancestors, precision=lax.Precision.HIGHEST), 1.0
        )
    return ancestors


def combine_parts(first, second):
    new_max = jnp.maximum(first[0], second[0])
    first_scale = jnp.exp(first[0] - new_max)
    second_scale = jnp.exp(second[0] - new_max)
    return (
        new_max,
        first[1] * first_scale + second[1] * second_scale,
        first[2] * first_scale[..., None] + second[2] * second_scale[..., None],
        jnp.maximum(first[3], second[3]),
    )


def finish_rows(cache_max, cache_total, cache_values, last_rows, tree_max, tree_total, tree_values):
    shifted = cache_max + last_rows
    top = jnp.maximum(shifted, tree_max)
    cache_scale = jnp.exp(shifted - top)
    tree_scale = jnp.exp(tree_max - top)
    attended = (
        (cache_values * cache_scale[..., None] + tree_values * tree_scale[..., None])
        / (cache_total * cache_scale + tree_total * tree_scale)[..., None]
    ).astype(jnp.bfloat16)
    return attended.reshape(attended.shape[0], attended.shape[1] * attended.shape[2])


def per_device(
    tokens,
    gain_pre,
    w_query,
    w_key,
    w_value,
    w_forget,
    b_forget,
    w_out,
    gain_post,
    key_cache,
    value_cache,
    cum_cache,
    lengths,
    accepted,
    parent,
):
    num_seqs, proposals, model_width = tokens.shape
    kv_rank = lax.axis_index("kv")
    tp_rank = lax.axis_index("tp")
    span = key_cache.shape[1]
    heads_local = key_cache.shape[2]
    head_dim = key_cache.shape[3]
    scale = head_dim ** (-0.5)
    all_rows = num_seqs * proposals
    tok_float = tokens.astype(jnp.float32)
    normed = (
        tok_float
        * lax.rsqrt(jnp.mean(tok_float * tok_float, -1, keepdims=True) + epsilon)
        * gain_pre
    ).astype(jnp.bfloat16)
    flat = normed.reshape(all_rows, model_width)
    weight_rows = w_query.shape[0]
    local_rows = lax.dynamic_slice_in_dim(flat, kv_rank * weight_rows, weight_rows, 1)
    query_part = jnp.dot(local_rows, w_query, preferred_element_type=jnp.float32)
    key_part = jnp.dot(local_rows, w_key, preferred_element_type=jnp.float32)
    value_part = jnp.dot(local_rows, w_value, preferred_element_type=jnp.float32)
    summed = (
        lax.psum(query_part.astype(jnp.bfloat16), "kv").astype(jnp.float32),
        lax.psum(key_part.astype(jnp.bfloat16), "kv").astype(jnp.float32),
        lax.psum(value_part.astype(jnp.bfloat16), "kv").astype(jnp.float32),
    )
    query_flat = summed[0].astype(jnp.bfloat16)
    key_flat = summed[1].astype(jnp.bfloat16)
    value_flat = summed[2].astype(jnp.bfloat16)
    query = query_flat.reshape(num_seqs, proposals, heads_local, head_dim)
    key_new = key_flat.reshape(num_seqs, proposals, heads_local, head_dim)
    value_new = value_flat.reshape(num_seqs, proposals, heads_local, head_dim)
    forget_cols = lax.dynamic_slice_in_dim(w_forget, tp_rank * heads_local, heads_local, 1)
    forget_bias = lax.dynamic_slice_in_dim(b_forget, tp_rank * heads_local, heads_local, 0)
    log_forget = jax.nn.log_sigmoid(
        jnp.dot(flat, forget_cols, preferred_element_type=jnp.float32) + forget_bias
    ).reshape(num_seqs, proposals, heads_local)
    ancestors = ancestry(parent, proposals)
    path = jnp.einsum("bij,bjh->bih", ancestors, log_forget, precision=lax.Precision.HIGHEST)
    valid = lengths + accepted
    positions = kv_rank * span + jnp.arange(span, dtype=jnp.int32)
    live = (positions[None, :] < valid[:, None])[:, None, None, :]
    score = (
        jnp.einsum("bihd,bkhd->bihk", query, key_cache, preferred_element_type=jnp.float32) * scale
        + path[..., None]
        - jnp.swapaxes(cum_cache, 1, 2)[:, None]
    )
    block_max = jnp.max(jnp.where(live, score, floor_value), axis=-1)
    weight = jnp.exp(jnp.where(live, score - block_max[..., None], floor_value))
    block_total = jnp.sum(weight, axis=-1)
    block_values = jnp.einsum(
        "bihk,bkhd->bihd",
        weight.astype(jnp.bfloat16),
        value_cache,
        preferred_element_type=jnp.float32,
    )
    owner = positions[None, :] == (valid - 1)[:, None]
    candidate = jnp.max(jnp.where(owner[:, :, None], cum_cache, floor_value), axis=1)
    tree_mask = (ancestors > 0.5)[:, :, None, :]
    tree_score = (
        jnp.einsum("bihd,bjhd->bihj", query, key_new, preferred_element_type=jnp.float32) * scale
        + path[..., None]
        - jnp.swapaxes(path, 1, 2)[:, None]
    )
    tree_max = jnp.max(jnp.where(tree_mask, tree_score, floor_value), axis=-1)
    tree_weight = jnp.exp(jnp.where(tree_mask, tree_score - tree_max[..., None], floor_value))
    tree_total = jnp.sum(tree_weight, axis=-1)
    tree_values = jnp.einsum(
        "bihj,bjhd->bihd",
        tree_weight.astype(jnp.bfloat16),
        value_new,
        preferred_element_type=jnp.float32,
    )
    tree_max_rows = tree_max.reshape(all_rows, heads_local)
    tree_total_rows = tree_total.reshape(all_rows, heads_local)
    tree_values_rows = tree_values.reshape(all_rows, heads_local, head_dim)
    cache_max, cache_total, cache_values, last_cum = merged(
        (block_max, block_total, block_values, candidate), "kv", combine_parts
    )
    last_rows = jnp.broadcast_to(last_cum[:, None, :], (num_seqs, proposals, heads_local)).reshape(
        all_rows, heads_local
    )
    attended = finish_rows(
        cache_max.reshape(all_rows, heads_local),
        cache_total.reshape(all_rows, heads_local),
        cache_values.reshape(all_rows, heads_local, head_dim),
        last_rows,
        tree_max_rows,
        tree_total_rows,
        tree_values_rows,
    )
    mixed_part = jnp.dot(attended, w_out, preferred_element_type=jnp.float32)
    mixed_sum = lax.psum_scatter(
        mixed_part.astype(jnp.bfloat16), "tp", scatter_dimension=1, tiled=True
    ).astype(jnp.float32)
    squares = lax.psum(jnp.sum(mixed_sum * mixed_sum, axis=1), ("kv", "tp"))
    mixed = (mixed_sum * lax.rsqrt(squares / model_width + epsilon)[:, None] * gain_post).astype(
        jnp.bfloat16
    )
    mixed = mixed.reshape(num_seqs, proposals, mixed_sum.shape[1])
    relative = positions[None, :] - valid[:, None]
    select = relative[:, :, None] == jnp.arange(proposals, dtype=jnp.int32)[None, None, :]
    written = (relative >= 0) & (relative < proposals)
    placed_keys = jnp.einsum(
        "bkj,bjhd->bkhd", select.astype(jnp.bfloat16), key_new, preferred_element_type=jnp.float32
    ).astype(jnp.bfloat16)
    placed_values = jnp.einsum(
        "bkj,bjhd->bkhd", select.astype(jnp.bfloat16), value_new, preferred_element_type=jnp.float32
    ).astype(jnp.bfloat16)
    key_out = jnp.where(written[:, :, None, None], placed_keys, key_cache)
    value_out = jnp.where(written[:, :, None, None], placed_values, value_cache)
    cum_new = last_cum[:, None, :] + path
    placed_cum = jnp.einsum(
        "bkj,bjh->bkh", select.astype(jnp.float32), cum_new, precision=lax.Precision.HIGHEST
    )
    cum_out = jnp.where(written[:, :, None], placed_cum, cum_cache)
    return (mixed, key_out, value_out, cum_out)


MESH = pl.DeviceIdType.MESH
HI = lax.Precision.HIGHEST
F32 = jnp.float32
BF = jnp.bfloat16


def iota(shape, dim):
    return lax.broadcasted_iota(jnp.int32, shape, dim)


def hot(mask):
    return jnp.where(mask, 1.0, 0.0).astype(F32)


def dot_hi(a, b, dims=(((1,), (0,)), ((), ()))):
    return lax.dot_general(a, b, dims, precision=HI, preferred_element_type=F32)


NT = (((1,), (1,)), ((), ()))


def flips(value, count):
    bit = 1
    out = [value]
    while bit < count:
        step = bit * (1 - 2 * lax.rem(lax.div(value, bit), 2))
        out = out + [other + step for other in out]
        bit *= 2
    return out


def layer_kernel(
    n,
    nt,
    num_seqs,
    prop,
    heads,
    hd,
    span,
    tok_h,
    gain_h,
    wq_h,
    wk_h,
    wv_h,
    wft_h,
    bias_h,
    wo_h,
    gpost_h,
    kc_h,
    vc_h,
    cum_h,
    lens_h,
    accs_h,
    parent_h,
    mixed_out,
    cum_out,
    knew_out,
    vnew_out,
    tokv,
    gain,
    wqkv,
    wft,
    bias,
    wov,
    gpost,
    kcv,
    vcv,
    cum,
    lens,
    accs,
    parent,
    ssq,
    invv,
    xloc,
    part_q,
    q_y,
    q_zs,
    q_zr,
    q_full,
    part_kv,
    kv_y,
    kv_zs,
    kv_zr,
    kv_full,
    st_send,
    val_send,
    st_recv,
    val_recv,
    cand_send,
    cand_recv,
    brow,
    anc,
    tpath,
    ptile,
    att,
    o_send,
    o_recv,
    sq_send,
    sq_recv,
    loc,
    ssem,
    rsem,
    tssem,
    trsem,
    qssem,
    qrsem,
):
    me = lax.axis_index("kv")
    mt = lax.axis_index("tp")
    rows, width = tokv.shape
    hw = heads * hd
    kdim = wq_h.shape[0]
    cols = heads * span
    sp = num_seqs // n
    R = sp * prop
    hp = heads * prop
    L = sp * hp
    scale = hd ** (-0.5)
    base = me * span
    heads_all = wft.shape[0]
    half = n // 2
    everyone = n * nt

    barrier = pltpu.get_barrier_semaphore()

    kvs = flips(me, n)
    tps = flips(mt, nt)

    chunks = 4
    crow = rows // chunks
    in_tok = [
        pltpu.make_async_copy(
            tok_h.at[pl.ds(i * crow, crow)], tokv.at[pl.ds(i * crow, crow)], loc.at[i]
        )
        for i in range(chunks)
    ]
    later = [
        (gain_h, gain),
        (wq_h, wqkv.at[0]),
        (wk_h, wqkv.at[1]),
        (wv_h, wqkv.at[2]),
        (wft_h, wft),
        (bias_h, bias),
        (lens_h, lens),
        (accs_h, accs),
        (parent_h, parent),
        (cum_h, cum),
        (gpost_h, gpost),
        (kc_h, kcv),
        (vc_h, vcv),
        (wo_h, wov),
    ]
    copies = [
        pltpu.make_async_copy(src, dst, loc.at[chunks + i]) for i, (src, dst) in enumerate(later)
    ]
    (
        in_gain,
        in_wq,
        in_wk,
        in_wv,
        in_wft,
        in_bias,
        in_lens,
        in_accs,
        in_parent,
        in_cum,
        in_gpost,
        in_kc,
        in_vc,
        in_wo,
    ) = copies
    for c in in_tok:
        c.start()
    for c in copies:
        c.start()
    for e in range(1, everyone):
        pl.semaphore_signal(
            barrier,
            inc=1,
            device_id={"kv": kvs[e // nt], "tp": tps[e % nt]},
            device_id_type=MESH,
        )

    def to_kv(ph, slot, mask, src, dst):
        return pltpu.make_async_remote_copy(
            src_ref=src,
            dst_ref=dst,
            send_sem=ssem.at[ph, slot],
            recv_sem=rsem.at[ph, slot],
            device_id={"kv": kvs[mask]},
            device_id_type=MESH,
        )

    def rrow(i):
        return pl.ds(pl.multiple_of(i * R, R), R)

    def q_yrs(m):
        return to_kv(0, m, 1, part_q.at[rrow(kvs[m + 1])], q_y.at[m // 2])

    def q_zrs(m):
        return to_kv(0, m + 1, m, q_zs.at[m // 2], q_zr.at[m // 2])

    def spread_to(ph, slot, mask, ref, rank):
        return to_kv(ph, slot, mask, ref.at[rrow(rank)], ref.at[rrow(rank)])

    def q_ag(m):
        return spread_to(1, m, 1, q_full, kvs[m - 1]) if m % 2 else spread_to(1, m, m, q_full, me)

    def kv_yrs(m):
        return to_kv(2, m, 1, part_kv.at[rrow(kvs[m + 1])], kv_y.at[m // 2])

    def kv_zrs(m):
        return to_kv(2, m + 1, m, kv_zs.at[m // 2], kv_zr.at[m // 2])

    def cand_copy(m):
        return to_kv(3, m, m, cand_send, cand_recv.at[m])

    def stat_copy(m):
        return to_kv(4, m, m, st_send.at[m], st_recv.at[m])

    def val_copy(m):
        return to_kv(5, m, m, val_send.at[m], val_recv.at[m])

    def att_ag(m):
        return spread_to(6, m, 1, att, kvs[m - 1]) if m % 2 else spread_to(6, m, m, att, me)

    def kv_cross():
        return spread_to(7, half, half, kv_full, me)

    def kv_pass(m):
        return spread_to(7, m, half // 2, kv_full, kvs[m - half // 2])

    def kv_side(m):
        return spread_to(7, m, 1, kv_full, kvs[m - 1])

    def each(count, fn):
        for d in range(1, count):
            fn(d)

    def each_far(count, fn):
        for d in range(count - 1, 0, -1):
            fn(d)

    zmasks = list(range(2, n, 2))
    nb = prop
    lanes = 128

    def sum_rows(i, c):
        sl = pl.ds(pl.multiple_of(i * nb, nb), nb)
        accs4 = [None] * 4
        for j in range(width // lanes):
            t = tokv[sl, j * lanes : (j + 1) * lanes].astype(F32)
            p = t * t
            accs4[j % 4] = p if accs4[j % 4] is None else accs4[j % 4] + p
        ssq[sl, :] = (accs4[0] + accs4[1]) + (accs4[2] + accs4[3])
        return c

    for i in range(chunks):
        in_tok[i].wait()
        lax.fori_loop(i * crow // nb, (i + 1) * crow // nb, sum_rows, 0)
    total = dot_hi(ssq[...], jnp.ones((lanes, lanes), F32))
    inv = lax.rsqrt(total / width + epsilon)
    invv[...] = inv
    in_gain.wait()
    for j in range(kdim // lanes):
        at = pl.ds(pl.multiple_of(me * kdim + j * lanes, lanes), lanes)
        xloc[:, j * lanes : (j + 1) * lanes] = (
            tokv[:, at].astype(F32) * inv * gain[:, at]
        ).astype(BF)
    in_wq.wait()
    part_q[...] = jnp.dot(xloc[...], wqkv[0], preferred_element_type=F32).astype(BF)
    pl.semaphore_wait(barrier, everyone - 1)
    for m in zmasks[::-1] + [0]:
        q_yrs(m).start()
    in_wk.wait()
    in_wv.wait()
    part_kv[:, 0:hw] = jnp.dot(xloc[...], wqkv[1], preferred_element_type=F32).astype(BF)
    part_kv[:, hw : 2 * hw] = jnp.dot(xloc[...], wqkv[2], preferred_element_type=F32).astype(BF)
    for m in zmasks[::-1] + [0]:
        kv_yrs(m).start()

    in_lens.wait()
    in_accs.wait()
    in_cum.wait()
    r64 = num_seqs * heads
    c64 = cum[...]
    srow = iota((r64, span), 0) // heads
    lane = iota((r64, span), 1)
    rel64 = jnp.zeros((r64, span), jnp.int32)
    rel16 = jnp.zeros((num_seqs, cols), jnp.int32)
    s16 = iota((num_seqs, cols), 0)
    for s in range(num_seqs):
        rel_s = lens[s] + accs[s] - base
        rel64 = jnp.where(srow == s, rel_s, rel64)
        rel16 = jnp.where(s16 == s, rel_s, rel16)
    cand = jnp.max(jnp.where(lane == rel64 - 1, c64, floor_value), axis=1, keepdims=True)
    diag = iota((r64, 128), 0) == iota((r64, 128), 1)
    cand_send[...] = jnp.sum(jnp.where(diag, cand, 0.0), axis=0, keepdims=True)
    each_far(n, lambda m: cand_copy(m).start())

    spread = hot(iota((span, cols), 1) // heads == iota((span, cols), 0))
    e1 = dot_hi(c64, spread)
    e1 = jnp.where(iota((r64, cols), 0) % heads == iota((r64, cols), 1) % heads, e1, 0.0)
    take = hot(iota((num_seqs, r64), 1) // heads == iota((num_seqs, r64), 0))
    cflat = dot_hi(take, e1)
    brow[...] = jnp.where(iota((num_seqs, cols), 1) // heads < rel16, -cflat, floor_value)

    in_parent.wait()
    ri = iota((rows, rows), 0)
    ci = iota((rows, rows), 1)
    pick = hot(iota((rows, num_seqs), 0) // prop == iota((rows, num_seqs), 1))
    pb = dot_hi(pick, parent[...].astype(F32))
    pcol = jnp.sum(
        jnp.where(iota((rows, prop), 1) == iota((rows, prop), 0) % prop, pb, 0.0),
        axis=1,
        keepdims=True,
    )
    target = jnp.where(pcol >= 0.0, (ri // prop * prop).astype(F32) + pcol, -1.0)
    a = jnp.where((ri == ci) | (ci.astype(F32) == target), 1.0, 0.0)
    for sweep in range(max(1, (prop - 1).bit_length())):
        low = a.astype(BF)
        a = jnp.minimum(jnp.dot(low, low, preferred_element_type=F32), 1.0)
    anc[...] = a
    for m in zmasks[::-1]:
        q_yrs(m).wait_recv()
        q_zs[m // 2] = (part_q[rrow(kvs[m])].astype(F32) + q_y[m // 2].astype(F32)).astype(BF)
        q_zrs(m).start()
    in_wft.wait()
    in_bias.wait()
    wscaled = wft[...].astype(F32) * gain[...]
    whigh = wscaled.astype(BF)
    wlow = (wscaled - whigh.astype(F32)).astype(BF)
    lf = lax.dot_general(
        jnp.concatenate([whigh, wlow], axis=0), tokv[...], NT, preferred_element_type=F32
    )
    lf = lf[0:heads_all] + lf[heads_all : 2 * heads_all]
    inv_lane = dot_hi(jnp.full((8, lanes), 1.0 / lanes, F32), invv[...], NT)[0:1]
    bcol = jnp.zeros((heads_all, rows), F32)
    for h in range(heads_all):
        bcol = jnp.where(iota((heads_all, rows), 0) == h, bias[h], bcol)
    z = lf * inv_lane + bcol
    lf = jnp.minimum(z, 0.0) - jnp.log1p(jnp.exp(-jnp.abs(z)))
    path_t = dot_hi(lf, a, NT)
    rep = hot(iota((r64, heads_all), 1) == mt * heads + iota((r64, heads_all), 0) % heads)
    pm = dot_hi(rep, path_t)
    pm = jnp.where(iota((r64, rows), 1) // prop == iota((r64, rows), 0) // heads, pm, 0.0)
    fold = hot(iota((rows, 128), 0) % prop == iota((rows, 128), 1) % prop)
    pt = dot_hi(pm, fold)
    ptile[...] = pt
    ptm = jnp.where((iota((r64, 128), 1) // prop) % heads == iota((r64, 128), 0) % heads, pt, 0.0)
    tpath[...] = dot_hi(take, ptm)
    in_kc.wait()
    in_vc.wait()

    q_yrs(0).wait_recv()
    own = part_q[rrow(me)].astype(F32) + q_y[0].astype(F32)
    for m in zmasks:
        q_zrs(m).wait_recv()
        own = own + q_zr[m // 2].astype(F32)
    q_full[rrow(me)] = own.astype(BF)
    for m in [1] + zmasks[::-1]:
        q_ag(m).start()

    for m in zmasks[::-1]:
        kv_yrs(m).wait_recv()
        kv_zs[m // 2] = (
            part_kv[rrow(kvs[m])].astype(F32) + kv_y[m // 2].astype(F32)
        ).astype(BF)
        kv_zrs(m).start()

    same_head = iota((hp, cols), 0) // prop == iota((hp, cols), 1) % heads
    diag_l = iota((L, L), 0) == iota((L, L), 1)

    def heads_of(ref, s, first):
        block = ref[pl.ds(pl.multiple_of(s * prop, prop), prop), first : first + hw]
        return jnp.concatenate([block[:, h * hd : (h + 1) * hd] for h in range(heads)], axis=0)

    def block_part(src):
        maxes, totals, values = [], [], []
        for j in range(sp):
            s = src * sp + j
            q = heads_of(q_full, s, 0)
            sc = lax.dot_general(q, kcv[s], NT, preferred_element_type=F32) * scale
            sc = jnp.where(same_head, sc + brow[pl.ds(s, 1), :], floor_value)
            m = jnp.max(sc, axis=1, keepdims=True)
            w = jnp.exp(sc - m)
            maxes.append(m)
            totals.append(jnp.sum(w, axis=1, keepdims=True))
            values.append(
                jnp.dot(w.astype(BF), vcv[s], preferred_element_type=F32).astype(BF)
            )
        m = jnp.concatenate(maxes, axis=0)
        t = jnp.concatenate(totals, axis=0)
        m_lane = jnp.sum(jnp.where(diag_l, m, 0.0), axis=0, keepdims=True)
        t_lane = jnp.sum(jnp.where(diag_l, t, 0.0), axis=0, keepdims=True)
        stats = jnp.where(iota((2, L), 0) == 0, m_lane, t_lane)
        return stats, jnp.concatenate(values, axis=0)

    def remote_blocks(masks):
        parts = [block_part(kvs[m]) for m in masks]
        for m, (stats, values) in zip(masks, parts):
            st_send[m] = stats
            val_send[m] = values
        for m in masks:
            stat_copy(m).start()
            val_copy(m).start()

    stats, values = block_part(me)
    st_recv[0] = stats
    val_recv[0] = values
    def take_q(m):
        q_ag(m).wait_recv()
        if m % 2 == 0:
            q_ag(m + 1).start()

    take_q(2)
    take_q(1)
    remote_blocks([1, 2])
    take_q(4)
    take_q(6)
    remote_blocks([4, 6])
    take_q(3)
    take_q(5)
    remote_blocks([3, 5])
    take_q(7)
    remote_blocks([7])

    kv_yrs(0).wait_recv()
    own = part_kv[rrow(me)].astype(F32) + kv_y[0].astype(F32)
    for m in zmasks:
        kv_zrs(m).wait_recv()
        own = own + kv_zr[m // 2].astype(F32)
    kv_full[rrow(me)] = own.astype(BF)

    fold_h = iota((rows, hp), 0)
    tmax, ttot, tval = [], [], []
    for j in range(sp):
        s = me * sp + j
        q = heads_of(q_full, s, 0)
        k = heads_of(kv_full, s, 0)
        v = heads_of(kv_full, s, hw)
        arows = anc[pl.ds(pl.multiple_of(s * prop, prop), prop), :]
        sel = hot(fold_h == s * prop + iota((rows, hp), 1) % prop).astype(BF)
        am = jnp.dot(arows.astype(BF), sel, preferred_element_type=F32)
        am = jnp.concatenate([am] * heads, axis=0)
        mask = (am > 0.5) & (iota((hp, hp), 0) // prop == iota((hp, hp), 1) // prop)
        sc = lax.dot_general(q, k, NT, preferred_element_type=F32) * scale
        sc = jnp.where(mask, sc - tpath[pl.ds(s, 1), 0:hp], floor_value)
        m = jnp.max(sc, axis=1, keepdims=True)
        w = jnp.where(mask, jnp.exp(sc - m), 0.0)
        tmax.append(m)
        ttot.append(jnp.sum(w, axis=1, keepdims=True))
        tval.append(jnp.dot(w.astype(BF), v, preferred_element_type=F32))
    tree_max = jnp.concatenate(tmax, axis=0)
    tree_tot = jnp.concatenate(ttot, axis=0)
    tree_val = jnp.concatenate(tval, axis=0)

    last_lane = cand_send[...]
    for m in range(1, n):
        cand_copy(m).wait_recv()
        last_lane = jnp.maximum(last_lane, cand_recv[m])
    own_rows = iota((L, 128), 0)
    own_pick = iota((L, 128), 1) == (me * sp + own_rows // hp) * heads + (own_rows % hp) // prop
    last_own = jnp.sum(jnp.where(own_pick, last_lane, 0.0), axis=1, keepdims=True)

    for m in range(1, n):
        stat_copy(m).wait_recv()
    top = st_recv[0, 0:1]
    for m in range(1, n):
        top = jnp.maximum(top, st_recv[m, 0:1])

    def col(x):
        return jnp.sum(jnp.where(diag_l, x, 0.0), axis=1, keepdims=True)

    cache_tot = jnp.zeros((1, L), F32)
    scales = []
    for m in range(n):
        sd = jnp.exp(st_recv[m, 0:1] - top)
        scales.append(col(sd))
        cache_tot = cache_tot + st_recv[m, 1:2] * sd
    shifted = col(top) + last_own
    both = jnp.maximum(shifted, tree_max)
    cscale = jnp.exp(shifted - both)
    tscale = jnp.exp(tree_max - both)
    denom = col(cache_tot) * cscale + tree_tot * tscale
    vals = val_recv[0].astype(F32) * scales[0]
    for m in range(1, n):
        val_copy(m).wait_recv()
        vals = vals + val_recv[m].astype(F32) * scales[m]
    attended = ((vals * cscale + tree_val * tscale) / denom).astype(BF)
    for j in range(sp):
        for h in range(heads):
            att[pl.ds(pl.multiple_of(me * R + j * prop, prop), prop), h * hd : (h + 1) * hd] = (
                attended[j * hp + h * prop : j * hp + (h + 1) * prop]
            )
    for m in [1] + zmasks[::-1]:
        att_ag(m).start()

    upper = me >= half

    @pl.when(upper)
    def _():
        kv_pass(2).start()
        kv_side(1).start()

    @pl.when(jnp.logical_not(upper))
    def _():
        kv_cross().start()

    last_col = jnp.sum(jnp.where(diag, last_lane, 0.0), axis=1, keepdims=True)
    shifted_path = ptile[...]
    for b in range((span - 1).bit_length()):
        moved = pltpu.roll(shifted_path, 1 << b, 1)
        shifted_path = jnp.where((rel64 >> b) & 1 == 1, moved, shifted_path)
    off = lane - rel64
    cum_out[...] = jnp.where((off >= 0) & (off < prop), last_col + shifted_path, c64)

    in_wo.wait()
    oc = o_send.shape[2]
    near = lax.div(me, half) * (half * R)
    grows = [
        pl.ds(pl.multiple_of(first, half * R), half * R) for first in (near, half * R - near)
    ]

    def o_copy(g, d):
        return pltpu.make_async_remote_copy(
            src_ref=o_send.at[tps[d], grows[g]],
            dst_ref=o_recv.at[d, grows[g]],
            send_sem=tssem.at[g, d],
            recv_sem=trsem.at[g, d],
            device_id={"tp": tps[d]},
            device_id_type=MESH,
        )

    for m in zmasks:
        att_ag(m).wait_recv()
        att_ag(m + 1).start()
    for g in range(2):
        for m in range(1 + g * half, (g + 1) * half, 2):
            att_ag(m).wait_recv()
        full = jnp.dot(att[grows[g]], wov[...], preferred_element_type=F32).astype(BF)
        for t in range(nt):
            o_send[t, grows[g]] = full[:, t * oc : (t + 1) * oc]
        each_far(nt, lambda d: o_copy(g, d).start())

    @pl.when(upper)
    def _():
        kv_cross().wait_recv()
        kv_pass(6).start()
        kv_side(5).start()
        kv_pass(2).wait_recv()
        kv_side(3).start()

    mixed = o_send[mt].astype(F32)
    for d in range(1, nt):
        o_copy(0, d).wait_recv()
        o_copy(1, d).wait_recv()
        mixed = mixed + o_recv[d].astype(F32)
    sq = dot_hi(jnp.ones((8, oc), F32), mixed * mixed, NT)[0:1]
    sq_send[...] = sq

    def sq_copy(e):
        return pltpu.make_async_remote_copy(
            src_ref=sq_send,
            dst_ref=sq_recv.at[e],
            send_sem=qssem.at[e],
            recv_sem=qrsem.at[e],
            device_id={"kv": kvs[e // nt], "tp": tps[e % nt]},
            device_id_type=MESH,
        )

    each_far(everyone, lambda e: sq_copy(e).start())

    order = hot(
        iota((hp, hp), 1) == iota((hp, hp), 0) % heads * prop + iota((hp, hp), 0) // heads
    ).astype(BF)

    unroll = 4

    @pl.when(upper)
    def _():
        kv_pass(6).wait_recv()
        kv_side(7).start()
        for m in range(1, n, 2):
            kv_side(m).wait_recv()

        def some(i, c):
            fresh = [
                heads_of(kv_full, i * unroll + j, first) for j in range(unroll) for first in (0, hw)
            ]
            placed = jnp.dot(
                order, jnp.concatenate(fresh, axis=1), preferred_element_type=F32
            ).astype(BF)
            for j in range(unroll):
                at = 2 * j * hd
                knew_out[i * unroll + j] = placed[:, at : at + hd]
                vnew_out[i * unroll + j] = placed[:, at + hd : at + 2 * hd]
            return c

        lax.fori_loop(0, num_seqs // unroll, some, 0)

    for e in range(1, everyone):
        sq_copy(e).wait_recv()
        sq = sq + sq_recv[e]
    ssum = dot_hi(
        jnp.broadcast_to(sq, (8, rows)), jnp.full((8, oc), 0.125, F32), (((0,), (0,)), ((), ()))
    )
    in_gpost.wait()
    mixed_out[...] = (mixed * lax.rsqrt(ssum / width + epsilon) * gpost[...]).astype(BF)

    def drain(m):
        q_ag(m).wait_send()
        cand_copy(m).wait_send()
        stat_copy(m).wait_send()
        val_copy(m).wait_send()
        att_ag(m).wait_send()

    each(n, drain)
    for m in [0] + zmasks:
        q_yrs(m).wait_send()
        kv_yrs(m).wait_send()
    for m in zmasks:
        q_zrs(m).wait_send()
        kv_zrs(m).wait_send()

    @pl.when(upper)
    def _():
        for m in (2, 6):
            kv_pass(m).wait_send()
        for m in range(1, n, 2):
            kv_side(m).wait_send()

    @pl.when(jnp.logical_not(upper))
    def _():
        kv_cross().wait_send()

    for g in range(2):
        each(nt, lambda d: o_copy(g, d).wait_send())
    each(everyone, lambda e: sq_copy(e).wait_send())


def patch_kernel(
    n, prop, kc, vc, knew, vnew, mixed, cum, lens, accs, k_out, v_out, mixed_out, cum_out, sem, bsem, wsem
):
    me = lax.axis_index("kv")
    num_seqs, span = k_out.shape[:2]
    out_m = pltpu.make_async_copy(mixed, mixed_out, sem.at[0])
    out_c = pltpu.make_async_copy(cum, cum_out, sem.at[1])
    bulk = [
        [
            pltpu.make_async_copy(src.at[s], dst.at[s], bsem.at[i, s])
            for i, (src, dst) in enumerate(((kc, k_out), (vc, v_out)))
        ]
        for s in range(num_seqs)
    ]
    for row in bulk:
        for c in row:
            c.start()
    out_m.start()
    out_c.start()

    def moves(act, before=None):
        for s in range(num_seqs):
            if before is not None:
                before(s)
            at = lens[s] + accs[s] - me * span
            pairs = ((knew, k_out), (vnew, v_out))

            @pl.when((at >= 0) & (at <= span - prop))
            def _():
                for i, (src, dst) in enumerate(pairs):
                    act(
                        pltpu.make_async_copy(
                            src.at[s], dst.at[s, pl.ds(at, prop)], wsem.at[i, s]
                        )
                    )

            @pl.when(((at > -prop) & (at < 0)) | ((at > span - prop) & (at < span)))
            def _():
                def one(j, c):
                    @pl.when((at + j >= 0) & (at + j < span))
                    def _():
                        for i, (src, dst) in enumerate(pairs):
                            act(
                                pltpu.make_async_copy(
                                    src.at[s, j], dst.at[s, at + j], wsem.at[i, s]
                                )
                            )

                    return c

                lax.fori_loop(0, prop, one, 0)

    def settle(s):
        for c in bulk[s]:
            c.wait()

    @pl.when(me >= n // 2)
    def _():
        moves(lambda c: c.start(), settle)
        moves(lambda c: c.wait())

    @pl.when(me < n // 2)
    def _():
        for s in range(num_seqs):
            settle(s)

    out_m.wait()
    out_c.wait()


def fast_device(
    n,
    nt,
    tokens,
    gain_pre,
    w_query,
    w_key,
    w_value,
    w_forget,
    b_forget,
    w_out,
    gain_post,
    key_cache,
    value_cache,
    cum_cache,
    lengths,
    accepted,
    parent,
):
    num_seqs, prop, width = tokens.shape
    span, heads, hd = key_cache.shape[1:]
    rows = num_seqs * prop
    hw = heads * hd
    cols = heads * span
    sp = num_seqs // n
    R = sp * prop
    L = sp * heads * prop
    oc = gain_post.shape[0]
    half = n // 2
    everyone = n * nt
    kc = key_cache.reshape(num_seqs, cols, hd)
    vc = value_cache.reshape(num_seqs, cols, hd)
    cum = jnp.swapaxes(cum_cache, 1, 2).reshape(num_seqs * heads, span)
    hbm = pl.BlockSpec(memory_space=pltpu.HBM)
    vmem = pl.BlockSpec(memory_space=pltpu.VMEM)
    smem = pl.BlockSpec(memory_space=pltpu.SMEM)
    V = pltpu.VMEM
    S = pltpu.SMEM
    D = pltpu.SemaphoreType.DMA
    mixed, cum_new, knew, vnew = pl.pallas_call(
        functools.partial(layer_kernel, n, nt, num_seqs, prop, heads, hd, span),
        out_shape=(
            V((rows, oc), BF),
            V(cum.shape, F32),
            V((num_seqs, heads * prop, hd), BF),
            V((num_seqs, heads * prop, hd), BF),
        ),
        in_specs=[hbm] * 15,
        out_specs=(vmem, vmem, vmem, vmem),
        scratch_shapes=[
            V((rows, width), BF),
            V((1, width), F32),
            V((3,) + w_query.shape, BF),
            V(w_forget.shape[::-1], BF),
            S(b_forget.shape, F32),
            V(w_out.shape, BF),
            V((1, oc), F32),
            V(kc.shape, BF),
            V(vc.shape, BF),
            V(cum.shape, F32),
            S(lengths.shape, jnp.int32),
            S(accepted.shape, jnp.int32),
            V(parent.shape, jnp.int32),
            V((rows, 128), F32),
            V((rows, 128), F32),
            V((rows, w_query.shape[0]), BF),
            V((rows, hw), BF),
            V((half, R, hw), BF),
            V((half, R, hw), BF),
            V((half, R, hw), BF),
            V((rows, hw), BF),
            V((rows, 2 * hw), BF),
            V((half, R, 2 * hw), BF),
            V((half, R, 2 * hw), BF),
            V((half, R, 2 * hw), BF),
            V((rows, 2 * hw), BF),
            V((n, 2, L), F32),
            V((n, L, hd), BF),
            V((n, 2, L), F32),
            V((n, L, hd), BF),
            V((1, 128), F32),
            V((n, 1, 128), F32),
            V((num_seqs, cols), F32),
            V((rows, rows), F32),
            V((num_seqs, 128), F32),
            V((num_seqs * heads, 128), F32),
            V((rows, hw), BF),
            V((nt, rows, oc), BF),
            V((nt, rows, oc), BF),
            V((1, rows), F32),
            V((everyone, 1, rows), F32),
            D((18,)),
            D((8, n)),
            D((8, n)),
            D((2, nt)),
            D((2, nt)),
            D((everyone,)),
            D((everyone,)),
        ],
        compiler_params=pltpu.CompilerParams(
            collective_id=0, has_side_effects=True, vmem_limit_bytes=50 * 1024 * 1024
        ),
        name="layer",
    )(
        *[
            pltpu.with_memory_space_constraint(operand, pltpu.HBM)
            for operand in (
                tokens.reshape(rows, width),
                gain_pre.reshape(1, width),
                w_query,
                w_key,
                w_value,
                w_forget.T,
                b_forget,
                w_out,
                gain_post.reshape(1, oc),
                kc,
                vc,
                cum,
                lengths,
                accepted,
                parent,
            )
        ]
    )
    fresh = (num_seqs, prop, heads, hd)
    key_out, value_out, mixed, cum_new = pl.pallas_call(
        functools.partial(patch_kernel, n, prop),
        out_shape=(
            pltpu.HBM(key_cache.shape, BF),
            pltpu.HBM(value_cache.shape, BF),
            pltpu.HBM(mixed.shape, BF),
            pltpu.HBM(cum.shape, F32),
        ),
        in_specs=[vmem, vmem, vmem, vmem, vmem, vmem, smem, smem],
        out_specs=(hbm, hbm, hbm, hbm),
        scratch_shapes=[D((2,)), D((2, num_seqs)), D((2, num_seqs))],
        compiler_params=pltpu.CompilerParams(
            has_side_effects=True, vmem_limit_bytes=4 * 1024 * 1024
        ),
        name="patch",
    )(
        *[
            pltpu.with_memory_space_constraint(operand, V)
            for operand in (key_cache, value_cache, knew.reshape(fresh), vnew.reshape(fresh), mixed, cum_new)
        ],
        lengths,
        accepted,
    )
    cum_out = jnp.swapaxes(cum_new.reshape(num_seqs, heads, span), 1, 2)
    return (
        mixed.reshape(num_seqs, prop, oc),
        key_out.reshape(key_cache.shape),
        value_out.reshape(value_cache.shape),
        cum_out,
    )


def choose(mesh):
    n, nt = mesh.shape["kv"], mesh.shape["tp"]

    def body(*args):
        tokens, key_cache = args[0], args[9]
        num_seqs, prop = tokens.shape[:2]
        span, heads = key_cache.shape[1:3]
        fits = (
            num_seqs % n == 0
            and n == 8
            and nt & (nt - 1) == 0
            and num_seqs % 4 == 0
            and (num_seqs // n) * heads * prop == 128
            and span == 128
            and num_seqs * heads <= 128
            and prop % 16 == 0
        )
        if fits:
            return fast_device(n, nt, *args)
        return per_device(*args)

    return body


def solution(mesh):
    return jax.shard_map(
        choose(mesh),
        mesh=mesh,
        in_specs=(
            P(),
            P(),
            P("kv", "tp"),
            P("kv", "tp"),
            P("kv", "tp"),
            P(),
            P(),
            P("tp", "kv"),
            P(("kv", "tp")),
            P(None, "kv", "tp", None),
            P(None, "kv", "tp", None),
            P(None, "kv", "tp"),
            P(),
            P(),
            P(),
        ),
        out_specs=(
            P(None, None, ("kv", "tp")),
            P(None, "kv", "tp", None),
            P(None, "kv", "tp", None),
            P(None, "kv", "tp"),
        ),
        check_vma=False,
    )
```

```python
import functools

import jax
import jax.numpy as jnp
from jax import lax
from jax.experimental import pallas as pl
from jax.experimental.pallas import tpu as pltpu
from jax.sharding import PartitionSpec as P

epsilon = 1e-06
floor_value = -1e30


def merged(part, axis, combine):
    gathered = jax.tree.map(lambda a: lax.all_gather(a, axis), part)

    def take(source):
        return jax.tree.map(lambda a: lax.dynamic_index_in_dim(a, source, 0, False), gathered)

    return lax.fori_loop(
        1, lax.axis_size(axis), lambda source, state: combine(state, take(source)), take(0)
    )


def ancestry(parent_ids, members):
    identity = jnp.eye(members, dtype=jnp.float32)
    parent_hot = (
        parent_ids[:, :, None] == jnp.arange(members, dtype=jnp.int32)[None, None, :]
    ).astype(jnp.float32)
    ancestors = jnp.minimum(identity[None] + parent_hot, 1.0)
    for sweep in range(max(1, (members - 1).bit_length())):
        ancestors = jnp.minimum(
            jnp.einsum("bij,bjk->bik", ancestors, ancestors, precision=lax.Precision.HIGHEST), 1.0
        )
    return ancestors


def combine_parts(first, second):
    new_max = jnp.maximum(first[0], second[0])
    first_scale = jnp.exp(first[0] - new_max)
    second_scale = jnp.exp(second[0] - new_max)
    return (
        new_max,
        first[1] * first_scale + second[1] * second_scale,
        first[2] * first_scale[..., None] + second[2] * second_scale[..., None],
        jnp.maximum(first[3], second[3]),
    )


def finish_rows(cache_max, cache_total, cache_values, last_rows, tree_max, tree_total, tree_values):
    shifted = cache_max + last_rows
    top = jnp.maximum(shifted, tree_max)
    cache_scale = jnp.exp(shifted - top)
    tree_scale = jnp.exp(tree_max - top)
    attended = (
        (cache_values * cache_scale[..., None] + tree_values * tree_scale[..., None])
        / (cache_total * cache_scale + tree_total * tree_scale)[..., None]
    ).astype(jnp.bfloat16)
    return attended.reshape(attended.shape[0], attended.shape[1] * attended.shape[2])


def per_device(
    tokens,
    gain_pre,
    w_query,
    w_key,
    w_value,
    w_forget,
    b_forget,
    w_out,
    gain_post,
    key_cache,
    value_cache,
    cum_cache,
    lengths,
    accepted,
    parent,
):
    num_seqs, proposals, model_width = tokens.shape
    kv_rank = lax.axis_index("kv")
    tp_rank = lax.axis_index("tp")
    span = key_cache.shape[1]
    heads_local = key_cache.shape[2]
    head_dim = key_cache.shape[3]
    scale = head_dim ** (-0.5)
    all_rows = num_seqs * proposals
    tok_float = tokens.astype(jnp.float32)
    normed = (
        tok_float
        * lax.rsqrt(jnp.mean(tok_float * tok_float, -1, keepdims=True) + epsilon)
        * gain_pre
    ).astype(jnp.bfloat16)
    flat = normed.reshape(all_rows, model_width)
    weight_rows = w_query.shape[0]
    local_rows = lax.dynamic_slice_in_dim(flat, kv_rank * weight_rows, weight_rows, 1)
    query_part = jnp.dot(local_rows, w_query, preferred_element_type=jnp.float32)
    key_part = jnp.dot(local_rows, w_key, preferred_element_type=jnp.float32)
    value_part = jnp.dot(local_rows, w_value, preferred_element_type=jnp.float32)
    summed = (
        lax.psum(query_part.astype(jnp.bfloat16), "kv").astype(jnp.float32),
        lax.psum(key_part.astype(jnp.bfloat16), "kv").astype(jnp.float32),
        lax.psum(value_part.astype(jnp.bfloat16), "kv").astype(jnp.float32),
    )
    query_flat = summed[0].astype(jnp.bfloat16)
    key_flat = summed[1].astype(jnp.bfloat16)
    value_flat = summed[2].astype(jnp.bfloat16)
    query = query_flat.reshape(num_seqs, proposals, heads_local, head_dim)
    key_new = key_flat.reshape(num_seqs, proposals, heads_local, head_dim)
    value_new = value_flat.reshape(num_seqs, proposals, heads_local, head_dim)
    forget_cols = lax.dynamic_slice_in_dim(w_forget, tp_rank * heads_local, heads_local, 1)
    forget_bias = lax.dynamic_slice_in_dim(b_forget, tp_rank * heads_local, heads_local, 0)
    log_forget = jax.nn.log_sigmoid(
        jnp.dot(flat, forget_cols, preferred_element_type=jnp.float32) + forget_bias
    ).reshape(num_seqs, proposals, heads_local)
    ancestors = ancestry(parent, proposals)
    path = jnp.einsum("bij,bjh->bih", ancestors, log_forget, precision=lax.Precision.HIGHEST)
    valid = lengths + accepted
    positions = kv_rank * span + jnp.arange(span, dtype=jnp.int32)
    live = (positions[None, :] < valid[:, None])[:, None, None, :]
    score = (
        jnp.einsum("bihd,bkhd->bihk", query, key_cache, preferred_element_type=jnp.float32) * scale
        + path[..., None]
        - jnp.swapaxes(cum_cache, 1, 2)[:, None]
    )
    block_max = jnp.max(jnp.where(live, score, floor_value), axis=-1)
    weight = jnp.exp(jnp.where(live, score - block_max[..., None], floor_value))
    block_total = jnp.sum(weight, axis=-1)
    block_values = jnp.einsum(
        "bihk,bkhd->bihd",
        weight.astype(jnp.bfloat16),
        value_cache,
        preferred_element_type=jnp.float32,
    )
    owner = positions[None, :] == (valid - 1)[:, None]
    candidate = jnp.max(jnp.where(owner[:, :, None], cum_cache, floor_value), axis=1)
    tree_mask = (ancestors > 0.5)[:, :, None, :]
    tree_score = (
        jnp.einsum("bihd,bjhd->bihj", query, key_new, preferred_element_type=jnp.float32) * scale
        + path[..., None]
        - jnp.swapaxes(path, 1, 2)[:, None]
    )
    tree_max = jnp.max(jnp.where(tree_mask, tree_score, floor_value), axis=-1)
    tree_weight = jnp.exp(jnp.where(tree_mask, tree_score - tree_max[..., None], floor_value))
    tree_total = jnp.sum(tree_weight, axis=-1)
    tree_values = jnp.einsum(
        "bihj,bjhd->bihd",
        tree_weight.astype(jnp.bfloat16),
        value_new,
        preferred_element_type=jnp.float32,
    )
    tree_max_rows = tree_max.reshape(all_rows, heads_local)
    tree_total_rows = tree_total.reshape(all_rows, heads_local)
    tree_values_rows = tree_values.reshape(all_rows, heads_local, head_dim)
    cache_max, cache_total, cache_values, last_cum = merged(
        (block_max, block_total, block_values, candidate), "kv", combine_parts
    )
    last_rows = jnp.broadcast_to(last_cum[:, None, :], (num_seqs, proposals, heads_local)).reshape(
        all_rows, heads_local
    )
    attended = finish_rows(
        cache_max.reshape(all_rows, heads_local),
        cache_total.reshape(all_rows, heads_local),
        cache_values.reshape(all_rows, heads_local, head_dim),
        last_rows,
        tree_max_rows,
        tree_total_rows,
        tree_values_rows,
    )
    mixed_part = jnp.dot(attended, w_out, preferred_element_type=jnp.float32)
    mixed_sum = lax.psum_scatter(
        mixed_part.astype(jnp.bfloat16), "tp", scatter_dimension=1, tiled=True
    ).astype(jnp.float32)
    squares = lax.psum(jnp.sum(mixed_sum * mixed_sum, axis=1), ("kv", "tp"))
    mixed = (mixed_sum * lax.rsqrt(squares / model_width + epsilon)[:, None] * gain_post).astype(
        jnp.bfloat16
    )
    mixed = mixed.reshape(num_seqs, proposals, mixed_sum.shape[1])
    relative = positions[None, :] - valid[:, None]
    select = relative[:, :, None] == jnp.arange(proposals, dtype=jnp.int32)[None, None, :]
    written = (relative >= 0) & (relative < proposals)
    placed_keys = jnp.einsum(
        "bkj,bjhd->bkhd", select.astype(jnp.bfloat16), key_new, preferred_element_type=jnp.float32
    ).astype(jnp.bfloat16)
    placed_values = jnp.einsum(
        "bkj,bjhd->bkhd", select.astype(jnp.bfloat16), value_new, preferred_element_type=jnp.float32
    ).astype(jnp.bfloat16)
    key_out = jnp.where(written[:, :, None, None], placed_keys, key_cache)
    value_out = jnp.where(written[:, :, None, None], placed_values, value_cache)
    cum_new = last_cum[:, None, :] + path
    placed_cum = jnp.einsum(
        "bkj,bjh->bkh", select.astype(jnp.float32), cum_new, precision=lax.Precision.HIGHEST
    )
    cum_out = jnp.where(written[:, :, None], placed_cum, cum_cache)
    return (mixed, key_out, value_out, cum_out)


MESH = pl.DeviceIdType.MESH
HI = lax.Precision.HIGHEST
F32 = jnp.float32
BF = jnp.bfloat16


def iota(shape, dim):
    return lax.broadcasted_iota(jnp.int32, shape, dim)


def hot(mask):
    return jnp.where(mask, 1.0, 0.0).astype(F32)


def dot_hi(a, b, dims=(((1,), (0,)), ((), ()))):
    return lax.dot_general(a, b, dims, precision=HI, preferred_element_type=F32)


NT = (((1,), (1,)), ((), ()))


def flips(value, count):
    bit = 1
    out = [value]
    while bit < count:
        step = bit * (1 - 2 * lax.rem(lax.div(value, bit), 2))
        out = out + [other + step for other in out]
        bit *= 2
    return out


def layer_kernel(
    n,
    nt,
    num_seqs,
    prop,
    heads,
    hd,
    span,
    tok_h,
    gain_h,
    wq_h,
    wk_h,
    wv_h,
    wft_h,
    bias_h,
    wo_h,
    gpost_h,
    kc_h,
    vc_h,
    cum_h,
    lens_h,
    accs_h,
    parent_h,
    mixed_out,
    cum_out,
    knew_out,
    vnew_out,
    kcv,
    vcv,
    tokv,
    gain,
    wqkv,
    wft,
    bias,
    wov,
    gpost,
    cum,
    lens,
    accs,
    parent,
    ssq,
    invv,
    xloc,
    part_q,
    q_y,
    q_zs,
    q_zr,
    q_full,
    part_kv,
    kv_y,
    kv_zs,
    kv_zr,
    kv_full,
    st_send,
    val_send,
    st_recv,
    val_recv,
    cand_send,
    cand_recv,
    brow,
    anc,
    tpath,
    ptile,
    att,
    o_send,
    o_recv,
    sq_send,
    sq_recv,
    loc,
    ssem,
    rsem,
):
    me = lax.axis_index("kv")
    mt = lax.axis_index("tp")
    rows, width = tokv.shape
    hw = heads * hd
    kdim = wq_h.shape[0]
    cols = heads * span
    sp = num_seqs // n
    R = sp * prop
    hp = heads * prop
    L = sp * hp
    scale = hd ** (-0.5)
    base = me * span
    heads_all = wft.shape[0]
    half = n // 2
    everyone = n * nt

    barrier = pltpu.get_barrier_semaphore()

    kvs = flips(me, n)
    tps = flips(mt, nt)

    chunks = 4
    crow = rows // chunks
    in_tok = [
        pltpu.make_async_copy(
            tok_h.at[pl.ds(i * crow, crow)], tokv.at[pl.ds(i * crow, crow)], loc.at[i]
        )
        for i in range(chunks)
    ]
    later = [
        (gain_h, gain),
        (wq_h, wqkv.at[0]),
        (wk_h, wqkv.at[1]),
        (wv_h, wqkv.at[2]),
        (wft_h, wft),
        (bias_h, bias),
        (lens_h, lens),
        (accs_h, accs),
        (parent_h, parent),
        (cum_h, cum),
        (gpost_h, gpost),
        (wo_h, wov),
        (kc_h, kcv),
        (vc_h, vcv),
    ]
    copies = [
        pltpu.make_async_copy(src, dst, loc.at[chunks + i]) for i, (src, dst) in enumerate(later)
    ]
    (
        in_gain,
        in_wq,
        in_wk,
        in_wv,
        in_wft,
        in_bias,
        in_lens,
        in_accs,
        in_parent,
        in_cum,
        in_gpost,
        in_wo,
        in_kc,
        in_vc,
    ) = copies
    for c in in_tok:
        c.start()
    for c in copies[:-3]:
        c.start()
    for e in range(1, everyone):
        pl.semaphore_signal(
            barrier,
            inc=1,
            device_id={"kv": kvs[e // nt], "tp": tps[e % nt]},
            device_id_type=MESH,
        )

    def send(kind, slot, device, src, dst):
        return pltpu.make_async_remote_copy(
            src_ref=src,
            dst_ref=dst,
            send_sem=ssem.at[kind],
            recv_sem=rsem.at[slot],
            device_id=device,
            device_id_type=MESH,
        )

    def to_kv(kind, slot, mask, src, dst):
        return send(kind, slot, {"kv": kvs[mask]}, src, dst)

    def rrow(i):
        return pl.ds(pl.multiple_of(i * R, R), R)

    def spread_to(kind, slot, mask, ref, rank):
        return to_kv(kind, slot, mask, ref.at[rrow(rank)], ref.at[rrow(rank)])

    def sent(kind, ref):
        to_kv(kind, 0, 1, ref, ref).wait_send()

    def received(slot, ref):
        to_kv(0, slot, 1, ref, ref).wait_recv()

    flat = [0]

    def slots(count):
        flat[0] += count
        return flat[0] - count

    on_qy, on_qz, on_ky, on_kz = slots(half), slots(1), slots(half), slots(1)
    on_qag, on_cand, on_stat, on_val = slots(n), slots(1), slots(1), slots(n)
    on_att, on_kvag, on_o, on_sq = slots(n), slots(n), slots(2), slots(1)
    last = n - 1

    def q_yrs(m):
        return to_kv(0, on_qy + m // 2, 1, part_q.at[rrow(kvs[m + 1])], q_y.at[m // 2])

    def q_zrs(m):
        return to_kv(1, on_qz, m, q_zs.at[m // 2], q_zr.at[m // 2])

    def kv_yrs(m):
        src = part_kv.at[rrow(kvs[(m + 1) ^ last])]
        return to_kv(2, on_ky + m // 2, 1, src, kv_y.at[m // 2])

    def kv_zrs(m):
        return to_kv(3, on_kz, m, kv_zs.at[m // 2], kv_zr.at[m // 2])

    def q_ag(m):
        if m % 2:
            return spread_to(4, on_qag + m, 1, q_full, kvs[m - 1])
        return spread_to(4, on_qag + m, m, q_full, me)

    def cand_copy(m):
        return to_kv(5, on_cand, m, cand_send, cand_recv.at[m])

    def stat_copy(m):
        return to_kv(6, on_stat, m, st_send.at[m], st_recv.at[m])

    def val_copy(m):
        return to_kv(7, on_val + m, m, val_send.at[m], val_recv.at[m])

    def att_ag(m):
        if m % 2:
            return spread_to(8, on_att + m, 1, att, kvs[(m - 1) ^ last])
        return spread_to(8, on_att + m, m, att, kvs[last])

    def kv_cross():
        return spread_to(9, on_kvag + half, half, kv_full, kvs[last])

    def kv_pass(m):
        return spread_to(9, on_kvag + m, half // 2, kv_full, kvs[(m - half // 2) ^ last])

    def kv_side(m):
        return spread_to(9, on_kvag + m, 1, kv_full, kvs[(m - 1) ^ last])

    def each(count, fn):
        for d in range(1, count):
            fn(d)

    def each_far(count, fn):
        for d in range(count - 1, 0, -1):
            fn(d)

    zmasks = list(range(2, n, 2))
    nb = prop
    lanes = 128

    def sum_rows(i, c):
        sl = pl.ds(pl.multiple_of(i * nb, nb), nb)
        accs4 = [None] * 4
        for j in range(width // lanes):
            t = tokv[sl, j * lanes : (j + 1) * lanes].astype(F32)
            p = t * t
            accs4[j % 4] = p if accs4[j % 4] is None else accs4[j % 4] + p
        ssq[sl, :] = (accs4[0] + accs4[1]) + (accs4[2] + accs4[3])
        return c

    for i in range(chunks):
        in_tok[i].wait()
        if i == chunks - 1:
            for c in copies[-3:]:
                c.start()
        lax.fori_loop(i * crow // nb, (i + 1) * crow // nb, sum_rows, 0)
    total = dot_hi(ssq[...], jnp.ones((lanes, lanes), F32))
    inv = lax.rsqrt(total / width + epsilon)
    invv[...] = inv
    in_gain.wait()
    for j in range(kdim // lanes):
        at = pl.ds(pl.multiple_of(me * kdim + j * lanes, lanes), lanes)
        xloc[:, j * lanes : (j + 1) * lanes] = (
            tokv[:, at].astype(F32) * inv * gain[:, at]
        ).astype(BF)
    in_wq.wait()
    part_q[...] = jnp.dot(xloc[...], wqkv[0], preferred_element_type=F32).astype(BF)
    pl.semaphore_wait(barrier, everyone - 1)
    for m in zmasks[::-1] + [0]:
        q_yrs(m).start()
    in_wk.wait()
    in_wv.wait()
    part_kv[:, 0:hw] = jnp.dot(xloc[...], wqkv[1], preferred_element_type=F32).astype(BF)
    part_kv[:, hw : 2 * hw] = jnp.dot(xloc[...], wqkv[2], preferred_element_type=F32).astype(BF)
    for m in zmasks[::-1] + [0]:
        kv_yrs(m).start()

    in_lens.wait()
    in_accs.wait()
    in_cum.wait()
    r64 = num_seqs * heads
    c64 = cum[...]
    srow = iota((r64, span), 0) // heads
    lane = iota((r64, span), 1)
    rel64 = jnp.zeros((r64, span), jnp.int32)
    rel16 = jnp.zeros((num_seqs, cols), jnp.int32)
    s16 = iota((num_seqs, cols), 0)
    for s in range(num_seqs):
        rel_s = lens[s] + accs[s] - base
        rel64 = jnp.where(srow == s, rel_s, rel64)
        rel16 = jnp.where(s16 == s, rel_s, rel16)
    cand = jnp.max(jnp.where(lane == rel64 - 1, c64, floor_value), axis=1, keepdims=True)
    diag = iota((r64, 128), 0) == iota((r64, 128), 1)
    cand_send[...] = jnp.sum(jnp.where(diag, cand, 0.0), axis=0, keepdims=True)
    each_far(n, lambda m: cand_copy(m).start())

    spread = hot(iota((span, cols), 1) // heads == iota((span, cols), 0))
    e1 = dot_hi(c64, spread)
    e1 = jnp.where(iota((r64, cols), 0) % heads == iota((r64, cols), 1) % heads, e1, 0.0)
    take = hot(iota((num_seqs, r64), 1) // heads == iota((num_seqs, r64), 0))
    cflat = dot_hi(take, e1)
    brow[...] = jnp.where(iota((num_seqs, cols), 1) // heads < rel16, -cflat, floor_value)

    in_parent.wait()
    ri = iota((rows, rows), 0)
    ci = iota((rows, rows), 1)
    pick = hot(iota((rows, num_seqs), 0) // prop == iota((rows, num_seqs), 1))
    pb = dot_hi(pick, parent[...].astype(F32))
    pcol = jnp.sum(
        jnp.where(iota((rows, prop), 1) == iota((rows, prop), 0) % prop, pb, 0.0),
        axis=1,
        keepdims=True,
    )
    target = jnp.where(pcol >= 0.0, (ri // prop * prop).astype(F32) + pcol, -1.0)
    a = jnp.where((ri == ci) | (ci.astype(F32) == target), 1.0, 0.0)
    for sweep in range(max(1, (prop - 1).bit_length())):
        low = a.astype(BF)
        a = jnp.minimum(jnp.dot(low, low, preferred_element_type=F32), 1.0)
    anc[...] = a
    for m in zmasks[::-1]:
        q_yrs(m).wait_recv()
        q_zs[m // 2] = (part_q[rrow(kvs[m])].astype(F32) + q_y[m // 2].astype(F32)).astype(BF)
        q_zrs(m).start()
    in_wft.wait()
    in_bias.wait()
    wscaled = wft[...].astype(F32) * gain[...]
    whigh = wscaled.astype(BF)
    wlow = (wscaled - whigh.astype(F32)).astype(BF)
    lf = lax.dot_general(
        jnp.concatenate([whigh, wlow], axis=0), tokv[...], NT, preferred_element_type=F32
    )
    lf = lf[0:heads_all] + lf[heads_all : 2 * heads_all]
    inv_lane = dot_hi(jnp.full((8, lanes), 1.0 / lanes, F32), invv[...], NT)[0:1]
    bcol = jnp.zeros((heads_all, rows), F32)
    for h in range(heads_all):
        bcol = jnp.where(iota((heads_all, rows), 0) == h, bias[h], bcol)
    z = lf * inv_lane + bcol
    lf = jnp.minimum(z, 0.0) - jnp.log1p(jnp.exp(-jnp.abs(z)))
    path_t = dot_hi(lf, a, NT)
    rep = hot(iota((r64, heads_all), 1) == mt * heads + iota((r64, heads_all), 0) % heads)
    pm = dot_hi(rep, path_t)
    pm = jnp.where(iota((r64, rows), 1) // prop == iota((r64, rows), 0) // heads, pm, 0.0)
    fold = hot(iota((rows, 128), 0) % prop == iota((rows, 128), 1) % prop)
    pt = dot_hi(pm, fold)
    ptile[...] = pt
    ptm = jnp.where((iota((r64, 128), 1) // prop) % heads == iota((r64, 128), 0) % heads, pt, 0.0)
    tpath[...] = dot_hi(take, ptm)
    in_kc.wait()
    in_vc.wait()

    q_yrs(0).wait_recv()
    own = part_q[rrow(me)].astype(F32) + q_y[0].astype(F32)
    received(on_qz, q_zr.at[pl.ds(1, half - 1)])
    for m in zmasks:
        own = own + q_zr[m // 2].astype(F32)
    q_full[rrow(me)] = own.astype(BF)
    for m in [1] + zmasks[::-1]:
        q_ag(m).start()

    same_head = iota((hp, cols), 0) // prop == iota((hp, cols), 1) % heads
    diag_l = iota((L, L), 0) == iota((L, L), 1)

    def heads_of(ref, s, first):
        block = ref[pl.ds(pl.multiple_of(s * prop, prop), prop), first : first + hw]
        return jnp.concatenate([block[:, h * hd : (h + 1) * hd] for h in range(heads)], axis=0)

    def block_part(src):
        maxes, totals, values = [], [], []
        for j in range(sp):
            s = src * sp + j
            q = heads_of(q_full, s, 0)
            sc = lax.dot_general(q, kcv[s], NT, preferred_element_type=F32) * scale
            sc = jnp.where(same_head, sc + brow[pl.ds(s, 1), :], floor_value)
            m = jnp.max(sc, axis=1, keepdims=True)
            w = jnp.exp(sc - m)
            maxes.append(m)
            totals.append(jnp.sum(w, axis=1, keepdims=True))
            values.append(
                jnp.dot(w.astype(BF), vcv[s], preferred_element_type=F32).astype(BF)
            )
        m = jnp.concatenate(maxes, axis=0)
        t = jnp.concatenate(totals, axis=0)
        m_lane = jnp.sum(jnp.where(diag_l, m, 0.0), axis=0, keepdims=True)
        t_lane = jnp.sum(jnp.where(diag_l, t, 0.0), axis=0, keepdims=True)
        stats = jnp.where(iota((2, L), 0) == 0, m_lane, t_lane)
        return stats, jnp.concatenate(values, axis=0)

    def blocks(masks):
        parts = [block_part(kvs[m]) for m in masks]
        for m, (stats, values) in zip(masks, parts):
            if m == last:
                st_recv[0] = stats
                val_recv[0] = values
            else:
                st_send[last - m] = stats
                val_send[last - m] = values
        for m in masks:
            if m != last:
                stat_copy(last - m).start()
                val_copy(last - m).start()

    blocks([0])
    for m in zmasks[::-1]:
        kv_yrs(m).wait_recv()
        kv_zs[m // 2] = (
            part_kv[rrow(kvs[m ^ last])].astype(F32) + kv_y[m // 2].astype(F32)
        ).astype(BF)
        kv_zrs(m).start()

    def take_q(m):
        q_ag(m).wait_recv()
        if m % 2 == 0:
            q_ag(m + 1).start()

    take_q(2)
    take_q(1)
    blocks([1, 2])
    take_q(4)
    take_q(6)
    blocks([4, 6])
    take_q(3)
    take_q(5)
    blocks([3, 5])
    take_q(7)
    blocks([7])

    kv_yrs(0).wait_recv()
    own = part_kv[rrow(kvs[last])].astype(F32) + kv_y[0].astype(F32)
    received(on_kz, kv_zr.at[pl.ds(1, half - 1)])
    for m in zmasks:
        own = own + kv_zr[m // 2].astype(F32)
    kv_full[rrow(kvs[last])] = own.astype(BF)

    fold_h = iota((rows, hp), 0)
    tmax, ttot, tval = [], [], []
    for j in range(sp):
        s = kvs[last] * sp + j
        q = heads_of(q_full, s, 0)
        k = heads_of(kv_full, s, 0)
        v = heads_of(kv_full, s, hw)
        arows = anc[pl.ds(pl.multiple_of(s * prop, prop), prop), :]
        sel = hot(fold_h == s * prop + iota((rows, hp), 1) % prop).astype(BF)
        am = jnp.dot(arows.astype(BF), sel, preferred_element_type=F32)
        am = jnp.concatenate([am] * heads, axis=0)
        mask = (am > 0.5) & (iota((hp, hp), 0) // prop == iota((hp, hp), 1) // prop)
        sc = lax.dot_general(q, k, NT, preferred_element_type=F32) * scale
        sc = jnp.where(mask, sc - tpath[pl.ds(s, 1), 0:hp], floor_value)
        m = jnp.max(sc, axis=1, keepdims=True)
        w = jnp.where(mask, jnp.exp(sc - m), 0.0)
        tmax.append(m)
        ttot.append(jnp.sum(w, axis=1, keepdims=True))
        tval.append(jnp.dot(w.astype(BF), v, preferred_element_type=F32))
    tree_max = jnp.concatenate(tmax, axis=0)
    tree_tot = jnp.concatenate(ttot, axis=0)
    tree_val = jnp.concatenate(tval, axis=0)

    last_lane = cand_send[...]
    received(on_cand, cand_recv.at[pl.ds(1, n - 1)])
    for m in range(1, n):
        last_lane = jnp.maximum(last_lane, cand_recv[m])
    own_rows = iota((L, 128), 0)
    own_head = (kvs[last] * sp + own_rows // hp) * heads + (own_rows % hp) // prop
    own_pick = iota((L, 128), 1) == own_head
    last_own = jnp.sum(jnp.where(own_pick, last_lane, 0.0), axis=1, keepdims=True)

    received(on_stat, st_recv.at[pl.ds(1, n - 1)])
    top = st_recv[0, 0:1]
    for m in range(1, n):
        top = jnp.maximum(top, st_recv[m, 0:1])

    def col(x):
        return jnp.sum(jnp.where(diag_l, x, 0.0), axis=1, keepdims=True)

    cache_tot = jnp.zeros((1, L), F32)
    scales = []
    for m in range(n):
        sd = jnp.exp(st_recv[m, 0:1] - top)
        scales.append(col(sd))
        cache_tot = cache_tot + st_recv[m, 1:2] * sd
    shifted = col(top) + last_own
    both = jnp.maximum(shifted, tree_max)
    cscale = jnp.exp(shifted - both)
    tscale = jnp.exp(tree_max - both)
    denom = col(cache_tot) * cscale + tree_tot * tscale
    vals = val_recv[0].astype(F32) * scales[0]
    for m in range(1, n):
        val_copy(m).wait_recv()
        vals = vals + val_recv[m].astype(F32) * scales[m]
    attended = ((vals * cscale + tree_val * tscale) / denom).astype(BF)
    for j in range(sp):
        for h in range(heads):
            att[pl.ds(pl.multiple_of(kvs[last] * R + j * prop, prop), prop), h * hd : (h + 1) * hd] = (
                attended[j * hp + h * prop : j * hp + (h + 1) * prop]
            )
    for m in [1] + zmasks[::-1]:
        att_ag(m).start()

    upper = me >= half

    @pl.when(upper)
    def _():
        kv_pass(2).start()
        kv_side(1).start()

    @pl.when(jnp.logical_not(upper))
    def _():
        kv_cross().start()

    last_col = jnp.sum(jnp.where(diag, last_lane, 0.0), axis=1, keepdims=True)
    shifted_path = ptile[...]
    for b in range((span - 1).bit_length()):
        moved = pltpu.roll(shifted_path, 1 << b, 1)
        shifted_path = jnp.where((rel64 >> b) & 1 == 1, moved, shifted_path)
    off = lane - rel64
    cum_out[...] = jnp.where((off >= 0) & (off < prop), last_col + shifted_path, c64)

    in_wo.wait()
    oc = o_send.shape[2]
    near = half * R - lax.div(me, half) * (half * R)
    grows = [
        pl.ds(pl.multiple_of(first, half * R), half * R) for first in (near, half * R - near)
    ]

    def o_copy(g, d):
        return send(
            10,
            on_o + g,
            {"tp": tps[d]},
            o_send.at[tps[d], grows[g]],
            o_recv.at[d, grows[g]],
        )

    for m in zmasks:
        att_ag(m).wait_recv()
        att_ag(m + 1).start()
    for g in range(2):
        for m in range(1 + g * half, (g + 1) * half, 2):
            att_ag(m).wait_recv()
        full = jnp.dot(att[grows[g]], wov[...], preferred_element_type=F32).astype(BF)
        for t in range(nt):
            o_send[t, grows[g]] = full[:, t * oc : (t + 1) * oc]
        each_far(nt, lambda d: o_copy(g, d).start())

    @pl.when(upper)
    def _():
        kv_cross().wait_recv()
        kv_pass(6).start()
        kv_side(5).start()
        kv_pass(2).wait_recv()
        kv_side(3).start()

    mixed = o_send[mt].astype(F32)
    for g in range(2):
        received(on_o + g, o_recv.at[pl.ds(1, nt - 1), grows[g]])
    for d in range(1, nt):
        mixed = mixed + o_recv[d].astype(F32)
    sq = dot_hi(jnp.ones((8, oc), F32), mixed * mixed, NT)[0:1]
    sq_send[...] = sq

    def sq_copy(e):
        peer = {"kv": kvs[e // nt], "tp": tps[e % nt]}
        return send(11, on_sq, peer, sq_send, sq_recv.at[e])

    each_far(everyone, lambda e: sq_copy(e).start())

    order = hot(
        iota((hp, hp), 1) == iota((hp, hp), 0) % heads * prop + iota((hp, hp), 0) // heads
    ).astype(BF)

    unroll = 4

    @pl.when(upper)
    def _():
        kv_pass(6).wait_recv()
        kv_side(7).start()
        for m in range(1, n, 2):
            kv_side(m).wait_recv()

        def some(i, c):
            fresh = [
                heads_of(kv_full, i * unroll + j, first) for j in range(unroll) for first in (0, hw)
            ]
            placed = jnp.dot(
                order, jnp.concatenate(fresh, axis=1), preferred_element_type=F32
            ).astype(BF)
            for j in range(unroll):
                at = 2 * j * hd
                knew_out[i * unroll + j] = placed[:, at : at + hd]
                vnew_out[i * unroll + j] = placed[:, at + hd : at + 2 * hd]
            return c

        lax.fori_loop(0, num_seqs // unroll, some, 0)

    received(on_sq, sq_recv.at[pl.ds(1, everyone - 1)])
    for e in range(1, everyone):
        sq = sq + sq_recv[e]
    ssum = dot_hi(
        jnp.broadcast_to(sq, (8, rows)), jnp.full((8, oc), 0.125, F32), (((0,), (0,)), ((), ()))
    )
    in_gpost.wait()
    mixed_out[...] = (mixed * lax.rsqrt(ssum / width + epsilon) * gpost[...]).astype(BF)

    sent(0, q_y)
    sent(1, q_zr.at[pl.ds(1, half - 1)])
    sent(2, kv_y)
    sent(3, kv_zr.at[pl.ds(1, half - 1)])
    sent(4, q_full.at[pl.ds(0, last * R)])
    sent(5, cand_recv.at[pl.ds(1, last)])
    sent(6, st_recv.at[pl.ds(1, last)])
    sent(7, val_recv.at[pl.ds(1, last)])
    sent(8, att.at[pl.ds(0, last * R)])

    @pl.when(upper)
    def _():
        sent(9, kv_full.at[pl.ds(0, (2 + half) * R)])

    @pl.when(jnp.logical_not(upper))
    def _():
        sent(9, kv_full.at[pl.ds(0, R)])

    sent(10, o_recv.at[pl.ds(1, nt - 1)])
    sent(11, sq_recv.at[pl.ds(1, everyone - 1)])


def patch_kernel(
    n, prop, kc, vc, knew, vnew, mixed, cum, lens, accs, k_out, v_out, mixed_out, cum_out, sem, bsem, wsem
):
    me = lax.axis_index("kv")
    num_seqs, span = k_out.shape[:2]
    out_m = pltpu.make_async_copy(mixed, mixed_out, sem.at[0])
    out_c = pltpu.make_async_copy(cum, cum_out, sem.at[1])
    bulk = [
        [
            pltpu.make_async_copy(src.at[s], dst.at[s], bsem.at[i, s])
            for i, (src, dst) in enumerate(((kc, k_out), (vc, v_out)))
        ]
        for s in range(num_seqs)
    ]
    for row in bulk:
        for c in row:
            c.start()
    out_m.start()
    out_c.start()

    def moves(act, before=None):
        for s in range(num_seqs):
            if before is not None:
                before(s)
            at = lens[s] + accs[s] - me * span
            pairs = ((knew, k_out), (vnew, v_out))

            @pl.when((at >= 0) & (at <= span - prop))
            def _():
                for i, (src, dst) in enumerate(pairs):
                    act(
                        pltpu.make_async_copy(
                            src.at[s], dst.at[s, pl.ds(at, prop)], wsem.at[i, s]
                        )
                    )

            @pl.when(((at > -prop) & (at < 0)) | ((at > span - prop) & (at < span)))
            def _():
                def one(j, c):
                    @pl.when((at + j >= 0) & (at + j < span))
                    def _():
                        for i, (src, dst) in enumerate(pairs):
                            act(
                                pltpu.make_async_copy(
                                    src.at[s, j], dst.at[s, at + j], wsem.at[i, s]
                                )
                            )

                    return c

                lax.fori_loop(0, prop, one, 0)

    def settle(s):
        for c in bulk[s]:
            c.wait()

    @pl.when(me >= n // 2)
    def _():
        moves(lambda c: c.start(), settle)
        moves(lambda c: c.wait())

    @pl.when(me < n // 2)
    def _():
        for s in range(num_seqs):
            settle(s)

    out_m.wait()
    out_c.wait()


def fast_device(
    n,
    nt,
    tokens,
    gain_pre,
    w_query,
    w_key,
    w_value,
    w_forget,
    b_forget,
    w_out,
    gain_post,
    key_cache,
    value_cache,
    cum_cache,
    lengths,
    accepted,
    parent,
):
    num_seqs, prop, width = tokens.shape
    span, heads, hd = key_cache.shape[1:]
    rows = num_seqs * prop
    hw = heads * hd
    cols = heads * span
    sp = num_seqs // n
    R = sp * prop
    L = sp * heads * prop
    oc = gain_post.shape[0]
    half = n // 2
    everyone = n * nt
    kc = key_cache.reshape(num_seqs, cols, hd)
    vc = value_cache.reshape(num_seqs, cols, hd)
    cum = jnp.swapaxes(cum_cache, 1, 2).reshape(num_seqs * heads, span)
    hbm = pl.BlockSpec(memory_space=pltpu.HBM)
    vmem = pl.BlockSpec(memory_space=pltpu.VMEM)
    smem = pl.BlockSpec(memory_space=pltpu.SMEM)
    V = pltpu.VMEM
    S = pltpu.SMEM
    D = pltpu.SemaphoreType.DMA
    mixed, cum_new, knew, vnew, kv, vv = pl.pallas_call(
        functools.partial(layer_kernel, n, nt, num_seqs, prop, heads, hd, span),
        out_shape=(
            V((rows, oc), BF),
            V(cum.shape, F32),
            V((num_seqs, heads * prop, hd), BF),
            V((num_seqs, heads * prop, hd), BF),
            V(kc.shape, BF),
            V(vc.shape, BF),
        ),
        in_specs=[hbm] * 15,
        out_specs=(vmem,) * 6,
        scratch_shapes=[
            V((rows, width), BF),
            V((1, width), F32),
            V((3,) + w_query.shape, BF),
            V(w_forget.shape[::-1], BF),
            S(b_forget.shape, F32),
            V(w_out.shape, BF),
            V((1, oc), F32),
            V(cum.shape, F32),
            S(lengths.shape, jnp.int32),
            S(accepted.shape, jnp.int32),
            V(parent.shape, jnp.int32),
            V((rows, 128), F32),
            V((rows, 128), F32),
            V((rows, w_query.shape[0]), BF),
            V((rows, hw), BF),
            V((half, R, hw), BF),
            V((half, R, hw), BF),
            V((half, R, hw), BF),
            V((rows, hw), BF),
            V((rows, 2 * hw), BF),
            V((half, R, 2 * hw), BF),
            V((half, R, 2 * hw), BF),
            V((half, R, 2 * hw), BF),
            V((rows, 2 * hw), BF),
            V((n, 2, L), F32),
            V((n, L, hd), BF),
            V((n, 2, L), F32),
            V((n, L, hd), BF),
            V((1, 128), F32),
            V((n, 1, 128), F32),
            V((num_seqs, cols), F32),
            V((rows, rows), F32),
            V((num_seqs, 128), F32),
            V((num_seqs * heads, 128), F32),
            V((rows, hw), BF),
            V((nt, rows, oc), BF),
            V((nt, rows, oc), BF),
            V((1, rows), F32),
            V((everyone, 1, rows), F32),
            D((18,)),
            D((12,)),
            D((2 * half + 4 * n + 7,)),
        ],
        compiler_params=pltpu.CompilerParams(
            collective_id=0, has_side_effects=True, vmem_limit_bytes=50 * 1024 * 1024
        ),
        name="layer",
    )(
        *[
            pltpu.with_memory_space_constraint(operand, pltpu.HBM)
            for operand in (
                tokens.reshape(rows, width),
                gain_pre.reshape(1, width),
                w_query,
                w_key,
                w_value,
                w_forget.T,
                b_forget,
                w_out,
                gain_post.reshape(1, oc),
                kc,
                vc,
                cum,
                lengths,
                accepted,
                parent,
            )
        ]
    )
    fresh = (num_seqs, prop, heads, hd)
    key_out, value_out, mixed, cum_new = pl.pallas_call(
        functools.partial(patch_kernel, n, prop),
        out_shape=(
            pltpu.HBM(key_cache.shape, BF),
            pltpu.HBM(value_cache.shape, BF),
            pltpu.HBM(mixed.shape, BF),
            pltpu.HBM(cum.shape, F32),
        ),
        in_specs=[vmem, vmem, vmem, vmem, vmem, vmem, smem, smem],
        out_specs=(hbm, hbm, hbm, hbm),
        scratch_shapes=[D((2,)), D((2, num_seqs)), D((2, num_seqs))],
        compiler_params=pltpu.CompilerParams(
            has_side_effects=True, vmem_limit_bytes=4 * 1024 * 1024
        ),
        name="patch",
    )(
        *[
            pltpu.with_memory_space_constraint(operand, V)
            for operand in (kv.reshape(key_cache.shape), vv.reshape(key_cache.shape), knew.reshape(fresh), vnew.reshape(fresh), mixed, cum_new)
        ],
        lengths,
        accepted,
    )
    cum_out = jnp.swapaxes(cum_new.reshape(num_seqs, heads, span), 1, 2)
    return (
        mixed.reshape(num_seqs, prop, oc),
        key_out.reshape(key_cache.shape),
        value_out.reshape(value_cache.shape),
        cum_out,
    )


def choose(mesh):
    n, nt = mesh.shape["kv"], mesh.shape["tp"]

    def body(*args):
        tokens, key_cache = args[0], args[9]
        num_seqs, prop = tokens.shape[:2]
        span, heads = key_cache.shape[1:3]
        fits = (
            num_seqs % n == 0
            and n == 8
            and nt & (nt - 1) == 0
            and num_seqs % 4 == 0
            and (num_seqs // n) * heads * prop == 128
            and span == 128
            and num_seqs * heads <= 128
            and prop % 16 == 0
        )
        if fits:
            return fast_device(n, nt, *args)
        return per_device(*args)

    return body


def solution(mesh):
    return jax.shard_map(
        choose(mesh),
        mesh=mesh,
        in_specs=(
            P(),
            P(),
            P("kv", "tp"),
            P("kv", "tp"),
            P("kv", "tp"),
            P(),
            P(),
            P("tp", "kv"),
            P(("kv", "tp")),
            P(None, "kv", "tp", None),
            P(None, "kv", "tp", None),
            P(None, "kv", "tp"),
            P(),
            P(),
            P(),
        ),
        out_specs=(
            P(None, None, ("kv", "tp")),
            P(None, "kv", "tp", None),
            P(None, "kv", "tp", None),
            P(None, "kv", "tp"),
        ),
        check_vma=False,
    )
```

```python
import functools

import jax
import jax.numpy as jnp
from jax import lax
from jax.experimental import pallas as pl
from jax.experimental.pallas import tpu as pltpu
from jax.sharding import PartitionSpec as P

epsilon = 1e-06
floor_value = -1e30


def merged(part, axis, combine):
    gathered = jax.tree.map(lambda a: lax.all_gather(a, axis), part)

    def take(source):
        return jax.tree.map(lambda a: lax.dynamic_index_in_dim(a, source, 0, False), gathered)

    return lax.fori_loop(
        1, lax.axis_size(axis), lambda source, state: combine(state, take(source)), take(0)
    )


def ancestry(parent_ids, members):
    identity = jnp.eye(members, dtype=jnp.float32)
    parent_hot = (
        parent_ids[:, :, None] == jnp.arange(members, dtype=jnp.int32)[None, None, :]
    ).astype(jnp.float32)
    ancestors = jnp.minimum(identity[None] + parent_hot, 1.0)
    for sweep in range(max(1, (members - 1).bit_length())):
        ancestors = jnp.minimum(
            jnp.einsum("bij,bjk->bik", ancestors, ancestors, precision=lax.Precision.HIGHEST), 1.0
        )
    return ancestors


def combine_parts(first, second):
    new_max = jnp.maximum(first[0], second[0])
    first_scale = jnp.exp(first[0] - new_max)
    second_scale = jnp.exp(second[0] - new_max)
    return (
        new_max,
        first[1] * first_scale + second[1] * second_scale,
        first[2] * first_scale[..., None] + second[2] * second_scale[..., None],
        jnp.maximum(first[3], second[3]),
    )


def finish_rows(cache_max, cache_total, cache_values, last_rows, tree_max, tree_total, tree_values):
    shifted = cache_max + last_rows
    top = jnp.maximum(shifted, tree_max)
    cache_scale = jnp.exp(shifted - top)
    tree_scale = jnp.exp(tree_max - top)
    attended = (
        (cache_values * cache_scale[..., None] + tree_values * tree_scale[..., None])
        / (cache_total * cache_scale + tree_total * tree_scale)[..., None]
    ).astype(jnp.bfloat16)
    return attended.reshape(attended.shape[0], attended.shape[1] * attended.shape[2])


def per_device(
    tokens,
    gain_pre,
    w_query,
    w_key,
    w_value,
    w_forget,
    b_forget,
    w_out,
    gain_post,
    key_cache,
    value_cache,
    cum_cache,
    lengths,
    accepted,
    parent,
):
    num_seqs, proposals, model_width = tokens.shape
    kv_rank = lax.axis_index("kv")
    tp_rank = lax.axis_index("tp")
    span = key_cache.shape[1]
    heads_local = key_cache.shape[2]
    head_dim = key_cache.shape[3]
    scale = head_dim ** (-0.5)
    all_rows = num_seqs * proposals
    tok_float = tokens.astype(jnp.float32)
    normed = (
        tok_float
        * lax.rsqrt(jnp.mean(tok_float * tok_float, -1, keepdims=True) + epsilon)
        * gain_pre
    ).astype(jnp.bfloat16)
    flat = normed.reshape(all_rows, model_width)
    weight_rows = w_query.shape[0]
    local_rows = lax.dynamic_slice_in_dim(flat, kv_rank * weight_rows, weight_rows, 1)
    query_part = jnp.dot(local_rows, w_query, preferred_element_type=jnp.float32)
    key_part = jnp.dot(local_rows, w_key, preferred_element_type=jnp.float32)
    value_part = jnp.dot(local_rows, w_value, preferred_element_type=jnp.float32)
    summed = (
        lax.psum(query_part.astype(jnp.bfloat16), "kv").astype(jnp.float32),
        lax.psum(key_part.astype(jnp.bfloat16), "kv").astype(jnp.float32),
        lax.psum(value_part.astype(jnp.bfloat16), "kv").astype(jnp.float32),
    )
    query_flat = summed[0].astype(jnp.bfloat16)
    key_flat = summed[1].astype(jnp.bfloat16)
    value_flat = summed[2].astype(jnp.bfloat16)
    query = query_flat.reshape(num_seqs, proposals, heads_local, head_dim)
    key_new = key_flat.reshape(num_seqs, proposals, heads_local, head_dim)
    value_new = value_flat.reshape(num_seqs, proposals, heads_local, head_dim)
    forget_cols = lax.dynamic_slice_in_dim(w_forget, tp_rank * heads_local, heads_local, 1)
    forget_bias = lax.dynamic_slice_in_dim(b_forget, tp_rank * heads_local, heads_local, 0)
    log_forget = jax.nn.log_sigmoid(
        jnp.dot(flat, forget_cols, preferred_element_type=jnp.float32) + forget_bias
    ).reshape(num_seqs, proposals, heads_local)
    ancestors = ancestry(parent, proposals)
    path = jnp.einsum("bij,bjh->bih", ancestors, log_forget, precision=lax.Precision.HIGHEST)
    valid = lengths + accepted
    positions = kv_rank * span + jnp.arange(span, dtype=jnp.int32)
    live = (positions[None, :] < valid[:, None])[:, None, None, :]
    score = (
        jnp.einsum("bihd,bkhd->bihk", query, key_cache, preferred_element_type=jnp.float32) * scale
        + path[..., None]
        - jnp.swapaxes(cum_cache, 1, 2)[:, None]
    )
    block_max = jnp.max(jnp.where(live, score, floor_value), axis=-1)
    weight = jnp.exp(jnp.where(live, score - block_max[..., None], floor_value))
    block_total = jnp.sum(weight, axis=-1)
    block_values = jnp.einsum(
        "bihk,bkhd->bihd",
        weight.astype(jnp.bfloat16),
        value_cache,
        preferred_element_type=jnp.float32,
    )
    owner = positions[None, :] == (valid - 1)[:, None]
    candidate = jnp.max(jnp.where(owner[:, :, None], cum_cache, floor_value), axis=1)
    tree_mask = (ancestors > 0.5)[:, :, None, :]
    tree_score = (
        jnp.einsum("bihd,bjhd->bihj", query, key_new, preferred_element_type=jnp.float32) * scale
        + path[..., None]
        - jnp.swapaxes(path, 1, 2)[:, None]
    )
    tree_max = jnp.max(jnp.where(tree_mask, tree_score, floor_value), axis=-1)
    tree_weight = jnp.exp(jnp.where(tree_mask, tree_score - tree_max[..., None], floor_value))
    tree_total = jnp.sum(tree_weight, axis=-1)
    tree_values = jnp.einsum(
        "bihj,bjhd->bihd",
        tree_weight.astype(jnp.bfloat16),
        value_new,
        preferred_element_type=jnp.float32,
    )
    tree_max_rows = tree_max.reshape(all_rows, heads_local)
    tree_total_rows = tree_total.reshape(all_rows, heads_local)
    tree_values_rows = tree_values.reshape(all_rows, heads_local, head_dim)
    cache_max, cache_total, cache_values, last_cum = merged(
        (block_max, block_total, block_values, candidate), "kv", combine_parts
    )
    last_rows = jnp.broadcast_to(last_cum[:, None, :], (num_seqs, proposals, heads_local)).reshape(
        all_rows, heads_local
    )
    attended = finish_rows(
        cache_max.reshape(all_rows, heads_local),
        cache_total.reshape(all_rows, heads_local),
        cache_values.reshape(all_rows, heads_local, head_dim),
        last_rows,
        tree_max_rows,
        tree_total_rows,
        tree_values_rows,
    )
    mixed_part = jnp.dot(attended, w_out, preferred_element_type=jnp.float32)
    mixed_sum = lax.psum_scatter(
        mixed_part.astype(jnp.bfloat16), "tp", scatter_dimension=1, tiled=True
    ).astype(jnp.float32)
    squares = lax.psum(jnp.sum(mixed_sum * mixed_sum, axis=1), ("kv", "tp"))
    mixed = (mixed_sum * lax.rsqrt(squares / model_width + epsilon)[:, None] * gain_post).astype(
        jnp.bfloat16
    )
    mixed = mixed.reshape(num_seqs, proposals, mixed_sum.shape[1])
    relative = positions[None, :] - valid[:, None]
    select = relative[:, :, None] == jnp.arange(proposals, dtype=jnp.int32)[None, None, :]
    written = (relative >= 0) & (relative < proposals)
    placed_keys = jnp.einsum(
        "bkj,bjhd->bkhd", select.astype(jnp.bfloat16), key_new, preferred_element_type=jnp.float32
    ).astype(jnp.bfloat16)
    placed_values = jnp.einsum(
        "bkj,bjhd->bkhd", select.astype(jnp.bfloat16), value_new, preferred_element_type=jnp.float32
    ).astype(jnp.bfloat16)
    key_out = jnp.where(written[:, :, None, None], placed_keys, key_cache)
    value_out = jnp.where(written[:, :, None, None], placed_values, value_cache)
    cum_new = last_cum[:, None, :] + path
    placed_cum = jnp.einsum(
        "bkj,bjh->bkh", select.astype(jnp.float32), cum_new, precision=lax.Precision.HIGHEST
    )
    cum_out = jnp.where(written[:, :, None], placed_cum, cum_cache)
    return (mixed, key_out, value_out, cum_out)


MESH = pl.DeviceIdType.MESH
HI = lax.Precision.HIGHEST
F32 = jnp.float32
BF = jnp.bfloat16


def iota(shape, dim):
    return lax.broadcasted_iota(jnp.int32, shape, dim)


def hot(mask):
    return jnp.where(mask, 1.0, 0.0).astype(F32)


def dot_hi(a, b, dims=(((1,), (0,)), ((), ()))):
    return lax.dot_general(a, b, dims, precision=HI, preferred_element_type=F32)


NT = (((1,), (1,)), ((), ()))


def flips(value, count):
    bit = 1
    out = [value]
    while bit < count:
        step = bit * (1 - 2 * lax.rem(lax.div(value, bit), 2))
        out = out + [other + step for other in out]
        bit *= 2
    return out


def layer_kernel(
    n,
    nt,
    num_seqs,
    prop,
    heads,
    hd,
    span,
    tok_h,
    gain_h,
    wq_h,
    wk_h,
    wv_h,
    wft_h,
    bias_h,
    wo_h,
    gpost_h,
    kc_h,
    vc_h,
    cum_h,
    lens_h,
    accs_h,
    parent_h,
    mixed_out,
    cum_out,
    knew_out,
    vnew_out,
    kcv,
    vcv,
    tokv,
    gain,
    wqkv,
    wft,
    bias,
    wov,
    gpost,
    cum,
    lens,
    accs,
    parent,
    ssq,
    invv,
    xraw,
    xloc,
    part_q,
    q_y,
    q_zs,
    q_zr,
    q_full,
    part_kv,
    kv_y,
    kv_zs,
    kv_zr,
    kv_full,
    st_send,
    val_send,
    st_recv,
    val_recv,
    cand_send,
    cand_recv,
    brow,
    anc,
    tpath,
    ptile,
    att,
    o_send,
    o_recv,
    sq_send,
    sq_recv,
    loc,
    ssem,
    rsem,
):
    me = lax.axis_index("kv")
    mt = lax.axis_index("tp")
    rows, width = tokv.shape
    hw = heads * hd
    kdim = wq_h.shape[0]
    cols = heads * span
    sp = num_seqs // n
    R = sp * prop
    hp = heads * prop
    L = sp * hp
    scale = hd ** (-0.5)
    base = me * span
    heads_all = wft.shape[0]
    half = n // 2
    everyone = n * nt

    barrier = pltpu.get_barrier_semaphore()

    kvs = flips(me, n)
    tps = flips(mt, nt)

    mine = pl.ds(pl.multiple_of(me * kdim, kdim), kdim)
    loads = [
        (tok_h.at[:, mine], xraw),
        (wq_h, wqkv.at[0]),
        (gain_h, gain),
        (wk_h, wqkv.at[1]),
        (wv_h, wqkv.at[2]),
        (tok_h, tokv),
        (lens_h, lens),
        (accs_h, accs),
        (cum_h, cum),
        (parent_h, parent),
        (wft_h, wft),
        (bias_h, bias),
        (gpost_h, gpost),
        (kc_h, kcv),
        (vc_h, vcv),
        (wo_h, wov),
    ]
    copies = [pltpu.make_async_copy(src, dst, loc.at[i]) for i, (src, dst) in enumerate(loads)]
    (
        in_x,
        in_wq,
        in_gain,
        in_wk,
        in_wv,
        in_tok,
        in_lens,
        in_accs,
        in_cum,
        in_parent,
        in_wft,
        in_bias,
        in_gpost,
        in_kc,
        in_vc,
        in_wo,
    ) = copies
    urgent = 5
    for c in copies[:urgent]:
        c.start()
    for e in range(1, everyone):
        pl.semaphore_signal(
            barrier,
            inc=1,
            device_id={"kv": kvs[e // nt], "tp": tps[e % nt]},
            device_id_type=MESH,
        )

    def send(kind, slot, device, src, dst):
        return pltpu.make_async_remote_copy(
            src_ref=src,
            dst_ref=dst,
            send_sem=ssem.at[kind],
            recv_sem=rsem.at[slot],
            device_id=device,
            device_id_type=MESH,
        )

    def to_kv(kind, slot, mask, src, dst):
        return send(kind, slot, {"kv": kvs[mask]}, src, dst)

    def rrow(i):
        return pl.ds(pl.multiple_of(i * R, R), R)

    def spread_to(kind, slot, mask, ref, rank):
        return to_kv(kind, slot, mask, ref.at[rrow(rank)], ref.at[rrow(rank)])

    def sent(kind, ref):
        to_kv(kind, 0, 1, ref, ref).wait_send()

    def received(slot, ref):
        to_kv(0, slot, 1, ref, ref).wait_recv()

    flat = [0]

    def slots(count):
        flat[0] += count
        return flat[0] - count

    on_qy, on_qz, on_ky, on_kz = slots(half), slots(1), slots(half), slots(2)
    on_qag, on_cand, on_stat, on_val = slots(n), slots(1), slots(1), slots(n)
    on_att, on_kvag, on_o, on_sq = slots(n), slots(n), slots(2), slots(1)
    last = n - 1

    def q_yrs(m):
        return to_kv(0, on_qy + m // 2, 1, part_q.at[rrow(kvs[m + 1])], q_y.at[m // 2])

    def q_zrs(m):
        return to_kv(1, on_qz, m, q_zs.at[m // 2], q_zr.at[m // 2])

    def kv_yrs(m):
        src = part_kv.at[rrow(kvs[(m + 1) ^ last])]
        return to_kv(2, on_ky + m // 2, 1, src, kv_y.at[m // 2])

    def kv_near():
        return to_kv(3, on_kz, 2, kv_zs.at[pl.ds(0, 2)], kv_zr.at[pl.ds(0, 2)])

    def kv_far():
        return to_kv(4, on_kz + 1, half, kv_zs.at[2], kv_zr.at[2])

    def q_ag(m):
        if m % 2:
            return spread_to(5, on_qag + m, 1, q_full, kvs[m - 1])
        return spread_to(5, on_qag + m, m, q_full, me)

    def cand_copy(m):
        return to_kv(6, on_cand, m, cand_send, cand_recv.at[m])

    def stat_copy(m):
        return to_kv(7, on_stat, m, st_send.at[m], st_recv.at[m])

    def val_copy(m):
        return to_kv(8, on_val + m, m, val_send.at[m], val_recv.at[m])

    def att_ag(m):
        if m % 2:
            return spread_to(9, on_att + m, 1, att, kvs[(m - 1) ^ last])
        return spread_to(9, on_att + m, m, att, kvs[last])

    def kv_cross():
        return spread_to(10, on_kvag + half, half, kv_full, kvs[last])

    def kv_pass(m):
        return spread_to(10, on_kvag + m, half // 2, kv_full, kvs[(m - half // 2) ^ last])

    def kv_side(m):
        return spread_to(10, on_kvag + m, 1, kv_full, kvs[(m - 1) ^ last])

    def each(count, fn):
        for d in range(1, count):
            fn(d)

    def each_far(count, fn):
        for d in range(count - 1, 0, -1):
            fn(d)

    def scaled(total, rank):
        inv = invv[rrow(rank)]
        return jnp.concatenate(
            [
                total[:, j * lanes : (j + 1) * lanes] * inv
                for j in range(total.shape[1] // lanes)
            ],
            axis=1,
        )

    zmasks = list(range(2, n, 2))
    nb = prop
    lanes = 128

    def sum_rows(i, c):
        sl = pl.ds(pl.multiple_of(i * nb, nb), nb)
        accs4 = [None] * 4
        for j in range(width // lanes):
            t = tokv[sl, j * lanes : (j + 1) * lanes].astype(F32)
            p = t * t
            accs4[j % 4] = p if accs4[j % 4] is None else accs4[j % 4] + p
        ssq[sl, :] = (accs4[0] + accs4[1]) + (accs4[2] + accs4[3])
        return c

    in_x.wait()
    in_gain.wait()
    xloc[...] = (xraw[...].astype(F32) * gain[:, mine]).astype(BF)
    in_wq.wait()
    part_q[...] = jnp.dot(xloc[...], wqkv[0], preferred_element_type=F32).astype(BF)
    pl.semaphore_wait(barrier, everyone - 1)
    for m in zmasks[::-1] + [0]:
        q_yrs(m).start()
    for c in copies[urgent:]:
        c.start()
    in_wk.wait()
    in_wv.wait()
    part_kv[:, 0:hw] = jnp.dot(xloc[...], wqkv[1], preferred_element_type=F32).astype(BF)
    part_kv[:, hw : 2 * hw] = jnp.dot(xloc[...], wqkv[2], preferred_element_type=F32).astype(BF)
    def kv_sum(m):
        return part_kv[rrow(kvs[m ^ last])].astype(F32) + kv_y[m // 2].astype(F32)
    for m in zmasks[::-1] + [0]:
        kv_yrs(m).start()
    in_lens.wait()
    in_accs.wait()
    in_cum.wait()
    r64 = num_seqs * heads
    c64 = cum[...]
    srow = iota((r64, span), 0) // heads
    lane = iota((r64, span), 1)
    rel64 = jnp.zeros((r64, span), jnp.int32)
    rel16 = jnp.zeros((num_seqs, cols), jnp.int32)
    s16 = iota((num_seqs, cols), 0)
    for s in range(num_seqs):
        rel_s = lens[s] + accs[s] - base
        rel64 = jnp.where(srow == s, rel_s, rel64)
        rel16 = jnp.where(s16 == s, rel_s, rel16)
    cand = jnp.max(jnp.where(lane == rel64 - 1, c64, floor_value), axis=1, keepdims=True)
    diag = iota((r64, 128), 0) == iota((r64, 128), 1)
    cand_send[...] = jnp.sum(jnp.where(diag, cand, 0.0), axis=0, keepdims=True)
    each_far(n, lambda m: cand_copy(m).start())

    spread = hot(iota((span, cols), 1) // heads == iota((span, cols), 0))
    e1 = dot_hi(c64, spread)
    e1 = jnp.where(iota((r64, cols), 0) % heads == iota((r64, cols), 1) % heads, e1, 0.0)
    take = hot(iota((num_seqs, r64), 1) // heads == iota((num_seqs, r64), 0))
    cflat = dot_hi(take, e1)
    brow[...] = jnp.where(iota((num_seqs, cols), 1) // heads < rel16, -cflat, floor_value)
    for m in zmasks[::-1]:
        q_yrs(m).wait_recv()
        q_zs[m // 2] = (part_q[rrow(kvs[m])].astype(F32) + q_y[m // 2].astype(F32)).astype(BF)
        q_zrs(m).start()
    in_tok.wait()
    lax.fori_loop(0, rows // nb, sum_rows, 0)
    total = dot_hi(ssq[...], jnp.ones((lanes, lanes), F32))
    invv[...] = lax.rsqrt(total / width + epsilon)
    in_parent.wait()
    ri = iota((rows, rows), 0)
    ci = iota((rows, rows), 1)
    pick = hot(iota((rows, num_seqs), 0) // prop == iota((rows, num_seqs), 1))
    pb = dot_hi(pick, parent[...].astype(F32))
    pcol = jnp.sum(
        jnp.where(iota((rows, prop), 1) == iota((rows, prop), 0) % prop, pb, 0.0),
        axis=1,
        keepdims=True,
    )
    target = jnp.where(pcol >= 0.0, (ri // prop * prop).astype(F32) + pcol, -1.0)
    a = jnp.where((ri == ci) | (ci.astype(F32) == target), 1.0, 0.0)
    for sweep in range(max(1, (prop - 1).bit_length())):
        low = a.astype(BF)
        a = jnp.minimum(jnp.dot(low, low, preferred_element_type=F32), 1.0)
    anc[...] = a
    q_yrs(0).wait_recv()
    own = part_q[rrow(me)].astype(F32) + q_y[0].astype(F32)
    received(on_qz, q_zr.at[pl.ds(1, half - 1)])
    for m in zmasks:
        own = own + q_zr[m // 2].astype(F32)
    q_full[rrow(me)] = scaled(own, me).astype(BF)
    for m in [1] + zmasks[::-1]:
        q_ag(m).start()
    same_head = iota((hp, cols), 0) // prop == iota((hp, cols), 1) % heads
    diag_l = iota((L, L), 0) == iota((L, L), 1)

    def heads_of(ref, s, first):
        block = ref[pl.ds(pl.multiple_of(s * prop, prop), prop), first : first + hw]
        return jnp.concatenate([block[:, h * hd : (h + 1) * hd] for h in range(heads)], axis=0)

    def block_part(src):
        maxes, totals, values = [], [], []
        for j in range(sp):
            s = src * sp + j
            q = heads_of(q_full, s, 0)
            sc = lax.dot_general(q, kcv[s], NT, preferred_element_type=F32) * scale
            sc = jnp.where(same_head, sc + brow[pl.ds(s, 1), :], floor_value)
            m = jnp.max(sc, axis=1, keepdims=True)
            w = jnp.exp(sc - m)
            maxes.append(m)
            totals.append(jnp.sum(w, axis=1, keepdims=True))
            values.append(
                jnp.dot(w.astype(BF), vcv[s], preferred_element_type=F32).astype(BF)
            )
        m = jnp.concatenate(maxes, axis=0)
        t = jnp.concatenate(totals, axis=0)
        m_lane = jnp.sum(jnp.where(diag_l, m, 0.0), axis=0, keepdims=True)
        t_lane = jnp.sum(jnp.where(diag_l, t, 0.0), axis=0, keepdims=True)
        stats = jnp.where(iota((2, L), 0) == 0, m_lane, t_lane)
        return stats, jnp.concatenate(values, axis=0)

    def blocks(masks):
        parts = [block_part(kvs[m]) for m in masks]
        for m, (stats, values) in zip(masks, parts):
            if m == last:
                st_recv[0] = stats
                val_recv[0] = values
            else:
                st_send[last - m] = stats
                val_send[last - m] = values
        for m in masks:
            if m != last:
                stat_copy(last - m).start()
                val_copy(last - m).start()
    def take_q(m):
        q_ag(m).wait_recv()
        if m % 2 == 0:
            q_ag(m + 1).start()
    in_kc.wait()
    in_vc.wait()
    blocks([0])
    for i, m in enumerate((2, 6)):
        kv_yrs(m).wait_recv()
        kv_zs[i] = kv_sum(m).astype(BF)
    kv_near().start()
    in_wft.wait()
    in_bias.wait()
    wscaled = wft[...].astype(F32) * gain[...]
    whigh = wscaled.astype(BF)
    wlow = (wscaled - whigh.astype(F32)).astype(BF)
    lf = lax.dot_general(
        jnp.concatenate([whigh, wlow], axis=0), tokv[...], NT, preferred_element_type=F32
    )
    lf = lf[0:heads_all] + lf[heads_all : 2 * heads_all]
    inv_lane = dot_hi(jnp.full((8, lanes), 1.0 / lanes, F32), invv[...], NT)[0:1]
    bcol = jnp.zeros((heads_all, rows), F32)
    for h in range(heads_all):
        bcol = jnp.where(iota((heads_all, rows), 0) == h, bias[h], bcol)
    z = lf * inv_lane + bcol
    lf = jnp.minimum(z, 0.0) - jnp.log1p(jnp.exp(-jnp.abs(z)))
    path_t = dot_hi(lf, a, NT)
    rep = hot(iota((r64, heads_all), 1) == mt * heads + iota((r64, heads_all), 0) % heads)
    pm = dot_hi(rep, path_t)
    pm = jnp.where(iota((r64, rows), 1) // prop == iota((r64, rows), 0) // heads, pm, 0.0)
    fold = hot(iota((rows, 128), 0) % prop == iota((rows, 128), 1) % prop)
    pt = dot_hi(pm, fold)
    ptile[...] = pt
    ptm = jnp.where((iota((r64, 128), 1) // prop) % heads == iota((r64, 128), 0) % heads, pt, 0.0)
    tpath[...] = dot_hi(take, ptm)
    take_q(2)
    take_q(1)
    blocks([1, 2])
    take_q(4)
    take_q(6)
    blocks([4, 6])
    kv_yrs(4).wait_recv()
    kv_near().wait_recv()
    kv_zs[2] = (kv_sum(4) + kv_zr[1].astype(F32)).astype(BF)
    kv_far().start()
    take_q(3)
    take_q(5)
    blocks([3, 5])
    take_q(7)
    blocks([7])


    kv_yrs(0).wait_recv()
    kv_far().wait_recv()
    own = kv_sum(0) + kv_zr[0].astype(F32) + kv_zr[2].astype(F32)
    kv_full[rrow(kvs[last])] = scaled(own, kvs[last]).astype(BF)

    fold_h = iota((rows, hp), 0)
    tmax, ttot, tval = [], [], []
    for j in range(sp):
        s = kvs[last] * sp + j
        q = heads_of(q_full, s, 0)
        k = heads_of(kv_full, s, 0)
        v = heads_of(kv_full, s, hw)
        arows = anc[pl.ds(pl.multiple_of(s * prop, prop), prop), :]
        sel = hot(fold_h == s * prop + iota((rows, hp), 1) % prop).astype(BF)
        am = jnp.dot(arows.astype(BF), sel, preferred_element_type=F32)
        am = jnp.concatenate([am] * heads, axis=0)
        mask = (am > 0.5) & (iota((hp, hp), 0) // prop == iota((hp, hp), 1) // prop)
        sc = lax.dot_general(q, k, NT, preferred_element_type=F32) * scale
        sc = jnp.where(mask, sc - tpath[pl.ds(s, 1), 0:hp], floor_value)
        m = jnp.max(sc, axis=1, keepdims=True)
        w = jnp.where(mask, jnp.exp(sc - m), 0.0)
        tmax.append(m)
        ttot.append(jnp.sum(w, axis=1, keepdims=True))
        tval.append(jnp.dot(w.astype(BF), v, preferred_element_type=F32))
    tree_max = jnp.concatenate(tmax, axis=0)
    tree_tot = jnp.concatenate(ttot, axis=0)
    tree_val = jnp.concatenate(tval, axis=0)

    last_lane = cand_send[...]
    received(on_cand, cand_recv.at[pl.ds(1, n - 1)])
    for m in range(1, n):
        last_lane = jnp.maximum(last_lane, cand_recv[m])
    own_rows = iota((L, 128), 0)
    own_head = (kvs[last] * sp + own_rows // hp) * heads + (own_rows % hp) // prop
    own_pick = iota((L, 128), 1) == own_head
    last_own = jnp.sum(jnp.where(own_pick, last_lane, 0.0), axis=1, keepdims=True)

    received(on_stat, st_recv.at[pl.ds(1, n - 1)])
    top = st_recv[0, 0:1]
    for m in range(1, n):
        top = jnp.maximum(top, st_recv[m, 0:1])

    def col(x):
        return jnp.sum(jnp.where(diag_l, x, 0.0), axis=1, keepdims=True)

    cache_tot = jnp.zeros((1, L), F32)
    scales = []
    for m in range(n):
        sd = jnp.exp(st_recv[m, 0:1] - top)
        scales.append(col(sd))
        cache_tot = cache_tot + st_recv[m, 1:2] * sd
    shifted = col(top) + last_own
    both = jnp.maximum(shifted, tree_max)
    cscale = jnp.exp(shifted - both)
    tscale = jnp.exp(tree_max - both)
    denom = col(cache_tot) * cscale + tree_tot * tscale
    vals = val_recv[0].astype(F32) * scales[0]
    for m in range(1, n):
        val_copy(m).wait_recv()
        vals = vals + val_recv[m].astype(F32) * scales[m]
    attended = ((vals * cscale + tree_val * tscale) / denom).astype(BF)
    for j in range(sp):
        for h in range(heads):
            att[pl.ds(pl.multiple_of(kvs[last] * R + j * prop, prop), prop), h * hd : (h + 1) * hd] = (
                attended[j * hp + h * prop : j * hp + (h + 1) * prop]
            )
    for m in [1] + zmasks[::-1]:
        att_ag(m).start()

    upper = me >= half

    @pl.when(upper)
    def _():
        kv_pass(2).start()
        kv_side(1).start()

    @pl.when(jnp.logical_not(upper))
    def _():
        kv_cross().start()

    last_col = jnp.sum(jnp.where(diag, last_lane, 0.0), axis=1, keepdims=True)
    shifted_path = ptile[...]
    for b in range((span - 1).bit_length()):
        moved = pltpu.roll(shifted_path, 1 << b, 1)
        shifted_path = jnp.where((rel64 >> b) & 1 == 1, moved, shifted_path)
    off = lane - rel64
    cum_out[...] = jnp.where((off >= 0) & (off < prop), last_col + shifted_path, c64)

    in_wo.wait()
    oc = o_send.shape[2]
    near = half * R - lax.div(me, half) * (half * R)
    grows = [
        pl.ds(pl.multiple_of(first, half * R), half * R) for first in (near, half * R - near)
    ]

    def o_copy(g, d):
        return send(
            11,
            on_o + g,
            {"tp": tps[d]},
            o_send.at[tps[d], grows[g]],
            o_recv.at[d, grows[g]],
        )

    for m in zmasks:
        att_ag(m).wait_recv()
        att_ag(m + 1).start()
    for g in range(2):
        for m in range(1 + g * half, (g + 1) * half, 2):
            att_ag(m).wait_recv()
        full = jnp.dot(att[grows[g]], wov[...], preferred_element_type=F32).astype(BF)
        for t in range(nt):
            o_send[t, grows[g]] = full[:, t * oc : (t + 1) * oc]
        each_far(nt, lambda d: o_copy(g, d).start())

    @pl.when(upper)
    def _():
        kv_cross().wait_recv()
        kv_pass(6).start()
        kv_side(5).start()
        kv_pass(2).wait_recv()
        kv_side(3).start()

    mixed = o_send[mt].astype(F32)
    for g in range(2):
        received(on_o + g, o_recv.at[pl.ds(1, nt - 1), grows[g]])
    for d in range(1, nt):
        mixed = mixed + o_recv[d].astype(F32)
    sq = dot_hi(jnp.ones((8, oc), F32), mixed * mixed, NT)[0:1]
    sq_send[...] = sq

    def sq_copy(e):
        peer = {"kv": kvs[e // nt], "tp": tps[e % nt]}
        return send(12, on_sq, peer, sq_send, sq_recv.at[e])

    each_far(everyone, lambda e: sq_copy(e).start())

    order = hot(
        iota((hp, hp), 1) == iota((hp, hp), 0) % heads * prop + iota((hp, hp), 0) // heads
    ).astype(BF)

    unroll = 4

    @pl.when(upper)
    def _():
        kv_pass(6).wait_recv()
        kv_side(7).start()
        for m in range(1, n, 2):
            kv_side(m).wait_recv()

        def some(i, c):
            fresh = [
                heads_of(kv_full, i * unroll + j, first) for j in range(unroll) for first in (0, hw)
            ]
            placed = jnp.dot(
                order, jnp.concatenate(fresh, axis=1), preferred_element_type=F32
            ).astype(BF)
            for j in range(unroll):
                at = 2 * j * hd
                knew_out[i * unroll + j] = placed[:, at : at + hd]
                vnew_out[i * unroll + j] = placed[:, at + hd : at + 2 * hd]
            return c

        lax.fori_loop(0, num_seqs // unroll, some, 0)

    received(on_sq, sq_recv.at[pl.ds(1, everyone - 1)])
    for e in range(1, everyone):
        sq = sq + sq_recv[e]
    ssum = dot_hi(
        jnp.broadcast_to(sq, (8, rows)), jnp.full((8, oc), 0.125, F32), (((0,), (0,)), ((), ()))
    )
    in_gpost.wait()
    mixed_out[...] = (mixed * lax.rsqrt(ssum / width + epsilon) * gpost[...]).astype(BF)

    sent(0, q_y)
    sent(1, q_zr.at[pl.ds(1, half - 1)])
    sent(2, kv_y)
    sent(3, kv_zr.at[pl.ds(0, 2)])
    sent(4, kv_zr.at[2])
    sent(5, q_full.at[pl.ds(0, last * R)])
    sent(6, cand_recv.at[pl.ds(1, last)])
    sent(7, st_recv.at[pl.ds(1, last)])
    sent(8, val_recv.at[pl.ds(1, last)])
    sent(9, att.at[pl.ds(0, last * R)])

    @pl.when(upper)
    def _():
        sent(10, kv_full.at[pl.ds(0, (2 + half) * R)])

    @pl.when(jnp.logical_not(upper))
    def _():
        sent(10, kv_full.at[pl.ds(0, R)])

    sent(11, o_recv.at[pl.ds(1, nt - 1)])
    sent(12, sq_recv.at[pl.ds(1, everyone - 1)])


def patch_kernel(
    n,
    prop,
    k_in,
    v_in,
    knew,
    vnew,
    mixed,
    cum,
    lens,
    accs,
    k_out,
    v_out,
    mixed_out,
    cum_out,
    k_buf,
    v_buf,
    sem,
):
    me = lax.axis_index("kv")
    num_seqs, span = k_out.shape[:2]
    out_m = pltpu.make_async_copy(mixed, mixed_out, sem.at[0])
    out_c = pltpu.make_async_copy(cum, cum_out, sem.at[1])
    out_m.start()
    out_c.start()

    def store(s):
        pltpu.make_async_copy(k_buf.at[s], k_out.at[s], sem.at[2]).start()
        pltpu.make_async_copy(v_buf.at[s], v_out.at[s], sem.at[3]).start()

    def place(s):
        at = lens[s] + accs[s] - me * span

        @pl.when((at >= 0) & (at <= span - prop))
        def _():
            k_buf[s, pl.ds(at, prop)] = knew[s]
            v_buf[s, pl.ds(at, prop)] = vnew[s]

        @pl.when(((at > -prop) & (at < 0)) | ((at > span - prop) & (at < span)))
        def _():
            def one(j, c):
                @pl.when((at + j >= 0) & (at + j < span))
                def _():
                    k_buf[s, pl.ds(at + j, 1)] = knew[s, pl.ds(j, 1)]
                    v_buf[s, pl.ds(at + j, 1)] = vnew[s, pl.ds(j, 1)]

                return c

            lax.fori_loop(0, prop, one, 0)

    @pl.when(me >= n // 2)
    def _():
        for s in range(num_seqs):
            place(s)
            if s > 0:
                store(s - 1)
        store(num_seqs - 1)

    @pl.when(me < n // 2)
    def _():
        for s in range(num_seqs):
            store(s)

    pltpu.make_async_copy(k_buf, k_out, sem.at[2]).wait()
    pltpu.make_async_copy(v_buf, v_out, sem.at[3]).wait()
    out_m.wait()
    out_c.wait()


def fast_device(
    n,
    nt,
    tokens,
    gain_pre,
    w_query,
    w_key,
    w_value,
    w_forget,
    b_forget,
    w_out,
    gain_post,
    key_cache,
    value_cache,
    cum_cache,
    lengths,
    accepted,
    parent,
):
    num_seqs, prop, width = tokens.shape
    span, heads, hd = key_cache.shape[1:]
    rows = num_seqs * prop
    hw = heads * hd
    cols = heads * span
    sp = num_seqs // n
    R = sp * prop
    L = sp * heads * prop
    oc = gain_post.shape[0]
    half = n // 2
    everyone = n * nt
    kc = key_cache.reshape(num_seqs, cols, hd)
    vc = value_cache.reshape(num_seqs, cols, hd)
    cum = jnp.swapaxes(cum_cache, 1, 2).reshape(num_seqs * heads, span)
    hbm = pl.BlockSpec(memory_space=pltpu.HBM)
    vmem = pl.BlockSpec(memory_space=pltpu.VMEM)
    smem = pl.BlockSpec(memory_space=pltpu.SMEM)
    V = pltpu.VMEM
    S = pltpu.SMEM
    D = pltpu.SemaphoreType.DMA
    mixed, cum_new, knew, vnew, kv, vv = pl.pallas_call(
        functools.partial(layer_kernel, n, nt, num_seqs, prop, heads, hd, span),
        out_shape=(
            V((rows, oc), BF),
            V(cum.shape, F32),
            V((num_seqs, heads * prop, hd), BF),
            V((num_seqs, heads * prop, hd), BF),
            V(kc.shape, BF),
            V(vc.shape, BF),
        ),
        in_specs=[hbm] * 15,
        out_specs=(vmem,) * 6,
        scratch_shapes=[
            V((rows, width), BF),
            V((1, width), F32),
            V((3,) + w_query.shape, BF),
            V(w_forget.shape[::-1], BF),
            S(b_forget.shape, F32),
            V(w_out.shape, BF),
            V((1, oc), F32),
            V(cum.shape, F32),
            S(lengths.shape, jnp.int32),
            S(accepted.shape, jnp.int32),
            V(parent.shape, jnp.int32),
            V((rows, 128), F32),
            V((rows, 128), F32),
            V((rows, w_query.shape[0]), BF),
            V((rows, w_query.shape[0]), BF),
            V((rows, hw), BF),
            V((half, R, hw), BF),
            V((half, R, hw), BF),
            V((half, R, hw), BF),
            V((rows, hw), BF),
            V((rows, 2 * hw), BF),
            V((half, R, 2 * hw), BF),
            V((half - 1, R, 2 * hw), BF),
            V((half - 1, R, 2 * hw), BF),
            V((rows, 2 * hw), BF),
            V((n, 2, L), F32),
            V((n, L, hd), BF),
            V((n, 2, L), F32),
            V((n, L, hd), BF),
            V((1, 128), F32),
            V((n, 1, 128), F32),
            V((num_seqs, cols), F32),
            V((rows, rows), F32),
            V((num_seqs, 128), F32),
            V((num_seqs * heads, 128), F32),
            V((rows, hw), BF),
            V((nt, rows, oc), BF),
            V((nt, rows, oc), BF),
            V((1, rows), F32),
            V((everyone, 1, rows), F32),
            D((16,)),
            D((13,)),
            D((2 * half + 4 * n + 8,)),
        ],
        compiler_params=pltpu.CompilerParams(
            collective_id=0, has_side_effects=True, vmem_limit_bytes=50 * 1024 * 1024
        ),
        name="layer",
    )(
        *[
            pltpu.with_memory_space_constraint(operand, pltpu.HBM)
            for operand in (
                tokens.reshape(rows, width),
                gain_pre.reshape(1, width),
                w_query,
                w_key,
                w_value,
                w_forget.T,
                b_forget,
                w_out,
                gain_post.reshape(1, oc),
                kc,
                vc,
                cum,
                lengths,
                accepted,
                parent,
            )
        ]
    )
    fresh = (num_seqs, prop, heads, hd)
    key_out, value_out, mixed, cum_new, *unused = pl.pallas_call(
        functools.partial(patch_kernel, n, prop),
        out_shape=(
            pltpu.HBM(key_cache.shape, BF),
            pltpu.HBM(value_cache.shape, BF),
            pltpu.HBM(mixed.shape, BF),
            pltpu.HBM(cum.shape, F32),
            V(key_cache.shape, BF),
            V(key_cache.shape, BF),
        ),
        in_specs=[vmem, vmem, vmem, vmem, vmem, vmem, smem, smem],
        out_specs=(hbm, hbm, hbm, hbm, vmem, vmem),
        input_output_aliases={0: 4, 1: 5},
        scratch_shapes=[D((4,))],
        compiler_params=pltpu.CompilerParams(
            has_side_effects=True, vmem_limit_bytes=4 * 1024 * 1024
        ),
        name="patch",
    )(
        *[
            pltpu.with_memory_space_constraint(operand, V)
            for operand in (kv.reshape(key_cache.shape), vv.reshape(key_cache.shape), knew.reshape(fresh), vnew.reshape(fresh), mixed, cum_new)
        ],
        lengths,
        accepted,
    )
    cum_out = jnp.swapaxes(cum_new.reshape(num_seqs, heads, span), 1, 2)
    return (
        mixed.reshape(num_seqs, prop, oc),
        key_out.reshape(key_cache.shape),
        value_out.reshape(value_cache.shape),
        cum_out,
    )


def choose(mesh):
    n, nt = mesh.shape["kv"], mesh.shape["tp"]

    def body(*args):
        tokens, key_cache = args[0], args[9]
        num_seqs, prop = tokens.shape[:2]
        span, heads = key_cache.shape[1:3]
        fits = (
            num_seqs % n == 0
            and n == 8
            and nt & (nt - 1) == 0
            and num_seqs % 4 == 0
            and (num_seqs // n) * heads * prop == 128
            and span == 128
            and num_seqs * heads <= 128
            and prop % 16 == 0
        )
        if fits:
            return fast_device(n, nt, *args)
        return per_device(*args)

    return body


def solution(mesh):
    return jax.shard_map(
        choose(mesh),
        mesh=mesh,
        in_specs=(
            P(),
            P(),
            P("kv", "tp"),
            P("kv", "tp"),
            P("kv", "tp"),
            P(),
            P(),
            P("tp", "kv"),
            P(("kv", "tp")),
            P(None, "kv", "tp", None),
            P(None, "kv", "tp", None),
            P(None, "kv", "tp"),
            P(),
            P(),
            P(),
        ),
        out_specs=(
            P(None, None, ("kv", "tp")),
            P(None, "kv", "tp", None),
            P(None, "kv", "tp", None),
            P(None, "kv", "tp"),
        ),
        check_vma=False,
    )
```

```python
import functools

import jax
import jax.numpy as jnp
from jax import lax
from jax.experimental import pallas as pl
from jax.experimental.pallas import tpu as pltpu
from jax.sharding import PartitionSpec as P

epsilon = 1e-06
floor_value = -1e30


def merged(part, axis, combine):
    gathered = jax.tree.map(lambda a: lax.all_gather(a, axis), part)

    def take(source):
        return jax.tree.map(lambda a: lax.dynamic_index_in_dim(a, source, 0, False), gathered)

    return lax.fori_loop(
        1, lax.axis_size(axis), lambda source, state: combine(state, take(source)), take(0)
    )


def ancestry(parent_ids, members):
    identity = jnp.eye(members, dtype=jnp.float32)
    parent_hot = (
        parent_ids[:, :, None] == jnp.arange(members, dtype=jnp.int32)[None, None, :]
    ).astype(jnp.float32)
    ancestors = jnp.minimum(identity[None] + parent_hot, 1.0)
    for sweep in range(max(1, (members - 1).bit_length())):
        ancestors = jnp.minimum(
            jnp.einsum("bij,bjk->bik", ancestors, ancestors, precision=lax.Precision.HIGHEST), 1.0
        )
    return ancestors


def combine_parts(first, second):
    new_max = jnp.maximum(first[0], second[0])
    first_scale = jnp.exp(first[0] - new_max)
    second_scale = jnp.exp(second[0] - new_max)
    return (
        new_max,
        first[1] * first_scale + second[1] * second_scale,
        first[2] * first_scale[..., None] + second[2] * second_scale[..., None],
        jnp.maximum(first[3], second[3]),
    )


def finish_rows(cache_max, cache_total, cache_values, last_rows, tree_max, tree_total, tree_values):
    shifted = cache_max + last_rows
    top = jnp.maximum(shifted, tree_max)
    cache_scale = jnp.exp(shifted - top)
    tree_scale = jnp.exp(tree_max - top)
    attended = (
        (cache_values * cache_scale[..., None] + tree_values * tree_scale[..., None])
        / (cache_total * cache_scale + tree_total * tree_scale)[..., None]
    ).astype(jnp.bfloat16)
    return attended.reshape(attended.shape[0], attended.shape[1] * attended.shape[2])


def per_device(
    tokens,
    gain_pre,
    w_query,
    w_key,
    w_value,
    w_forget,
    b_forget,
    w_out,
    gain_post,
    key_cache,
    value_cache,
    cum_cache,
    lengths,
    accepted,
    parent,
):
    num_seqs, proposals, model_width = tokens.shape
    kv_rank = lax.axis_index("kv")
    tp_rank = lax.axis_index("tp")
    span = key_cache.shape[1]
    heads_local = key_cache.shape[2]
    head_dim = key_cache.shape[3]
    scale = head_dim ** (-0.5)
    all_rows = num_seqs * proposals
    tok_float = tokens.astype(jnp.float32)
    normed = (
        tok_float
        * lax.rsqrt(jnp.mean(tok_float * tok_float, -1, keepdims=True) + epsilon)
        * gain_pre
    ).astype(jnp.bfloat16)
    flat = normed.reshape(all_rows, model_width)
    weight_rows = w_query.shape[0]
    local_rows = lax.dynamic_slice_in_dim(flat, kv_rank * weight_rows, weight_rows, 1)
    query_part = jnp.dot(local_rows, w_query, preferred_element_type=jnp.float32)
    key_part = jnp.dot(local_rows, w_key, preferred_element_type=jnp.float32)
    value_part = jnp.dot(local_rows, w_value, preferred_element_type=jnp.float32)
    summed = (
        lax.psum(query_part.astype(jnp.bfloat16), "kv").astype(jnp.float32),
        lax.psum(key_part.astype(jnp.bfloat16), "kv").astype(jnp.float32),
        lax.psum(value_part.astype(jnp.bfloat16), "kv").astype(jnp.float32),
    )
    query_flat = summed[0].astype(jnp.bfloat16)
    key_flat = summed[1].astype(jnp.bfloat16)
    value_flat = summed[2].astype(jnp.bfloat16)
    query = query_flat.reshape(num_seqs, proposals, heads_local, head_dim)
    key_new = key_flat.reshape(num_seqs, proposals, heads_local, head_dim)
    value_new = value_flat.reshape(num_seqs, proposals, heads_local, head_dim)
    forget_cols = lax.dynamic_slice_in_dim(w_forget, tp_rank * heads_local, heads_local, 1)
    forget_bias = lax.dynamic_slice_in_dim(b_forget, tp_rank * heads_local, heads_local, 0)
    log_forget = jax.nn.log_sigmoid(
        jnp.dot(flat, forget_cols, preferred_element_type=jnp.float32) + forget_bias
    ).reshape(num_seqs, proposals, heads_local)
    ancestors = ancestry(parent, proposals)
    path = jnp.einsum("bij,bjh->bih", ancestors, log_forget, precision=lax.Precision.HIGHEST)
    valid = lengths + accepted
    positions = kv_rank * span + jnp.arange(span, dtype=jnp.int32)
    live = (positions[None, :] < valid[:, None])[:, None, None, :]
    score = (
        jnp.einsum("bihd,bkhd->bihk", query, key_cache, preferred_element_type=jnp.float32) * scale
        + path[..., None]
        - jnp.swapaxes(cum_cache, 1, 2)[:, None]
    )
    block_max = jnp.max(jnp.where(live, score, floor_value), axis=-1)
    weight = jnp.exp(jnp.where(live, score - block_max[..., None], floor_value))
    block_total = jnp.sum(weight, axis=-1)
    block_values = jnp.einsum(
        "bihk,bkhd->bihd",
        weight.astype(jnp.bfloat16),
        value_cache,
        preferred_element_type=jnp.float32,
    )
    owner = positions[None, :] == (valid - 1)[:, None]
    candidate = jnp.max(jnp.where(owner[:, :, None], cum_cache, floor_value), axis=1)
    tree_mask = (ancestors > 0.5)[:, :, None, :]
    tree_score = (
        jnp.einsum("bihd,bjhd->bihj", query, key_new, preferred_element_type=jnp.float32) * scale
        + path[..., None]
        - jnp.swapaxes(path, 1, 2)[:, None]
    )
    tree_max = jnp.max(jnp.where(tree_mask, tree_score, floor_value), axis=-1)
    tree_weight = jnp.exp(jnp.where(tree_mask, tree_score - tree_max[..., None], floor_value))
    tree_total = jnp.sum(tree_weight, axis=-1)
    tree_values = jnp.einsum(
        "bihj,bjhd->bihd",
        tree_weight.astype(jnp.bfloat16),
        value_new,
        preferred_element_type=jnp.float32,
    )
    tree_max_rows = tree_max.reshape(all_rows, heads_local)
    tree_total_rows = tree_total.reshape(all_rows, heads_local)
    tree_values_rows = tree_values.reshape(all_rows, heads_local, head_dim)
    cache_max, cache_total, cache_values, last_cum = merged(
        (block_max, block_total, block_values, candidate), "kv", combine_parts
    )
    last_rows = jnp.broadcast_to(last_cum[:, None, :], (num_seqs, proposals, heads_local)).reshape(
        all_rows, heads_local
    )
    attended = finish_rows(
        cache_max.reshape(all_rows, heads_local),
        cache_total.reshape(all_rows, heads_local),
        cache_values.reshape(all_rows, heads_local, head_dim),
        last_rows,
        tree_max_rows,
        tree_total_rows,
        tree_values_rows,
    )
    mixed_part = jnp.dot(attended, w_out, preferred_element_type=jnp.float32)
    mixed_sum = lax.psum_scatter(
        mixed_part.astype(jnp.bfloat16), "tp", scatter_dimension=1, tiled=True
    ).astype(jnp.float32)
    squares = lax.psum(jnp.sum(mixed_sum * mixed_sum, axis=1), ("kv", "tp"))
    mixed = (mixed_sum * lax.rsqrt(squares / model_width + epsilon)[:, None] * gain_post).astype(
        jnp.bfloat16
    )
    mixed = mixed.reshape(num_seqs, proposals, mixed_sum.shape[1])
    relative = positions[None, :] - valid[:, None]
    select = relative[:, :, None] == jnp.arange(proposals, dtype=jnp.int32)[None, None, :]
    written = (relative >= 0) & (relative < proposals)
    placed_keys = jnp.einsum(
        "bkj,bjhd->bkhd", select.astype(jnp.bfloat16), key_new, preferred_element_type=jnp.float32
    ).astype(jnp.bfloat16)
    placed_values = jnp.einsum(
        "bkj,bjhd->bkhd", select.astype(jnp.bfloat16), value_new, preferred_element_type=jnp.float32
    ).astype(jnp.bfloat16)
    key_out = jnp.where(written[:, :, None, None], placed_keys, key_cache)
    value_out = jnp.where(written[:, :, None, None], placed_values, value_cache)
    cum_new = last_cum[:, None, :] + path
    placed_cum = jnp.einsum(
        "bkj,bjh->bkh", select.astype(jnp.float32), cum_new, precision=lax.Precision.HIGHEST
    )
    cum_out = jnp.where(written[:, :, None], placed_cum, cum_cache)
    return (mixed, key_out, value_out, cum_out)


MESH = pl.DeviceIdType.MESH
HI = lax.Precision.HIGHEST
F32 = jnp.float32
BF = jnp.bfloat16


def iota(shape, dim):
    return lax.broadcasted_iota(jnp.int32, shape, dim)


def hot(mask):
    return jnp.where(mask, 1.0, 0.0).astype(F32)


def dot_hi(a, b, dims=(((1,), (0,)), ((), ()))):
    return lax.dot_general(a, b, dims, precision=HI, preferred_element_type=F32)


NT = (((1,), (1,)), ((), ()))


def flips(value, count):
    bit = 1
    out = [value]
    while bit < count:
        step = bit * (1 - 2 * lax.rem(lax.div(value, bit), 2))
        out = out + [other + step for other in out]
        bit *= 2
    return out


def layer_kernel(
    n,
    nt,
    num_seqs,
    prop,
    heads,
    hd,
    span,
    tok_h,
    gain_h,
    wq_h,
    wk_h,
    wv_h,
    wft_h,
    bias_h,
    wo_h,
    gpost_h,
    kc_h,
    vc_h,
    cum_h,
    lens_h,
    accs_h,
    parent_h,
    mixed_out,
    cum_out,
    knew_out,
    vnew_out,
    kcv,
    vcv,
    at_out,
    tokv,
    gain,
    wqkv,
    wft,
    bias,
    wov,
    gpost,
    cum,
    lens,
    accs,
    parent,
    ssq,
    invv,
    xraw,
    xloc,
    part_q,
    q_y,
    q_zs,
    q_zr,
    q_full,
    part_kv,
    kv_y,
    kv_zs,
    kv_zr,
    kv_full,
    st_send,
    val_send,
    st_recv,
    val_recv,
    cand_send,
    cand_recv,
    brow,
    anc,
    tpath,
    ptile,
    att,
    o_send,
    o_recv,
    sq_send,
    sq_recv,
    loc,
    ssem,
    rsem,
):
    me = lax.axis_index("kv")
    mt = lax.axis_index("tp")
    rows, width = tokv.shape
    hw = heads * hd
    kdim = wq_h.shape[0]
    cols = heads * span
    sp = num_seqs // n
    R = sp * prop
    hp = heads * prop
    L = sp * hp
    scale = hd ** (-0.5)
    base = me * span
    heads_all = wft.shape[0]
    half = n // 2
    everyone = n * nt

    barrier = pltpu.get_barrier_semaphore()

    kvs = flips(me, n)
    tps = flips(mt, nt)

    mine = pl.ds(pl.multiple_of(me * kdim, kdim), kdim)
    loads = [
        (tok_h.at[:, mine], xraw),
        (wq_h, wqkv.at[0]),
        (gain_h, gain),
        (wk_h, wqkv.at[1]),
        (wv_h, wqkv.at[2]),
        (tok_h, tokv),
        (lens_h, lens),
        (accs_h, accs),
        (cum_h, cum),
        (parent_h, parent),
        (wft_h, wft),
        (bias_h, bias),
        (gpost_h, gpost),
        (kc_h, kcv),
        (vc_h, vcv),
        (wo_h, wov),
    ]
    copies = [pltpu.make_async_copy(src, dst, loc.at[i]) for i, (src, dst) in enumerate(loads)]
    (
        in_x,
        in_wq,
        in_gain,
        in_wk,
        in_wv,
        in_tok,
        in_lens,
        in_accs,
        in_cum,
        in_parent,
        in_wft,
        in_bias,
        in_gpost,
        in_kc,
        in_vc,
        in_wo,
    ) = copies
    urgent = 5
    for c in copies[:urgent]:
        c.start()
    for e in range(1, everyone):
        pl.semaphore_signal(
            barrier,
            inc=1,
            device_id={"kv": kvs[e // nt], "tp": tps[e % nt]},
            device_id_type=MESH,
        )

    def send(kind, slot, device, src, dst):
        return pltpu.make_async_remote_copy(
            src_ref=src,
            dst_ref=dst,
            send_sem=ssem.at[kind],
            recv_sem=rsem.at[slot],
            device_id=device,
            device_id_type=MESH,
        )

    def to_kv(kind, slot, mask, src, dst):
        return send(kind, slot, {"kv": kvs[mask]}, src, dst)

    def rrow(i):
        return pl.ds(pl.multiple_of(i * R, R), R)

    def spread_to(kind, slot, mask, ref, rank):
        return to_kv(kind, slot, mask, ref.at[rrow(rank)], ref.at[rrow(rank)])

    def sent(kind, ref):
        to_kv(kind, 0, 1, ref, ref).wait_send()

    def received(slot, ref):
        to_kv(0, slot, 1, ref, ref).wait_recv()

    flat = [0]

    def slots(count):
        flat[0] += count
        return flat[0] - count

    on_qy, on_qz, on_ky, on_kz = slots(half), slots(1), slots(half), slots(2)
    on_qag, on_cand, on_stat, on_val = slots(n), slots(1), slots(1), slots(n)
    on_att, on_kvag, on_o, on_sq = slots(n), slots(n), slots(2), slots(1)
    last = n - 1

    def q_yrs(m):
        return to_kv(0, on_qy + m // 2, 1, part_q.at[rrow(kvs[m + 1])], q_y.at[m // 2])

    def q_zrs(m):
        return to_kv(1, on_qz, m, q_zs.at[m // 2], q_zr.at[m // 2])

    def kv_yrs(m):
        src = part_kv.at[rrow(kvs[(m + 1) ^ last])]
        return to_kv(2, on_ky + m // 2, 1, src, kv_y.at[m // 2])

    def kv_near():
        return to_kv(3, on_kz, 2, kv_zs.at[pl.ds(0, 2)], kv_zr.at[pl.ds(0, 2)])

    def kv_far():
        return to_kv(4, on_kz + 1, half, kv_zs.at[2], kv_zr.at[2])

    def q_ag(m):
        if m % 2:
            return spread_to(5, on_qag + m, 1, q_full, kvs[m - 1])
        return spread_to(5, on_qag + m, m, q_full, me)

    def cand_copy(m):
        return to_kv(6, on_cand, m, cand_send, cand_recv.at[m])

    def stat_copy(m):
        return to_kv(7, on_stat, m, st_send.at[m], st_recv.at[m])

    def val_copy(m):
        return to_kv(8, on_val + m, m, val_send.at[m], val_recv.at[m])

    def att_ag(m):
        if m % 2:
            return spread_to(9, on_att + m, 1, att, kvs[(m - 1) ^ last])
        return spread_to(9, on_att + m, m, att, kvs[last])

    def kv_cross():
        return spread_to(10, on_kvag + half, half, kv_full, kvs[last])

    def kv_pass(m):
        return spread_to(10, on_kvag + m, half // 2, kv_full, kvs[(m - half // 2) ^ last])

    def kv_side(m):
        return spread_to(10, on_kvag + m, 1, kv_full, kvs[(m - 1) ^ last])

    def each(count, fn):
        for d in range(1, count):
            fn(d)

    def each_far(count, fn):
        for d in range(count - 1, 0, -1):
            fn(d)

    def scaled(total, rank):
        inv = invv[rrow(rank)]
        return jnp.concatenate(
            [
                total[:, j * lanes : (j + 1) * lanes] * inv
                for j in range(total.shape[1] // lanes)
            ],
            axis=1,
        )

    zmasks = list(range(2, n, 2))
    nb = prop
    lanes = 128

    def sum_rows(i, c):
        sl = pl.ds(pl.multiple_of(i * nb, nb), nb)
        accs4 = [None] * 4
        for j in range(width // lanes):
            t = tokv[sl, j * lanes : (j + 1) * lanes].astype(F32)
            p = t * t
            accs4[j % 4] = p if accs4[j % 4] is None else accs4[j % 4] + p
        ssq[sl, :] = (accs4[0] + accs4[1]) + (accs4[2] + accs4[3])
        return c

    in_x.wait()
    in_gain.wait()
    xloc[...] = (xraw[...].astype(F32) * gain[:, mine]).astype(BF)
    in_wq.wait()
    part_q[...] = jnp.dot(xloc[...], wqkv[0], preferred_element_type=F32).astype(BF)
    pl.semaphore_wait(barrier, everyone - 1)
    for m in zmasks[::-1] + [0]:
        q_yrs(m).start()
    for c in copies[urgent:]:
        c.start()
    in_wk.wait()
    in_wv.wait()
    part_kv[:, 0:hw] = jnp.dot(xloc[...], wqkv[1], preferred_element_type=F32).astype(BF)
    part_kv[:, hw : 2 * hw] = jnp.dot(xloc[...], wqkv[2], preferred_element_type=F32).astype(BF)
    def kv_sum(m):
        return part_kv[rrow(kvs[m ^ last])].astype(F32) + kv_y[m // 2].astype(F32)
    for m in zmasks[::-1] + [0]:
        kv_yrs(m).start()
    in_lens.wait()
    in_accs.wait()
    in_cum.wait()
    r64 = num_seqs * heads
    c64 = cum[...]
    srow = iota((r64, span), 0) // heads
    lane = iota((r64, span), 1)
    rel64 = jnp.zeros((r64, span), jnp.int32)
    rel16 = jnp.zeros((num_seqs, cols), jnp.int32)
    s16 = iota((num_seqs, cols), 0)
    for s in range(num_seqs):
        rel_s = lens[s] + accs[s] - base
        at_out[s] = rel_s
        rel64 = jnp.where(srow == s, rel_s, rel64)
        rel16 = jnp.where(s16 == s, rel_s, rel16)
    cand = jnp.max(jnp.where(lane == rel64 - 1, c64, floor_value), axis=1, keepdims=True)
    diag = iota((r64, 128), 0) == iota((r64, 128), 1)
    cand_send[...] = jnp.sum(jnp.where(diag, cand, 0.0), axis=0, keepdims=True)
    each_far(n, lambda m: cand_copy(m).start())

    spread = hot(iota((span, cols), 1) // heads == iota((span, cols), 0))
    e1 = dot_hi(c64, spread)
    e1 = jnp.where(iota((r64, cols), 0) % heads == iota((r64, cols), 1) % heads, e1, 0.0)
    take = hot(iota((num_seqs, r64), 1) // heads == iota((num_seqs, r64), 0))
    cflat = dot_hi(take, e1)
    brow[...] = jnp.where(iota((num_seqs, cols), 1) // heads < rel16, -cflat, floor_value)
    for m in zmasks[::-1]:
        q_yrs(m).wait_recv()
        q_zs[m // 2] = (part_q[rrow(kvs[m])].astype(F32) + q_y[m // 2].astype(F32)).astype(BF)
        q_zrs(m).start()
    in_tok.wait()
    lax.fori_loop(0, rows // nb, sum_rows, 0)
    total = dot_hi(ssq[...], jnp.ones((lanes, lanes), F32))
    invv[...] = lax.rsqrt(total / width + epsilon)
    in_parent.wait()
    ri = iota((rows, rows), 0)
    ci = iota((rows, rows), 1)
    pick = hot(iota((rows, num_seqs), 0) // prop == iota((rows, num_seqs), 1))
    pb = dot_hi(pick, parent[...].astype(F32))
    pcol = jnp.sum(
        jnp.where(iota((rows, prop), 1) == iota((rows, prop), 0) % prop, pb, 0.0),
        axis=1,
        keepdims=True,
    )
    target = jnp.where(pcol >= 0.0, (ri // prop * prop).astype(F32) + pcol, -1.0)
    a = jnp.where((ri == ci) | (ci.astype(F32) == target), 1.0, 0.0)
    for sweep in range(max(1, (prop - 1).bit_length())):
        low = a.astype(BF)
        a = jnp.minimum(jnp.dot(low, low, preferred_element_type=F32), 1.0)
    anc[...] = a
    q_yrs(0).wait_recv()
    own = part_q[rrow(me)].astype(F32) + q_y[0].astype(F32)
    received(on_qz, q_zr.at[pl.ds(1, half - 1)])
    for m in zmasks:
        own = own + q_zr[m // 2].astype(F32)
    q_full[rrow(me)] = scaled(own, me).astype(BF)
    for m in [1] + zmasks[::-1]:
        q_ag(m).start()
    same_head = iota((hp, cols), 0) // prop == iota((hp, cols), 1) % heads
    diag_l = iota((L, L), 0) == iota((L, L), 1)

    def heads_of(ref, s, first):
        block = ref[pl.ds(pl.multiple_of(s * prop, prop), prop), first : first + hw]
        return jnp.concatenate([block[:, h * hd : (h + 1) * hd] for h in range(heads)], axis=0)

    def block_part(src):
        maxes, totals, values = [], [], []
        for j in range(sp):
            s = src * sp + j
            q = heads_of(q_full, s, 0)
            sc = lax.dot_general(q, kcv[s], NT, preferred_element_type=F32) * scale
            sc = jnp.where(same_head, sc + brow[pl.ds(s, 1), :], floor_value)
            m = jnp.max(sc, axis=1, keepdims=True)
            w = jnp.exp(sc - m)
            maxes.append(m)
            totals.append(jnp.sum(w, axis=1, keepdims=True))
            values.append(
                jnp.dot(w.astype(BF), vcv[s], preferred_element_type=F32).astype(BF)
            )
        m = jnp.concatenate(maxes, axis=0)
        t = jnp.concatenate(totals, axis=0)
        m_lane = jnp.sum(jnp.where(diag_l, m, 0.0), axis=0, keepdims=True)
        t_lane = jnp.sum(jnp.where(diag_l, t, 0.0), axis=0, keepdims=True)
        stats = jnp.where(iota((2, L), 0) == 0, m_lane, t_lane)
        return stats, jnp.concatenate(values, axis=0)

    def blocks(masks):
        parts = [block_part(kvs[m]) for m in masks]
        for m, (stats, values) in zip(masks, parts):
            if m == last:
                st_recv[0] = stats
                val_recv[0] = values
            else:
                st_send[last - m] = stats
                val_send[last - m] = values
        for m in masks:
            if m != last:
                stat_copy(last - m).start()
                val_copy(last - m).start()
    def take_q(m):
        q_ag(m).wait_recv()
        if m % 2 == 0:
            q_ag(m + 1).start()
    in_kc.wait()
    in_vc.wait()
    blocks([0])
    for i, m in enumerate((2, 6)):
        kv_yrs(m).wait_recv()
        kv_zs[i] = kv_sum(m).astype(BF)
    kv_near().start()
    in_wft.wait()
    in_bias.wait()
    wscaled = wft[...].astype(F32) * gain[...]
    whigh = wscaled.astype(BF)
    wlow = (wscaled - whigh.astype(F32)).astype(BF)
    lf = lax.dot_general(
        jnp.concatenate([whigh, wlow], axis=0), tokv[...], NT, preferred_element_type=F32
    )
    lf = lf[0:heads_all] + lf[heads_all : 2 * heads_all]
    inv_lane = dot_hi(jnp.full((8, lanes), 1.0 / lanes, F32), invv[...], NT)[0:1]
    bcol = jnp.zeros((heads_all, rows), F32)
    for h in range(heads_all):
        bcol = jnp.where(iota((heads_all, rows), 0) == h, bias[h], bcol)
    z = lf * inv_lane + bcol
    lf = jnp.minimum(z, 0.0) - jnp.log1p(jnp.exp(-jnp.abs(z)))
    path_t = dot_hi(lf, a, NT)
    rep = hot(iota((r64, heads_all), 1) == mt * heads + iota((r64, heads_all), 0) % heads)
    pm = dot_hi(rep, path_t)
    pm = jnp.where(iota((r64, rows), 1) // prop == iota((r64, rows), 0) // heads, pm, 0.0)
    fold = hot(iota((rows, 128), 0) % prop == iota((rows, 128), 1) % prop)
    pt = dot_hi(pm, fold)
    ptile[...] = pt
    ptm = jnp.where((iota((r64, 128), 1) // prop) % heads == iota((r64, 128), 0) % heads, pt, 0.0)
    tpath[...] = dot_hi(take, ptm)
    take_q(2)
    take_q(1)
    blocks([1, 2])
    take_q(4)
    take_q(6)
    blocks([4, 6])
    kv_yrs(4).wait_recv()
    kv_near().wait_recv()
    kv_zs[2] = (kv_sum(4) + kv_zr[1].astype(F32)).astype(BF)
    kv_far().start()
    take_q(3)
    take_q(5)
    blocks([3, 5])
    take_q(7)
    blocks([7])


    kv_yrs(0).wait_recv()
    kv_far().wait_recv()
    own = kv_sum(0) + kv_zr[0].astype(F32) + kv_zr[2].astype(F32)
    kv_full[rrow(kvs[last])] = scaled(own, kvs[last]).astype(BF)

    fold_h = iota((rows, hp), 0)
    tmax, ttot, tval = [], [], []
    for j in range(sp):
        s = kvs[last] * sp + j
        q = heads_of(q_full, s, 0)
        k = heads_of(kv_full, s, 0)
        v = heads_of(kv_full, s, hw)
        arows = anc[pl.ds(pl.multiple_of(s * prop, prop), prop), :]
        sel = hot(fold_h == s * prop + iota((rows, hp), 1) % prop).astype(BF)
        am = jnp.dot(arows.astype(BF), sel, preferred_element_type=F32)
        am = jnp.concatenate([am] * heads, axis=0)
        mask = (am > 0.5) & (iota((hp, hp), 0) // prop == iota((hp, hp), 1) // prop)
        sc = lax.dot_general(q, k, NT, preferred_element_type=F32) * scale
        sc = jnp.where(mask, sc - tpath[pl.ds(s, 1), 0:hp], floor_value)
        m = jnp.max(sc, axis=1, keepdims=True)
        w = jnp.where(mask, jnp.exp(sc - m), 0.0)
        tmax.append(m)
        ttot.append(jnp.sum(w, axis=1, keepdims=True))
        tval.append(jnp.dot(w.astype(BF), v, preferred_element_type=F32))
    tree_max = jnp.concatenate(tmax, axis=0)
    tree_tot = jnp.concatenate(ttot, axis=0)
    tree_val = jnp.concatenate(tval, axis=0)

    last_lane = cand_send[...]
    received(on_cand, cand_recv.at[pl.ds(1, n - 1)])
    for m in range(1, n):
        last_lane = jnp.maximum(last_lane, cand_recv[m])
    own_rows = iota((L, 128), 0)
    own_head = (kvs[last] * sp + own_rows // hp) * heads + (own_rows % hp) // prop
    own_pick = iota((L, 128), 1) == own_head
    last_own = jnp.sum(jnp.where(own_pick, last_lane, 0.0), axis=1, keepdims=True)

    received(on_stat, st_recv.at[pl.ds(1, n - 1)])
    top = st_recv[0, 0:1]
    for m in range(1, n):
        top = jnp.maximum(top, st_recv[m, 0:1])

    def col(x):
        return jnp.sum(jnp.where(diag_l, x, 0.0), axis=1, keepdims=True)

    cache_tot = jnp.zeros((1, L), F32)
    scales = []
    for m in range(n):
        sd = jnp.exp(st_recv[m, 0:1] - top)
        scales.append(col(sd))
        cache_tot = cache_tot + st_recv[m, 1:2] * sd
    shifted = col(top) + last_own
    both = jnp.maximum(shifted, tree_max)
    cscale = jnp.exp(shifted - both)
    tscale = jnp.exp(tree_max - both)
    denom = col(cache_tot) * cscale + tree_tot * tscale
    vals = val_recv[0].astype(F32) * scales[0]
    for m in range(1, n):
        val_copy(m).wait_recv()
        vals = vals + val_recv[m].astype(F32) * scales[m]
    attended = ((vals * cscale + tree_val * tscale) / denom).astype(BF)
    for j in range(sp):
        for h in range(heads):
            att[pl.ds(pl.multiple_of(kvs[last] * R + j * prop, prop), prop), h * hd : (h + 1) * hd] = (
                attended[j * hp + h * prop : j * hp + (h + 1) * prop]
            )
    for m in [1] + zmasks[::-1]:
        att_ag(m).start()

    upper = me >= half

    @pl.when(upper)
    def _():
        kv_pass(2).start()
        kv_side(1).start()

    @pl.when(jnp.logical_not(upper))
    def _():
        kv_cross().start()

    last_col = jnp.sum(jnp.where(diag, last_lane, 0.0), axis=1, keepdims=True)
    shifted_path = ptile[...]
    for b in range((span - 1).bit_length()):
        moved = pltpu.roll(shifted_path, 1 << b, 1)
        shifted_path = jnp.where((rel64 >> b) & 1 == 1, moved, shifted_path)
    off = lane - rel64
    cum_out[...] = jnp.where((off >= 0) & (off < prop), last_col + shifted_path, c64)

    in_wo.wait()
    oc = o_send.shape[2]
    near = half * R - lax.div(me, half) * (half * R)
    grows = [
        pl.ds(pl.multiple_of(first, half * R), half * R) for first in (near, half * R - near)
    ]

    def o_copy(g, d):
        return send(
            11,
            on_o + g,
            {"tp": tps[d]},
            o_send.at[tps[d], grows[g]],
            o_recv.at[d, grows[g]],
        )

    for m in zmasks:
        att_ag(m).wait_recv()
        att_ag(m + 1).start()
    for g in range(2):
        for m in range(1 + g * half, (g + 1) * half, 2):
            att_ag(m).wait_recv()
        full = jnp.dot(att[grows[g]], wov[...], preferred_element_type=F32).astype(BF)
        for t in range(nt):
            o_send[t, grows[g]] = full[:, t * oc : (t + 1) * oc]
        each_far(nt, lambda d: o_copy(g, d).start())

    @pl.when(upper)
    def _():
        kv_cross().wait_recv()
        kv_pass(6).start()
        kv_side(5).start()
        kv_pass(2).wait_recv()
        kv_side(3).start()

    mixed = o_send[mt].astype(F32)
    for g in range(2):
        received(on_o + g, o_recv.at[pl.ds(1, nt - 1), grows[g]])
    for d in range(1, nt):
        mixed = mixed + o_recv[d].astype(F32)
    sq = dot_hi(jnp.ones((8, oc), F32), mixed * mixed, NT)[0:1]
    sq_send[...] = sq

    def sq_copy(e):
        peer = {"kv": kvs[e // nt], "tp": tps[e % nt]}
        return send(12, on_sq, peer, sq_send, sq_recv.at[e])

    each_far(everyone, lambda e: sq_copy(e).start())

    order = hot(
        iota((hp, hp), 1) == iota((hp, hp), 0) % heads * prop + iota((hp, hp), 0) // heads
    ).astype(BF)

    unroll = 4

    @pl.when(upper)
    def _():
        kv_pass(6).wait_recv()
        kv_side(7).start()
        for m in range(1, n, 2):
            kv_side(m).wait_recv()

        def some(i, c):
            fresh = [
                heads_of(kv_full, i * unroll + j, first) for j in range(unroll) for first in (0, hw)
            ]
            placed = jnp.dot(
                order, jnp.concatenate(fresh, axis=1), preferred_element_type=F32
            ).astype(BF)
            for j in range(unroll):
                at = 2 * j * hd
                knew_out[i * unroll + j] = placed[:, at : at + hd]
                vnew_out[i * unroll + j] = placed[:, at + hd : at + 2 * hd]
            return c

        lax.fori_loop(0, num_seqs // unroll, some, 0)

    received(on_sq, sq_recv.at[pl.ds(1, everyone - 1)])
    for e in range(1, everyone):
        sq = sq + sq_recv[e]
    ssum = dot_hi(
        jnp.broadcast_to(sq, (8, rows)), jnp.full((8, oc), 0.125, F32), (((0,), (0,)), ((), ()))
    )
    in_gpost.wait()
    mixed_out[...] = (mixed * lax.rsqrt(ssum / width + epsilon) * gpost[...]).astype(BF)

    sent(0, q_y)
    sent(1, q_zr.at[pl.ds(1, half - 1)])
    sent(2, kv_y)
    sent(3, kv_zr.at[pl.ds(0, 2)])
    sent(4, kv_zr.at[2])
    sent(5, q_full.at[pl.ds(0, last * R)])
    sent(6, cand_recv.at[pl.ds(1, last)])
    sent(7, st_recv.at[pl.ds(1, last)])
    sent(8, val_recv.at[pl.ds(1, last)])
    sent(9, att.at[pl.ds(0, last * R)])

    @pl.when(upper)
    def _():
        sent(10, kv_full.at[pl.ds(0, (2 + half) * R)])

    @pl.when(jnp.logical_not(upper))
    def _():
        sent(10, kv_full.at[pl.ds(0, R)])

    sent(11, o_recv.at[pl.ds(1, nt - 1)])
    sent(12, sq_recv.at[pl.ds(1, everyone - 1)])


def patch_kernel(
    n,
    prop,
    k_in,
    v_in,
    knew,
    vnew,
    mixed,
    cum,
    starts,
    k_out,
    v_out,
    mixed_out,
    cum_out,
    k_buf,
    v_buf,
    sem,
):
    me = lax.axis_index("kv")
    num_seqs, span = k_out.shape[:2]
    out_m = pltpu.make_async_copy(mixed, mixed_out, sem.at[0])
    out_c = pltpu.make_async_copy(cum, cum_out, sem.at[1])
    out_m.start()
    out_c.start()

    def store(s):
        pltpu.make_async_copy(k_buf.at[s], k_out.at[s], sem.at[2]).start()
        pltpu.make_async_copy(v_buf.at[s], v_out.at[s], sem.at[3]).start()

    def place(s):
        at = starts[s]

        @pl.when((at >= 0) & (at <= span - prop))
        def _():
            k_buf[s, pl.ds(at, prop)] = knew[s]
            v_buf[s, pl.ds(at, prop)] = vnew[s]

        @pl.when(((at > -prop) & (at < 0)) | ((at > span - prop) & (at < span)))
        def _():
            def one(j, c):
                @pl.when((at + j >= 0) & (at + j < span))
                def _():
                    k_buf[s, pl.ds(at + j, 1)] = knew[s, pl.ds(j, 1)]
                    v_buf[s, pl.ds(at + j, 1)] = vnew[s, pl.ds(j, 1)]

                return c

            lax.fori_loop(0, prop, one, 0)

    @pl.when(me >= n // 2)
    def _():
        for s in range(num_seqs):
            place(s)
            if s > 0:
                store(s - 1)
        store(num_seqs - 1)

    @pl.when(me < n // 2)
    def _():
        for s in range(num_seqs):
            store(s)

    pltpu.make_async_copy(k_buf, k_out, sem.at[2]).wait()
    pltpu.make_async_copy(v_buf, v_out, sem.at[3]).wait()
    out_m.wait()
    out_c.wait()


def fast_device(
    n,
    nt,
    tokens,
    gain_pre,
    w_query,
    w_key,
    w_value,
    w_forget,
    b_forget,
    w_out,
    gain_post,
    key_cache,
    value_cache,
    cum_cache,
    lengths,
    accepted,
    parent,
):
    num_seqs, prop, width = tokens.shape
    span, heads, hd = key_cache.shape[1:]
    rows = num_seqs * prop
    hw = heads * hd
    cols = heads * span
    sp = num_seqs // n
    R = sp * prop
    L = sp * heads * prop
    oc = gain_post.shape[0]
    half = n // 2
    everyone = n * nt
    kc = key_cache.reshape(num_seqs, cols, hd)
    vc = value_cache.reshape(num_seqs, cols, hd)
    cum = jnp.swapaxes(cum_cache, 1, 2).reshape(num_seqs * heads, span)
    hbm = pl.BlockSpec(memory_space=pltpu.HBM)
    vmem = pl.BlockSpec(memory_space=pltpu.VMEM)
    smem = pl.BlockSpec(memory_space=pltpu.SMEM)
    V = pltpu.VMEM
    S = pltpu.SMEM
    D = pltpu.SemaphoreType.DMA
    mixed, cum_new, knew, vnew, kv, vv, starts = pl.pallas_call(
        functools.partial(layer_kernel, n, nt, num_seqs, prop, heads, hd, span),
        out_shape=(
            V((rows, oc), BF),
            V(cum.shape, F32),
            V((num_seqs, heads * prop, hd), BF),
            V((num_seqs, heads * prop, hd), BF),
            V(kc.shape, BF),
            V(vc.shape, BF),
            S(lengths.shape, jnp.int32),
        ),
        in_specs=[hbm] * 15,
        out_specs=(vmem,) * 6 + (smem,),
        scratch_shapes=[
            V((rows, width), BF),
            V((1, width), F32),
            V((3,) + w_query.shape, BF),
            V(w_forget.shape[::-1], BF),
            S(b_forget.shape, F32),
            V(w_out.shape, BF),
            V((1, oc), F32),
            V(cum.shape, F32),
            S(lengths.shape, jnp.int32),
            S(accepted.shape, jnp.int32),
            V(parent.shape, jnp.int32),
            V((rows, 128), F32),
            V((rows, 128), F32),
            V((rows, w_query.shape[0]), BF),
            V((rows, w_query.shape[0]), BF),
            V((rows, hw), BF),
            V((half, R, hw), BF),
            V((half, R, hw), BF),
            V((half, R, hw), BF),
            V((rows, hw), BF),
            V((rows, 2 * hw), BF),
            V((half, R, 2 * hw), BF),
            V((half - 1, R, 2 * hw), BF),
            V((half - 1, R, 2 * hw), BF),
            V((rows, 2 * hw), BF),
            V((n, 2, L), F32),
            V((n, L, hd), BF),
            V((n, 2, L), F32),
            V((n, L, hd), BF),
            V((1, 128), F32),
            V((n, 1, 128), F32),
            V((num_seqs, cols), F32),
            V((rows, rows), F32),
            V((num_seqs, 128), F32),
            V((num_seqs * heads, 128), F32),
            V((rows, hw), BF),
            V((nt, rows, oc), BF),
            V((nt, rows, oc), BF),
            V((1, rows), F32),
            V((everyone, 1, rows), F32),
            D((16,)),
            D((13,)),
            D((2 * half + 4 * n + 8,)),
        ],
        compiler_params=pltpu.CompilerParams(
            collective_id=0, has_side_effects=True, vmem_limit_bytes=50 * 1024 * 1024
        ),
        name="layer",
    )(
        *[
            pltpu.with_memory_space_constraint(operand, pltpu.HBM)
            for operand in (
                tokens.reshape(rows, width),
                gain_pre.reshape(1, width),
                w_query,
                w_key,
                w_value,
                w_forget.T,
                b_forget,
                w_out,
                gain_post.reshape(1, oc),
                kc,
                vc,
                cum,
                lengths,
                accepted,
                parent,
            )
        ]
    )
    fresh = (num_seqs, prop, heads, hd)
    key_out, value_out, mixed, cum_new, *unused = pl.pallas_call(
        functools.partial(patch_kernel, n, prop),
        out_shape=(
            pltpu.HBM(key_cache.shape, BF),
            pltpu.HBM(value_cache.shape, BF),
            pltpu.HBM(mixed.shape, BF),
            pltpu.HBM(cum.shape, F32),
            V(key_cache.shape, BF),
            V(key_cache.shape, BF),
        ),
        in_specs=[vmem, vmem, vmem, vmem, vmem, vmem, smem],
        out_specs=(hbm, hbm, hbm, hbm, vmem, vmem),
        input_output_aliases={0: 4, 1: 5},
        scratch_shapes=[D((4,))],
        compiler_params=pltpu.CompilerParams(
            has_side_effects=True, vmem_limit_bytes=4 * 1024 * 1024
        ),
        name="patch",
    )(
        *[
            pltpu.with_memory_space_constraint(operand, V)
            for operand in (kv.reshape(key_cache.shape), vv.reshape(key_cache.shape), knew.reshape(fresh), vnew.reshape(fresh), mixed, cum_new)
        ],
        starts,
    )
    cum_out = jnp.swapaxes(cum_new.reshape(num_seqs, heads, span), 1, 2)
    return (
        mixed.reshape(num_seqs, prop, oc),
        key_out.reshape(key_cache.shape),
        value_out.reshape(value_cache.shape),
        cum_out,
    )


def choose(mesh):
    n, nt = mesh.shape["kv"], mesh.shape["tp"]

    def body(*args):
        tokens, key_cache = args[0], args[9]
        num_seqs, prop = tokens.shape[:2]
        span, heads = key_cache.shape[1:3]
        fits = (
            num_seqs % n == 0
            and n == 8
            and nt & (nt - 1) == 0
            and num_seqs % 4 == 0
            and (num_seqs // n) * heads * prop == 128
            and span == 128
            and num_seqs * heads <= 128
            and prop % 16 == 0
        )
        if fits:
            return fast_device(n, nt, *args)
        return per_device(*args)

    return body


def solution(mesh):
    return jax.shard_map(
        choose(mesh),
        mesh=mesh,
        in_specs=(
            P(),
            P(),
            P("kv", "tp"),
            P("kv", "tp"),
            P("kv", "tp"),
            P(),
            P(),
            P("tp", "kv"),
            P(("kv", "tp")),
            P(None, "kv", "tp", None),
            P(None, "kv", "tp", None),
            P(None, "kv", "tp"),
            P(),
            P(),
            P(),
        ),
        out_specs=(
            P(None, None, ("kv", "tp")),
            P(None, "kv", "tp", None),
            P(None, "kv", "tp", None),
            P(None, "kv", "tp"),
        ),
        check_vma=False,
    )
```

```python
import functools

import jax
import jax.numpy as jnp
from jax import lax
from jax.experimental import pallas as pl
from jax.experimental.pallas import tpu as pltpu
from jax.sharding import PartitionSpec as P

epsilon = 1e-06
floor_value = -1e30


def merged(part, axis, combine):
    gathered = jax.tree.map(lambda a: lax.all_gather(a, axis), part)

    def take(source):
        return jax.tree.map(lambda a: lax.dynamic_index_in_dim(a, source, 0, False), gathered)

    return lax.fori_loop(
        1, lax.axis_size(axis), lambda source, state: combine(state, take(source)), take(0)
    )


def ancestry(parent_ids, members):
    identity = jnp.eye(members, dtype=jnp.float32)
    parent_hot = (
        parent_ids[:, :, None] == jnp.arange(members, dtype=jnp.int32)[None, None, :]
    ).astype(jnp.float32)
    ancestors = jnp.minimum(identity[None] + parent_hot, 1.0)
    for sweep in range(max(1, (members - 1).bit_length())):
        ancestors = jnp.minimum(
            jnp.einsum("bij,bjk->bik", ancestors, ancestors, precision=lax.Precision.HIGHEST), 1.0
        )
    return ancestors


def combine_parts(first, second):
    new_max = jnp.maximum(first[0], second[0])
    first_scale = jnp.exp(first[0] - new_max)
    second_scale = jnp.exp(second[0] - new_max)
    return (
        new_max,
        first[1] * first_scale + second[1] * second_scale,
        first[2] * first_scale[..., None] + second[2] * second_scale[..., None],
        jnp.maximum(first[3], second[3]),
    )


def finish_rows(cache_max, cache_total, cache_values, last_rows, tree_max, tree_total, tree_values):
    shifted = cache_max + last_rows
    top = jnp.maximum(shifted, tree_max)
    cache_scale = jnp.exp(shifted - top)
    tree_scale = jnp.exp(tree_max - top)
    attended = (
        (cache_values * cache_scale[..., None] + tree_values * tree_scale[..., None])
        / (cache_total * cache_scale + tree_total * tree_scale)[..., None]
    ).astype(jnp.bfloat16)
    return attended.reshape(attended.shape[0], attended.shape[1] * attended.shape[2])


def per_device(
    tokens,
    gain_pre,
    w_query,
    w_key,
    w_value,
    w_forget,
    b_forget,
    w_out,
    gain_post,
    key_cache,
    value_cache,
    cum_cache,
    lengths,
    accepted,
    parent,
):
    num_seqs, proposals, model_width = tokens.shape
    kv_rank = lax.axis_index("kv")
    tp_rank = lax.axis_index("tp")
    span = key_cache.shape[1]
    heads_local = key_cache.shape[2]
    head_dim = key_cache.shape[3]
    scale = head_dim ** (-0.5)
    all_rows = num_seqs * proposals
    tok_float = tokens.astype(jnp.float32)
    normed = (
        tok_float
        * lax.rsqrt(jnp.mean(tok_float * tok_float, -1, keepdims=True) + epsilon)
        * gain_pre
    ).astype(jnp.bfloat16)
    flat = normed.reshape(all_rows, model_width)
    weight_rows = w_query.shape[0]
    local_rows = lax.dynamic_slice_in_dim(flat, kv_rank * weight_rows, weight_rows, 1)
    query_part = jnp.dot(local_rows, w_query, preferred_element_type=jnp.float32)
    key_part = jnp.dot(local_rows, w_key, preferred_element_type=jnp.float32)
    value_part = jnp.dot(local_rows, w_value, preferred_element_type=jnp.float32)
    summed = (
        lax.psum(query_part.astype(jnp.bfloat16), "kv").astype(jnp.float32),
        lax.psum(key_part.astype(jnp.bfloat16), "kv").astype(jnp.float32),
        lax.psum(value_part.astype(jnp.bfloat16), "kv").astype(jnp.float32),
    )
    query_flat = summed[0].astype(jnp.bfloat16)
    key_flat = summed[1].astype(jnp.bfloat16)
    value_flat = summed[2].astype(jnp.bfloat16)
    query = query_flat.reshape(num_seqs, proposals, heads_local, head_dim)
    key_new = key_flat.reshape(num_seqs, proposals, heads_local, head_dim)
    value_new = value_flat.reshape(num_seqs, proposals, heads_local, head_dim)
    forget_cols = lax.dynamic_slice_in_dim(w_forget, tp_rank * heads_local, heads_local, 1)
    forget_bias = lax.dynamic_slice_in_dim(b_forget, tp_rank * heads_local, heads_local, 0)
    log_forget = jax.nn.log_sigmoid(
        jnp.dot(flat, forget_cols, preferred_element_type=jnp.float32) + forget_bias
    ).reshape(num_seqs, proposals, heads_local)
    ancestors = ancestry(parent, proposals)
    path = jnp.einsum("bij,bjh->bih", ancestors, log_forget, precision=lax.Precision.HIGHEST)
    valid = lengths + accepted
    positions = kv_rank * span + jnp.arange(span, dtype=jnp.int32)
    live = (positions[None, :] < valid[:, None])[:, None, None, :]
    score = (
        jnp.einsum("bihd,bkhd->bihk", query, key_cache, preferred_element_type=jnp.float32) * scale
        + path[..., None]
        - jnp.swapaxes(cum_cache, 1, 2)[:, None]
    )
    block_max = jnp.max(jnp.where(live, score, floor_value), axis=-1)
    weight = jnp.exp(jnp.where(live, score - block_max[..., None], floor_value))
    block_total = jnp.sum(weight, axis=-1)
    block_values = jnp.einsum(
        "bihk,bkhd->bihd",
        weight.astype(jnp.bfloat16),
        value_cache,
        preferred_element_type=jnp.float32,
    )
    owner = positions[None, :] == (valid - 1)[:, None]
    candidate = jnp.max(jnp.where(owner[:, :, None], cum_cache, floor_value), axis=1)
    tree_mask = (ancestors > 0.5)[:, :, None, :]
    tree_score = (
        jnp.einsum("bihd,bjhd->bihj", query, key_new, preferred_element_type=jnp.float32) * scale
        + path[..., None]
        - jnp.swapaxes(path, 1, 2)[:, None]
    )
    tree_max = jnp.max(jnp.where(tree_mask, tree_score, floor_value), axis=-1)
    tree_weight = jnp.exp(jnp.where(tree_mask, tree_score - tree_max[..., None], floor_value))
    tree_total = jnp.sum(tree_weight, axis=-1)
    tree_values = jnp.einsum(
        "bihj,bjhd->bihd",
        tree_weight.astype(jnp.bfloat16),
        value_new,
        preferred_element_type=jnp.float32,
    )
    tree_max_rows = tree_max.reshape(all_rows, heads_local)
    tree_total_rows = tree_total.reshape(all_rows, heads_local)
    tree_values_rows = tree_values.reshape(all_rows, heads_local, head_dim)
    cache_max, cache_total, cache_values, last_cum = merged(
        (block_max, block_total, block_values, candidate), "kv", combine_parts
    )
    last_rows = jnp.broadcast_to(last_cum[:, None, :], (num_seqs, proposals, heads_local)).reshape(
        all_rows, heads_local
    )
    attended = finish_rows(
        cache_max.reshape(all_rows, heads_local),
        cache_total.reshape(all_rows, heads_local),
        cache_values.reshape(all_rows, heads_local, head_dim),
        last_rows,
        tree_max_rows,
        tree_total_rows,
        tree_values_rows,
    )
    mixed_part = jnp.dot(attended, w_out, preferred_element_type=jnp.float32)
    mixed_sum = lax.psum_scatter(
        mixed_part.astype(jnp.bfloat16), "tp", scatter_dimension=1, tiled=True
    ).astype(jnp.float32)
    squares = lax.psum(jnp.sum(mixed_sum * mixed_sum, axis=1), ("kv", "tp"))
    mixed = (mixed_sum * lax.rsqrt(squares / model_width + epsilon)[:, None] * gain_post).astype(
        jnp.bfloat16
    )
    mixed = mixed.reshape(num_seqs, proposals, mixed_sum.shape[1])
    relative = positions[None, :] - valid[:, None]
    select = relative[:, :, None] == jnp.arange(proposals, dtype=jnp.int32)[None, None, :]
    written = (relative >= 0) & (relative < proposals)
    placed_keys = jnp.einsum(
        "bkj,bjhd->bkhd", select.astype(jnp.bfloat16), key_new, preferred_element_type=jnp.float32
    ).astype(jnp.bfloat16)
    placed_values = jnp.einsum(
        "bkj,bjhd->bkhd", select.astype(jnp.bfloat16), value_new, preferred_element_type=jnp.float32
    ).astype(jnp.bfloat16)
    key_out = jnp.where(written[:, :, None, None], placed_keys, key_cache)
    value_out = jnp.where(written[:, :, None, None], placed_values, value_cache)
    cum_new = last_cum[:, None, :] + path
    placed_cum = jnp.einsum(
        "bkj,bjh->bkh", select.astype(jnp.float32), cum_new, precision=lax.Precision.HIGHEST
    )
    cum_out = jnp.where(written[:, :, None], placed_cum, cum_cache)
    return (mixed, key_out, value_out, cum_out)


MESH = pl.DeviceIdType.MESH
HI = lax.Precision.HIGHEST
F32 = jnp.float32
BF = jnp.bfloat16


def iota(shape, dim):
    return lax.broadcasted_iota(jnp.int32, shape, dim)


def hot(mask):
    return jnp.where(mask, 1.0, 0.0).astype(F32)


def dot_hi(a, b, dims=(((1,), (0,)), ((), ()))):
    return lax.dot_general(a, b, dims, precision=HI, preferred_element_type=F32)


NT = (((1,), (1,)), ((), ()))
TN = (((0,), (0,)), ((), ()))


def thirds(x):
    high = x.astype(BF)
    rest = x - high.astype(F32)
    middle = rest.astype(BF)
    return high, middle, (rest - middle.astype(F32)).astype(BF)


def flips(value, count):
    bit = 1
    out = [value]
    while bit < count:
        step = bit * (1 - 2 * lax.rem(lax.div(value, bit), 2))
        out = out + [other + step for other in out]
        bit *= 2
    return out


def layer_kernel(
    n,
    nt,
    num_seqs,
    prop,
    heads,
    hd,
    span,
    tok_h,
    gain_h,
    wq_h,
    wk_h,
    wv_h,
    wft_h,
    bias_h,
    wo_h,
    gpost_h,
    kc_h,
    vc_h,
    cum_h,
    lens_h,
    accs_h,
    parent_h,
    mixed_out,
    cum_out,
    knew_out,
    vnew_out,
    kcv,
    vcv,
    at_out,
    tokv,
    gain,
    wqkv,
    wft,
    bias,
    wov,
    gpost,
    cum,
    lens,
    accs,
    parent,
    ssq,
    invv,
    xraw,
    xloc,
    part_q,
    q_y,
    q_zs,
    q_zr,
    q_full,
    part_kv,
    kv_y,
    kv_zs,
    kv_zr,
    kv_full,
    st_send,
    val_send,
    st_recv,
    val_recv,
    cand_send,
    cand_recv,
    brow,
    anc,
    tpath,
    ptile,
    att,
    o_send,
    o_recv,
    sq_send,
    sq_recv,
    loc,
    ssem,
    rsem,
):
    me = lax.axis_index("kv")
    mt = lax.axis_index("tp")
    rows, width = tokv.shape
    hw = heads * hd
    kdim = wq_h.shape[0]
    cols = heads * span
    sp = num_seqs // n
    R = sp * prop
    hp = heads * prop
    L = sp * hp
    scale = hd ** (-0.5)
    base = me * span
    heads_all = wft.shape[0]
    half = n // 2
    everyone = n * nt

    barrier = pltpu.get_barrier_semaphore()

    kvs = flips(me, n)
    tps = flips(mt, nt)

    mine = pl.ds(pl.multiple_of(me * kdim, kdim), kdim)
    loads = [
        (tok_h.at[:, mine], xraw),
        (wq_h, wqkv.at[0]),
        (gain_h, gain),
        (wk_h, wqkv.at[1]),
        (wv_h, wqkv.at[2]),
        (tok_h, tokv),
        (lens_h, lens),
        (accs_h, accs),
        (cum_h, cum),
        (parent_h, parent),
        (wft_h, wft),
        (bias_h, bias),
        (gpost_h, gpost),
        (kc_h, kcv),
        (vc_h, vcv),
        (wo_h, wov),
    ]
    copies = [pltpu.make_async_copy(src, dst, loc.at[i]) for i, (src, dst) in enumerate(loads)]
    (
        in_x,
        in_wq,
        in_gain,
        in_wk,
        in_wv,
        in_tok,
        in_lens,
        in_accs,
        in_cum,
        in_parent,
        in_wft,
        in_bias,
        in_gpost,
        in_kc,
        in_vc,
        in_wo,
    ) = copies
    urgent = 5
    for c in copies[:urgent]:
        c.start()
    for e in range(1, everyone):
        pl.semaphore_signal(
            barrier,
            inc=1,
            device_id={"kv": kvs[e // nt], "tp": tps[e % nt]},
            device_id_type=MESH,
        )

    def send(kind, slot, device, src, dst):
        return pltpu.make_async_remote_copy(
            src_ref=src,
            dst_ref=dst,
            send_sem=ssem.at[kind],
            recv_sem=rsem.at[slot],
            device_id=device,
            device_id_type=MESH,
        )

    def to_kv(kind, slot, mask, src, dst):
        return send(kind, slot, {"kv": kvs[mask]}, src, dst)

    def rrow(i):
        return pl.ds(pl.multiple_of(i * R, R), R)

    def spread_to(kind, slot, mask, ref, rank):
        return to_kv(kind, slot, mask, ref.at[rrow(rank)], ref.at[rrow(rank)])

    def sent(kind, ref):
        to_kv(kind, 0, 1, ref, ref).wait_send()

    def received(slot, ref):
        to_kv(0, slot, 1, ref, ref).wait_recv()

    flat = [0]

    def slots(count):
        flat[0] += count
        return flat[0] - count

    on_qy, on_qz, on_ky, on_kz = slots(half), slots(1), slots(half), slots(2)
    on_qag, on_cand, on_stat, on_val = slots(n - 1), slots(1), slots(1), slots(n - 1)
    on_att, on_kvag, on_o, on_sq = slots(half + 1), slots(half), slots(2), slots(1)
    last = n - 1

    def q_yrs(m):
        return to_kv(0, on_qy + m // 2, 1, part_q.at[rrow(kvs[m + 1])], q_y.at[m // 2])

    def q_zrs(m):
        return to_kv(1, on_qz, m, q_zs.at[m // 2], q_zr.at[m // 2])

    def kv_yrs(m):
        src = part_kv.at[rrow(kvs[(m + 1) ^ last])]
        return to_kv(2, on_ky + m // 2, 1, src, kv_y.at[m // 2])

    def kv_near():
        return to_kv(3, on_kz, 2, kv_zs.at[pl.ds(0, 2)], kv_zr.at[pl.ds(0, 2)])

    def kv_far():
        return to_kv(4, on_kz + 1, half, kv_zs.at[2], kv_zr.at[2])

    def q_ag(m):
        if m % 2:
            return spread_to(5, on_qag + m - 1, 1, q_full, kvs[m - 1])
        return spread_to(5, on_qag + m - 1, m, q_full, me)

    def cand_copy(m):
        return to_kv(6, on_cand, m, cand_send, cand_recv.at[m])

    def stat_copy(m):
        return to_kv(7, on_stat, m, st_send.at[m], st_recv.at[m])

    def val_copy(m):
        return to_kv(8, on_val + m - 1, m, val_send.at[m], val_recv.at[m])

    def att_ag(m):
        if m % 2:
            return spread_to(9, on_att + half - 1 + m // half, 1, att, kvs[(m - 1) ^ last])
        return spread_to(9, on_att + m // 2 - 1, m, att, kvs[last])

    def kv_cross():
        return spread_to(10, on_kvag, half, kv_full, kvs[last])

    def kv_pass(m):
        return spread_to(10, on_kvag + 1 + m // half, half // 2, kv_full, kvs[(m - half // 2) ^ last])

    def kv_side(m):
        return spread_to(10, on_kvag + half - 1, 1, kv_full, kvs[(m - 1) ^ last])

    def each(count, fn):
        for d in range(1, count):
            fn(d)

    def each_far(count, fn):
        for d in range(count - 1, 0, -1):
            fn(d)

    def scaled(total, rank):
        inv = invv[rrow(rank)]
        return jnp.concatenate(
            [
                total[:, j * lanes : (j + 1) * lanes] * inv
                for j in range(total.shape[1] // lanes)
            ],
            axis=1,
        )

    zmasks = list(range(2, n, 2))
    nb = prop
    lanes = 128

    def sum_rows(i, c):
        sl = pl.ds(pl.multiple_of(i * nb, nb), nb)
        accs4 = [None] * 4
        for j in range(width // lanes):
            t = tokv[sl, j * lanes : (j + 1) * lanes].astype(F32)
            p = t * t
            accs4[j % 4] = p if accs4[j % 4] is None else accs4[j % 4] + p
        ssq[sl, :] = (accs4[0] + accs4[1]) + (accs4[2] + accs4[3])
        return c

    in_x.wait()
    in_gain.wait()
    xloc[...] = (xraw[...].astype(F32) * gain[:, mine]).astype(BF)
    in_wq.wait()
    part_q[...] = jnp.dot(xloc[...], wqkv[0], preferred_element_type=F32).astype(BF)
    pl.semaphore_wait(barrier, everyone - 1)
    for m in zmasks[::-1] + [0]:
        q_yrs(m).start()
    for c in copies[urgent:]:
        c.start()
    in_wk.wait()
    in_wv.wait()
    part_kv[:, 0:hw] = jnp.dot(xloc[...], wqkv[1], preferred_element_type=F32).astype(BF)
    part_kv[:, hw : 2 * hw] = jnp.dot(xloc[...], wqkv[2], preferred_element_type=F32).astype(BF)
    def kv_sum(m):
        return part_kv[rrow(kvs[m ^ last])].astype(F32) + kv_y[m // 2].astype(F32)
    for m in zmasks[::-1] + [0]:
        kv_yrs(m).start()
    in_lens.wait()
    in_accs.wait()
    in_cum.wait()
    r64 = num_seqs * heads
    c64 = cum[...]
    srow = iota((r64, span), 0) // heads
    lane = iota((r64, span), 1)
    rel64 = jnp.zeros((r64, span), jnp.int32)
    rel16 = jnp.zeros((num_seqs, cols), jnp.int32)
    s16 = iota((num_seqs, cols), 0)
    for s in range(num_seqs):
        rel_s = lens[s] + accs[s] - base
        at_out[s] = rel_s
        rel64 = jnp.where(srow == s, rel_s, rel64)
        rel16 = jnp.where(s16 == s, rel_s, rel16)
    cand = jnp.max(jnp.where(lane == rel64 - 1, c64, floor_value), axis=1, keepdims=True)
    diag = iota((r64, 128), 0) == iota((r64, 128), 1)
    cand_send[...] = jnp.sum(jnp.where(diag, cand, 0.0), axis=0, keepdims=True)
    each_far(n, lambda m: cand_copy(m).start())

    spread = hot(iota((span, cols), 1) // heads == iota((span, cols), 0))
    e1 = dot_hi(c64, spread)
    e1 = jnp.where(iota((r64, cols), 0) % heads == iota((r64, cols), 1) % heads, e1, 0.0)
    take = hot(iota((num_seqs, r64), 1) // heads == iota((num_seqs, r64), 0))
    cflat = dot_hi(take, e1)
    brow[...] = jnp.where(iota((num_seqs, cols), 1) // heads < rel16, -cflat, floor_value)
    for m in zmasks[::-1]:
        q_yrs(m).wait_recv()
        q_zs[m // 2] = (part_q[rrow(kvs[m])].astype(F32) + q_y[m // 2].astype(F32)).astype(BF)
        q_zrs(m).start()
    in_tok.wait()
    lax.fori_loop(0, rows // nb, sum_rows, 0)
    total = dot_hi(ssq[...], jnp.ones((lanes, lanes), F32))
    invv[...] = lax.rsqrt(total / width + epsilon)
    in_parent.wait()
    ri = iota((rows, rows), 0)
    ci = iota((rows, rows), 1)
    pick = hot(iota((rows, num_seqs), 0) // prop == iota((rows, num_seqs), 1))
    pb = dot_hi(pick, parent[...].astype(F32))
    pcol = jnp.sum(
        jnp.where(iota((rows, prop), 1) == iota((rows, prop), 0) % prop, pb, 0.0),
        axis=1,
        keepdims=True,
    )
    target = jnp.where(pcol >= 0.0, (ri // prop * prop).astype(F32) + pcol, -1.0)
    a = jnp.where((ri == ci) | (ci.astype(F32) == target), 1.0, 0.0)
    for sweep in range(max(1, (prop - 1).bit_length())):
        low = a.astype(BF)
        a = jnp.minimum(jnp.dot(low, low, preferred_element_type=F32), 1.0)
    anc[...] = a
    q_yrs(0).wait_recv()
    own = part_q[rrow(me)].astype(F32) + q_y[0].astype(F32)
    received(on_qz, q_zr.at[pl.ds(1, half - 1)])
    for m in zmasks:
        own = own + q_zr[m // 2].astype(F32)
    q_full[rrow(me)] = scaled(own, me).astype(BF)
    for m in [1] + zmasks[::-1]:
        q_ag(m).start()
    same_head = iota((hp, cols), 0) // prop == iota((hp, cols), 1) % heads
    diag_l = iota((L, L), 0) == iota((L, L), 1)

    def heads_of(ref, s, first):
        block = ref[pl.ds(pl.multiple_of(s * prop, prop), prop), first : first + hw]
        return jnp.concatenate([block[:, h * hd : (h + 1) * hd] for h in range(heads)], axis=0)

    def block_part(src):
        maxes, totals, values = [], [], []
        for j in range(sp):
            s = src * sp + j
            q = heads_of(q_full, s, 0)
            sc = lax.dot_general(q, kcv[s], NT, preferred_element_type=F32) * scale
            sc = jnp.where(same_head, sc + brow[pl.ds(s, 1), :], floor_value)
            m = jnp.max(sc, axis=1, keepdims=True)
            w = jnp.exp(sc - m)
            maxes.append(m)
            totals.append(jnp.sum(w, axis=1, keepdims=True))
            values.append(
                jnp.dot(w.astype(BF), vcv[s], preferred_element_type=F32).astype(BF)
            )
        m = jnp.concatenate(maxes, axis=0)
        t = jnp.concatenate(totals, axis=0)
        m_lane = jnp.sum(jnp.where(diag_l, m, 0.0), axis=0, keepdims=True)
        t_lane = jnp.sum(jnp.where(diag_l, t, 0.0), axis=0, keepdims=True)
        stats = jnp.where(iota((2, L), 0) == 0, m_lane, t_lane)
        return stats, jnp.concatenate(values, axis=0)

    def blocks(masks):
        parts = [block_part(kvs[m]) for m in masks]
        for m, (stats, values) in zip(masks, parts):
            if m == last:
                st_recv[0] = stats
                val_recv[0] = values
            else:
                st_send[last - m] = stats
                val_send[last - m] = values
        for m in masks:
            if m != last:
                stat_copy(last - m).start()
                val_copy(last - m).start()
    def take_q(m):
        q_ag(m).wait_recv()
        if m % 2 == 0:
            q_ag(m + 1).start()
    in_kc.wait()
    in_vc.wait()
    blocks([0])
    for i, m in enumerate((2, 6)):
        kv_yrs(m).wait_recv()
        kv_zs[i] = kv_sum(m).astype(BF)
    kv_near().start()
    in_wft.wait()
    in_bias.wait()
    wscaled = wft[...].astype(F32) * gain[...]
    whigh = wscaled.astype(BF)
    wlow = (wscaled - whigh.astype(F32)).astype(BF)
    lf = lax.dot_general(
        jnp.concatenate([whigh, wlow], axis=0), tokv[...], NT, preferred_element_type=F32
    )
    lf = lf[0:heads_all] + lf[heads_all : 2 * heads_all]
    inv_lane = dot_hi(jnp.full((8, lanes), 1.0 / lanes, F32), invv[...], NT)[0:1]
    bcol = jnp.zeros((heads_all, rows), F32)
    for h in range(heads_all):
        bcol = jnp.where(iota((heads_all, rows), 0) == h, bias[h], bcol)
    z = lf * inv_lane + bcol
    lf = jnp.minimum(z, 0.0) - jnp.log1p(jnp.exp(-jnp.abs(z)))
    path_t = dot_hi(lf, a, NT)
    rep = hot(iota((r64, heads_all), 1) == mt * heads + iota((r64, heads_all), 0) % heads)
    pm = dot_hi(rep, path_t)
    pm = jnp.where(iota((r64, rows), 1) // prop == iota((r64, rows), 0) // heads, pm, 0.0)
    fold = hot(iota((rows, 128), 0) % prop == iota((rows, 128), 1) % prop)
    pt = dot_hi(pm, fold)
    ptile[...] = pt
    ptm = jnp.where((iota((r64, 128), 1) // prop) % heads == iota((r64, 128), 0) % heads, pt, 0.0)
    tpath[...] = dot_hi(take, ptm)
    take_q(2)
    take_q(1)
    blocks([1, 2])
    take_q(4)
    take_q(6)
    blocks([4, 6])
    kv_yrs(4).wait_recv()
    kv_near().wait_recv()
    kv_zs[2] = (kv_sum(4) + kv_zr[1].astype(F32)).astype(BF)
    kv_far().start()
    take_q(3)
    take_q(5)
    blocks([3, 5])
    take_q(7)
    blocks([7])


    kv_yrs(0).wait_recv()
    kv_far().wait_recv()
    own = kv_sum(0) + kv_zr[0].astype(F32) + kv_zr[2].astype(F32)
    kv_full[rrow(kvs[last])] = scaled(own, kvs[last]).astype(BF)

    fold_h = iota((rows, hp), 0)
    tmax, ttot, tval = [], [], []
    for j in range(sp):
        s = kvs[last] * sp + j
        q = heads_of(q_full, s, 0)
        k = heads_of(kv_full, s, 0)
        v = heads_of(kv_full, s, hw)
        arows = anc[pl.ds(pl.multiple_of(s * prop, prop), prop), :]
        sel = hot(fold_h == s * prop + iota((rows, hp), 1) % prop).astype(BF)
        am = jnp.dot(arows.astype(BF), sel, preferred_element_type=F32)
        am = jnp.concatenate([am] * heads, axis=0)
        mask = (am > 0.5) & (iota((hp, hp), 0) // prop == iota((hp, hp), 1) // prop)
        sc = lax.dot_general(q, k, NT, preferred_element_type=F32) * scale
        sc = jnp.where(mask, sc - tpath[pl.ds(s, 1), 0:hp], floor_value)
        m = jnp.max(sc, axis=1, keepdims=True)
        w = jnp.where(mask, jnp.exp(sc - m), 0.0)
        tmax.append(m)
        ttot.append(jnp.sum(w, axis=1, keepdims=True))
        tval.append(jnp.dot(w.astype(BF), v, preferred_element_type=F32))
    tree_max = jnp.concatenate(tmax, axis=0)
    tree_tot = jnp.concatenate(ttot, axis=0)
    tree_val = jnp.concatenate(tval, axis=0)

    last_lane = cand_send[...]
    received(on_cand, cand_recv.at[pl.ds(1, n - 1)])
    for m in range(1, n):
        last_lane = jnp.maximum(last_lane, cand_recv[m])
    own_rows = iota((L, 128), 0)
    own_head = (kvs[last] * sp + own_rows // hp) * heads + (own_rows % hp) // prop
    own_pick = iota((L, 128), 1) == own_head
    last_own = jnp.sum(jnp.where(own_pick, last_lane, 0.0), axis=1, keepdims=True)

    received(on_stat, st_recv.at[pl.ds(1, n - 1)])
    top = st_recv[0, 0:1]
    for m in range(1, n):
        top = jnp.maximum(top, st_recv[m, 0:1])

    def col(x):
        return jnp.sum(jnp.where(diag_l, x, 0.0), axis=1, keepdims=True)

    cache_tot = jnp.zeros((1, L), F32)
    scales = []
    for m in range(n):
        sd = jnp.exp(st_recv[m, 0:1] - top)
        scales.append(col(sd))
        cache_tot = cache_tot + st_recv[m, 1:2] * sd
    shifted = col(top) + last_own
    both = jnp.maximum(shifted, tree_max)
    cscale = jnp.exp(shifted - both)
    tscale = jnp.exp(tree_max - both)
    denom = col(cache_tot) * cscale + tree_tot * tscale
    vals = val_recv[0].astype(F32) * scales[0]
    for m in range(1, n):
        val_copy(m).wait_recv()
        vals = vals + val_recv[m].astype(F32) * scales[m]
    attended = ((vals * cscale + tree_val * tscale) / denom).astype(BF)
    for j in range(sp):
        for h in range(heads):
            att[pl.ds(pl.multiple_of(kvs[last] * R + j * prop, prop), prop), h * hd : (h + 1) * hd] = (
                attended[j * hp + h * prop : j * hp + (h + 1) * prop]
            )
    for m in [1] + zmasks[::-1]:
        att_ag(m).start()

    upper = me >= half

    @pl.when(upper)
    def _():
        kv_pass(2).start()
        kv_side(1).start()

    @pl.when(jnp.logical_not(upper))
    def _():
        kv_cross().start()

    last_col = jnp.sum(jnp.where(diag, last_lane, 0.0), axis=1, keepdims=True)
    shifted_path = ptile[...]
    for b in range((span - 1).bit_length()):
        moved = pltpu.roll(shifted_path, 1 << b, 1)
        shifted_path = jnp.where((rel64 >> b) & 1 == 1, moved, shifted_path)
    off = lane - rel64
    cum_out[...] = jnp.where((off >= 0) & (off < prop), last_col + shifted_path, c64)

    in_wo.wait()
    oc = o_send.shape[2]
    near = half * R - lax.div(me, half) * (half * R)
    grows = [
        pl.ds(pl.multiple_of(first, half * R), half * R) for first in (near, half * R - near)
    ]

    def o_copy(g, d):
        return send(
            11,
            on_o + g,
            {"tp": tps[d]},
            o_send.at[tps[d], grows[g]],
            o_recv.at[d, grows[g]],
        )

    for m in zmasks:
        att_ag(m).wait_recv()
        att_ag(m + 1).start()
    for g in range(2):
        received(on_att + half - 1 + g, att.at[pl.ds(0, half // 2 * R)])
        full = jnp.dot(att[grows[g]], wov[...], preferred_element_type=F32).astype(BF)
        for t in range(nt):
            o_send[t, grows[g]] = full[:, t * oc : (t + 1) * oc]
        each_far(nt, lambda d: o_copy(g, d).start())

    @pl.when(upper)
    def _():
        kv_cross().wait_recv()
        kv_pass(6).start()
        kv_side(5).start()
        kv_pass(2).wait_recv()
        kv_side(3).start()

    mixed = o_send[mt].astype(F32)
    for g in range(2):
        received(on_o + g, o_recv.at[pl.ds(1, nt - 1), grows[g]])
    for d in range(1, nt):
        mixed = mixed + o_recv[d].astype(F32)
    ones = jnp.ones((8, oc), BF)
    sq = sum(
        lax.dot_general(ones, part, NT, preferred_element_type=F32)
        for part in thirds(mixed * mixed)
    )[0:1]
    sq_send[...] = sq

    def sq_copy(e):
        peer = {"kv": kvs[e // nt], "tp": tps[e % nt]}
        return send(12, on_sq, peer, sq_send, sq_recv.at[e])

    each_far(everyone, lambda e: sq_copy(e).start())

    order = hot(
        iota((hp, hp), 1) == iota((hp, hp), 0) % heads * prop + iota((hp, hp), 0) // heads
    ).astype(BF)

    unroll = 4

    @pl.when(upper)
    def _():
        kv_pass(6).wait_recv()
        kv_side(7).start()
        received(on_kvag + half - 1, kv_full.at[pl.ds(0, half * R)])

        def some(i, c):
            fresh = [
                heads_of(kv_full, i * unroll + j, first) for j in range(unroll) for first in (0, hw)
            ]
            placed = jnp.dot(
                order, jnp.concatenate(fresh, axis=1), preferred_element_type=F32
            ).astype(BF)
            for j in range(unroll):
                at = 2 * j * hd
                knew_out[i * unroll + j] = placed[:, at : at + hd]
                vnew_out[i * unroll + j] = placed[:, at + hd : at + 2 * hd]
            return c

        lax.fori_loop(0, num_seqs // unroll, some, 0)

    received(on_sq, sq_recv.at[pl.ds(1, everyone - 1)])
    for e in range(1, everyone):
        sq = sq + sq_recv[e]
    eighth = jnp.full((8, oc), 0.125, BF)
    ssum = sum(
        lax.dot_general(part, eighth, TN, preferred_element_type=F32)
        for part in thirds(jnp.broadcast_to(sq, (8, rows)))
    )
    in_gpost.wait()
    mixed_out[...] = (mixed * lax.rsqrt(ssum / width + epsilon) * gpost[...]).astype(BF)

    sent(0, q_y)
    sent(1, q_zr.at[pl.ds(1, half - 1)])
    sent(2, kv_y)
    sent(3, kv_zr.at[pl.ds(0, 2)])
    sent(4, kv_zr.at[2])
    sent(5, q_full.at[pl.ds(0, last * R)])
    sent(6, cand_recv.at[pl.ds(1, last)])
    sent(7, st_recv.at[pl.ds(1, last)])
    sent(8, val_recv.at[pl.ds(1, last)])
    sent(9, att.at[pl.ds(0, last * R)])

    @pl.when(upper)
    def _():
        sent(10, kv_full.at[pl.ds(0, (2 + half) * R)])

    @pl.when(jnp.logical_not(upper))
    def _():
        sent(10, kv_full.at[pl.ds(0, R)])

    sent(11, o_recv.at[pl.ds(1, nt - 1)])
    sent(12, sq_recv.at[pl.ds(1, everyone - 1)])


def patch_kernel(
    n,
    prop,
    k_in,
    v_in,
    knew,
    vnew,
    mixed,
    cum,
    starts,
    k_out,
    v_out,
    mixed_out,
    cum_out,
    k_buf,
    v_buf,
    sem,
):
    me = lax.axis_index("kv")
    num_seqs, span = k_out.shape[:2]
    out_m = pltpu.make_async_copy(mixed, mixed_out, sem.at[0])
    out_c = pltpu.make_async_copy(cum, cum_out, sem.at[1])
    out_m.start()
    out_c.start()

    def store(s):
        pltpu.make_async_copy(k_buf.at[s], k_out.at[s], sem.at[2]).start()
        pltpu.make_async_copy(v_buf.at[s], v_out.at[s], sem.at[3]).start()

    def place(s):
        at = starts[s]

        @pl.when((at >= 0) & (at <= span - prop))
        def _():
            k_buf[s, pl.ds(at, prop)] = knew[s]
            v_buf[s, pl.ds(at, prop)] = vnew[s]

        @pl.when(((at > -prop) & (at < 0)) | ((at > span - prop) & (at < span)))
        def _():
            def one(j, c):
                @pl.when((at + j >= 0) & (at + j < span))
                def _():
                    k_buf[s, pl.ds(at + j, 1)] = knew[s, pl.ds(j, 1)]
                    v_buf[s, pl.ds(at + j, 1)] = vnew[s, pl.ds(j, 1)]

                return c

            lax.fori_loop(0, prop, one, 0)

    @pl.when(me >= n // 2)
    def _():
        for s in range(num_seqs):
            place(s)
            if s > 0:
                store(s - 1)
        store(num_seqs - 1)

    @pl.when(me < n // 2)
    def _():
        for s in range(num_seqs):
            store(s)

    pltpu.make_async_copy(k_buf, k_out, sem.at[2]).wait()
    pltpu.make_async_copy(v_buf, v_out, sem.at[3]).wait()
    out_m.wait()
    out_c.wait()


def fast_device(
    n,
    nt,
    tokens,
    gain_pre,
    w_query,
    w_key,
    w_value,
    w_forget,
    b_forget,
    w_out,
    gain_post,
    key_cache,
    value_cache,
    cum_cache,
    lengths,
    accepted,
    parent,
):
    num_seqs, prop, width = tokens.shape
    span, heads, hd = key_cache.shape[1:]
    rows = num_seqs * prop
    hw = heads * hd
    cols = heads * span
    sp = num_seqs // n
    R = sp * prop
    L = sp * heads * prop
    oc = gain_post.shape[0]
    half = n // 2
    everyone = n * nt
    kc = key_cache.reshape(num_seqs, cols, hd)
    vc = value_cache.reshape(num_seqs, cols, hd)
    cum = jnp.swapaxes(cum_cache, 1, 2).reshape(num_seqs * heads, span)
    hbm = pl.BlockSpec(memory_space=pltpu.HBM)
    vmem = pl.BlockSpec(memory_space=pltpu.VMEM)
    smem = pl.BlockSpec(memory_space=pltpu.SMEM)
    V = pltpu.VMEM
    S = pltpu.SMEM
    D = pltpu.SemaphoreType.DMA
    mixed, cum_new, knew, vnew, kv, vv, starts = pl.pallas_call(
        functools.partial(layer_kernel, n, nt, num_seqs, prop, heads, hd, span),
        out_shape=(
            V((rows, oc), BF),
            V(cum.shape, F32),
            V((num_seqs, heads * prop, hd), BF),
            V((num_seqs, heads * prop, hd), BF),
            V(kc.shape, BF),
            V(vc.shape, BF),
            S(lengths.shape, jnp.int32),
        ),
        in_specs=[hbm] * 15,
        out_specs=(vmem,) * 6 + (smem,),
        scratch_shapes=[
            V((rows, width), BF),
            V((1, width), F32),
            V((3,) + w_query.shape, BF),
            V(w_forget.shape[::-1], BF),
            S(b_forget.shape, F32),
            V(w_out.shape, BF),
            V((1, oc), F32),
            V(cum.shape, F32),
            S(lengths.shape, jnp.int32),
            S(accepted.shape, jnp.int32),
            V(parent.shape, jnp.int32),
            V((rows, 128), F32),
            V((rows, 128), F32),
            V((rows, w_query.shape[0]), BF),
            V((rows, w_query.shape[0]), BF),
            V((rows, hw), BF),
            V((half, R, hw), BF),
            V((half, R, hw), BF),
            V((half, R, hw), BF),
            V((rows, hw), BF),
            V((rows, 2 * hw), BF),
            V((half, R, 2 * hw), BF),
            V((half - 1, R, 2 * hw), BF),
            V((half - 1, R, 2 * hw), BF),
            V((rows, 2 * hw), BF),
            V((n, 2, L), F32),
            V((n, L, hd), BF),
            V((n, 2, L), F32),
            V((n, L, hd), BF),
            V((1, 128), F32),
            V((n, 1, 128), F32),
            V((num_seqs, cols), F32),
            V((rows, rows), F32),
            V((num_seqs, 128), F32),
            V((num_seqs * heads, 128), F32),
            V((rows, hw), BF),
            V((nt, rows, oc), BF),
            V((nt, rows, oc), BF),
            V((1, rows), F32),
            V((everyone, 1, rows), F32),
            D((16,)),
            D((13,)),
            D((4 * half + 2 * n + 7,)),
        ],
        compiler_params=pltpu.CompilerParams(
            collective_id=0, has_side_effects=True, vmem_limit_bytes=50 * 1024 * 1024
        ),
        name="layer",
    )(
        *[
            pltpu.with_memory_space_constraint(operand, pltpu.HBM)
            for operand in (
                tokens.reshape(rows, width),
                gain_pre.reshape(1, width),
                w_query,
                w_key,
                w_value,
                w_forget.T,
                b_forget,
                w_out,
                gain_post.reshape(1, oc),
                kc,
                vc,
                cum,
                lengths,
                accepted,
                parent,
            )
        ]
    )
    fresh = (num_seqs, prop, heads, hd)
    key_out, value_out, mixed, cum_new, *unused = pl.pallas_call(
        functools.partial(patch_kernel, n, prop),
        out_shape=(
            pltpu.HBM(key_cache.shape, BF),
            pltpu.HBM(value_cache.shape, BF),
            pltpu.HBM(mixed.shape, BF),
            pltpu.HBM(cum.shape, F32),
            V(key_cache.shape, BF),
            V(key_cache.shape, BF),
        ),
        in_specs=[vmem, vmem, vmem, vmem, vmem, vmem, smem],
        out_specs=(hbm, hbm, hbm, hbm, vmem, vmem),
        input_output_aliases={0: 4, 1: 5},
        scratch_shapes=[D((4,))],
        compiler_params=pltpu.CompilerParams(
            has_side_effects=True, vmem_limit_bytes=4 * 1024 * 1024
        ),
        name="patch",
    )(
        *[
            pltpu.with_memory_space_constraint(operand, V)
            for operand in (kv.reshape(key_cache.shape), vv.reshape(key_cache.shape), knew.reshape(fresh), vnew.reshape(fresh), mixed, cum_new)
        ],
        starts,
    )
    cum_out = jnp.swapaxes(cum_new.reshape(num_seqs, heads, span), 1, 2)
    return (
        mixed.reshape(num_seqs, prop, oc),
        key_out.reshape(key_cache.shape),
        value_out.reshape(value_cache.shape),
        cum_out,
    )


def choose(mesh):
    n, nt = mesh.shape["kv"], mesh.shape["tp"]

    def body(*args):
        tokens, key_cache = args[0], args[9]
        num_seqs, prop = tokens.shape[:2]
        span, heads = key_cache.shape[1:3]
        fits = (
            num_seqs % n == 0
            and n == 8
            and nt & (nt - 1) == 0
            and num_seqs % 4 == 0
            and (num_seqs // n) * heads * prop == 128
            and span == 128
            and num_seqs * heads <= 128
            and prop % 16 == 0
        )
        if fits:
            return fast_device(n, nt, *args)
        return per_device(*args)

    return body


def solution(mesh):
    return jax.shard_map(
        choose(mesh),
        mesh=mesh,
        in_specs=(
            P(),
            P(),
            P("kv", "tp"),
            P("kv", "tp"),
            P("kv", "tp"),
            P(),
            P(),
            P("tp", "kv"),
            P(("kv", "tp")),
            P(None, "kv", "tp", None),
            P(None, "kv", "tp", None),
            P(None, "kv", "tp"),
            P(),
            P(),
            P(),
        ),
        out_specs=(
            P(None, None, ("kv", "tp")),
            P(None, "kv", "tp", None),
            P(None, "kv", "tp", None),
            P(None, "kv", "tp"),
        ),
        check_vma=False,
    )
```

```python
import functools

import jax
import jax.numpy as jnp
from jax import lax
from jax.experimental import pallas as pl
from jax.experimental.pallas import tpu as pltpu
from jax.sharding import PartitionSpec as P

epsilon = 1e-06
floor_value = -1e30


def merged(part, axis, combine):
    gathered = jax.tree.map(lambda a: lax.all_gather(a, axis), part)

    def take(source):
        return jax.tree.map(lambda a: lax.dynamic_index_in_dim(a, source, 0, False), gathered)

    return lax.fori_loop(
        1, lax.axis_size(axis), lambda source, state: combine(state, take(source)), take(0)
    )


def ancestry(parent_ids, members):
    identity = jnp.eye(members, dtype=jnp.float32)
    parent_hot = (
        parent_ids[:, :, None] == jnp.arange(members, dtype=jnp.int32)[None, None, :]
    ).astype(jnp.float32)
    ancestors = jnp.minimum(identity[None] + parent_hot, 1.0)
    for sweep in range(max(1, (members - 1).bit_length())):
        ancestors = jnp.minimum(
            jnp.einsum("bij,bjk->bik", ancestors, ancestors, precision=lax.Precision.HIGHEST), 1.0
        )
    return ancestors


def combine_parts(first, second):
    new_max = jnp.maximum(first[0], second[0])
    first_scale = jnp.exp(first[0] - new_max)
    second_scale = jnp.exp(second[0] - new_max)
    return (
        new_max,
        first[1] * first_scale + second[1] * second_scale,
        first[2] * first_scale[..., None] + second[2] * second_scale[..., None],
        jnp.maximum(first[3], second[3]),
    )


def finish_rows(cache_max, cache_total, cache_values, last_rows, tree_max, tree_total, tree_values):
    shifted = cache_max + last_rows
    top = jnp.maximum(shifted, tree_max)
    cache_scale = jnp.exp(shifted - top)
    tree_scale = jnp.exp(tree_max - top)
    attended = (
        (cache_values * cache_scale[..., None] + tree_values * tree_scale[..., None])
        / (cache_total * cache_scale + tree_total * tree_scale)[..., None]
    ).astype(jnp.bfloat16)
    return attended.reshape(attended.shape[0], attended.shape[1] * attended.shape[2])


def per_device(
    tokens,
    gain_pre,
    w_query,
    w_key,
    w_value,
    w_forget,
    b_forget,
    w_out,
    gain_post,
    key_cache,
    value_cache,
    cum_cache,
    lengths,
    accepted,
    parent,
):
    num_seqs, proposals, model_width = tokens.shape
    kv_rank = lax.axis_index("kv")
    tp_rank = lax.axis_index("tp")
    span = key_cache.shape[1]
    heads_local = key_cache.shape[2]
    head_dim = key_cache.shape[3]
    scale = head_dim ** (-0.5)
    all_rows = num_seqs * proposals
    tok_float = tokens.astype(jnp.float32)
    normed = (
        tok_float
        * lax.rsqrt(jnp.mean(tok_float * tok_float, -1, keepdims=True) + epsilon)
        * gain_pre
    ).astype(jnp.bfloat16)
    flat = normed.reshape(all_rows, model_width)
    weight_rows = w_query.shape[0]
    local_rows = lax.dynamic_slice_in_dim(flat, kv_rank * weight_rows, weight_rows, 1)
    query_part = jnp.dot(local_rows, w_query, preferred_element_type=jnp.float32)
    key_part = jnp.dot(local_rows, w_key, preferred_element_type=jnp.float32)
    value_part = jnp.dot(local_rows, w_value, preferred_element_type=jnp.float32)
    summed = (
        lax.psum(query_part.astype(jnp.bfloat16), "kv").astype(jnp.float32),
        lax.psum(key_part.astype(jnp.bfloat16), "kv").astype(jnp.float32),
        lax.psum(value_part.astype(jnp.bfloat16), "kv").astype(jnp.float32),
    )
    query_flat = summed[0].astype(jnp.bfloat16)
    key_flat = summed[1].astype(jnp.bfloat16)
    value_flat = summed[2].astype(jnp.bfloat16)
    query = query_flat.reshape(num_seqs, proposals, heads_local, head_dim)
    key_new = key_flat.reshape(num_seqs, proposals, heads_local, head_dim)
    value_new = value_flat.reshape(num_seqs, proposals, heads_local, head_dim)
    forget_cols = lax.dynamic_slice_in_dim(w_forget, tp_rank * heads_local, heads_local, 1)
    forget_bias = lax.dynamic_slice_in_dim(b_forget, tp_rank * heads_local, heads_local, 0)
    log_forget = jax.nn.log_sigmoid(
        jnp.dot(flat, forget_cols, preferred_element_type=jnp.float32) + forget_bias
    ).reshape(num_seqs, proposals, heads_local)
    ancestors = ancestry(parent, proposals)
    path = jnp.einsum("bij,bjh->bih", ancestors, log_forget, precision=lax.Precision.HIGHEST)
    valid = lengths + accepted
    positions = kv_rank * span + jnp.arange(span, dtype=jnp.int32)
    live = (positions[None, :] < valid[:, None])[:, None, None, :]
    score = (
        jnp.einsum("bihd,bkhd->bihk", query, key_cache, preferred_element_type=jnp.float32) * scale
        + path[..., None]
        - jnp.swapaxes(cum_cache, 1, 2)[:, None]
    )
    block_max = jnp.max(jnp.where(live, score, floor_value), axis=-1)
    weight = jnp.exp(jnp.where(live, score - block_max[..., None], floor_value))
    block_total = jnp.sum(weight, axis=-1)
    block_values = jnp.einsum(
        "bihk,bkhd->bihd",
        weight.astype(jnp.bfloat16),
        value_cache,
        preferred_element_type=jnp.float32,
    )
    owner = positions[None, :] == (valid - 1)[:, None]
    candidate = jnp.max(jnp.where(owner[:, :, None], cum_cache, floor_value), axis=1)
    tree_mask = (ancestors > 0.5)[:, :, None, :]
    tree_score = (
        jnp.einsum("bihd,bjhd->bihj", query, key_new, preferred_element_type=jnp.float32) * scale
        + path[..., None]
        - jnp.swapaxes(path, 1, 2)[:, None]
    )
    tree_max = jnp.max(jnp.where(tree_mask, tree_score, floor_value), axis=-1)
    tree_weight = jnp.exp(jnp.where(tree_mask, tree_score - tree_max[..., None], floor_value))
    tree_total = jnp.sum(tree_weight, axis=-1)
    tree_values = jnp.einsum(
        "bihj,bjhd->bihd",
        tree_weight.astype(jnp.bfloat16),
        value_new,
        preferred_element_type=jnp.float32,
    )
    tree_max_rows = tree_max.reshape(all_rows, heads_local)
    tree_total_rows = tree_total.reshape(all_rows, heads_local)
    tree_values_rows = tree_values.reshape(all_rows, heads_local, head_dim)
    cache_max, cache_total, cache_values, last_cum = merged(
        (block_max, block_total, block_values, candidate), "kv", combine_parts
    )
    last_rows = jnp.broadcast_to(last_cum[:, None, :], (num_seqs, proposals, heads_local)).reshape(
        all_rows, heads_local
    )
    attended = finish_rows(
        cache_max.reshape(all_rows, heads_local),
        cache_total.reshape(all_rows, heads_local),
        cache_values.reshape(all_rows, heads_local, head_dim),
        last_rows,
        tree_max_rows,
        tree_total_rows,
        tree_values_rows,
    )
    mixed_part = jnp.dot(attended, w_out, preferred_element_type=jnp.float32)
    mixed_sum = lax.psum_scatter(
        mixed_part.astype(jnp.bfloat16), "tp", scatter_dimension=1, tiled=True
    ).astype(jnp.float32)
    squares = lax.psum(jnp.sum(mixed_sum * mixed_sum, axis=1), ("kv", "tp"))
    mixed = (mixed_sum * lax.rsqrt(squares / model_width + epsilon)[:, None] * gain_post).astype(
        jnp.bfloat16
    )
    mixed = mixed.reshape(num_seqs, proposals, mixed_sum.shape[1])
    relative = positions[None, :] - valid[:, None]
    select = relative[:, :, None] == jnp.arange(proposals, dtype=jnp.int32)[None, None, :]
    written = (relative >= 0) & (relative < proposals)
    placed_keys = jnp.einsum(
        "bkj,bjhd->bkhd", select.astype(jnp.bfloat16), key_new, preferred_element_type=jnp.float32
    ).astype(jnp.bfloat16)
    placed_values = jnp.einsum(
        "bkj,bjhd->bkhd", select.astype(jnp.bfloat16), value_new, preferred_element_type=jnp.float32
    ).astype(jnp.bfloat16)
    key_out = jnp.where(written[:, :, None, None], placed_keys, key_cache)
    value_out = jnp.where(written[:, :, None, None], placed_values, value_cache)
    cum_new = last_cum[:, None, :] + path
    placed_cum = jnp.einsum(
        "bkj,bjh->bkh", select.astype(jnp.float32), cum_new, precision=lax.Precision.HIGHEST
    )
    cum_out = jnp.where(written[:, :, None], placed_cum, cum_cache)
    return (mixed, key_out, value_out, cum_out)


MESH = pl.DeviceIdType.MESH
HI = lax.Precision.HIGHEST
F32 = jnp.float32
BF = jnp.bfloat16


def iota(shape, dim):
    return lax.broadcasted_iota(jnp.int32, shape, dim)


def hot(mask):
    return jnp.where(mask, 1.0, 0.0).astype(F32)


def dot_hi(a, b, dims=(((1,), (0,)), ((), ()))):
    return lax.dot_general(a, b, dims, precision=HI, preferred_element_type=F32)


NT = (((1,), (1,)), ((), ()))
TN = (((0,), (0,)), ((), ()))


def thirds(x):
    high = x.astype(BF)
    rest = x - high.astype(F32)
    middle = rest.astype(BF)
    return high, middle, (rest - middle.astype(F32)).astype(BF)


NN = (((1,), (0,)), ((), ()))


def dot_left(x, exact, dims=NN):
    exact = exact.astype(BF)
    return sum(lax.dot_general(p, exact, dims, preferred_element_type=F32) for p in thirds(x))


def dot_right(exact, y, dims=NN):
    exact = exact.astype(BF)
    return sum(lax.dot_general(exact, p, dims, preferred_element_type=F32) for p in thirds(y))


def flips(value, count):
    bit = 1
    out = [value]
    while bit < count:
        step = bit * (1 - 2 * lax.rem(lax.div(value, bit), 2))
        out = out + [other + step for other in out]
        bit *= 2
    return out


def layer_kernel(
    n,
    nt,
    num_seqs,
    prop,
    heads,
    hd,
    span,
    tok_h,
    gain_h,
    wq_h,
    wk_h,
    wv_h,
    wft_h,
    bias_h,
    wo_h,
    gpost_h,
    kc_h,
    vc_h,
    cum_h,
    lens_h,
    accs_h,
    parent_h,
    mixed_out,
    cum_out,
    knew_out,
    vnew_out,
    kcv,
    vcv,
    at_out,
    tokv,
    gain,
    wqkv,
    wft,
    bias,
    wov,
    gpost,
    cum,
    lens,
    accs,
    parent,
    ssq,
    invv,
    xraw,
    xloc,
    part_q,
    q_y,
    q_zs,
    q_zr,
    q_full,
    part_kv,
    kv_y,
    kv_zs,
    kv_zr,
    kv_full,
    st_send,
    val_send,
    st_recv,
    val_recv,
    cand_send,
    cand_recv,
    brow,
    anc,
    tpath,
    ptile,
    att,
    o_send,
    o_recv,
    sq_send,
    sq_recv,
    loc,
    ssem,
    rsem,
):
    me = lax.axis_index("kv")
    mt = lax.axis_index("tp")
    rows, width = tokv.shape
    hw = heads * hd
    kdim = wq_h.shape[0]
    cols = heads * span
    sp = num_seqs // n
    R = sp * prop
    hp = heads * prop
    L = sp * hp
    scale = hd ** (-0.5)
    base = me * span
    heads_all = wft.shape[0]
    half = n // 2
    everyone = n * nt

    barrier = pltpu.get_barrier_semaphore()

    kvs = flips(me, n)
    tps = flips(mt, nt)

    mine = pl.ds(pl.multiple_of(me * kdim, kdim), kdim)
    loads = [
        (tok_h.at[:, mine], xraw),
        (wq_h, wqkv.at[0]),
        (gain_h, gain),
        (wk_h, wqkv.at[1]),
        (wv_h, wqkv.at[2]),
        (tok_h, tokv),
        (lens_h, lens),
        (accs_h, accs),
        (cum_h, cum),
        (parent_h, parent),
        (wft_h, wft),
        (bias_h, bias),
        (gpost_h, gpost),
        (kc_h, kcv),
        (vc_h, vcv),
        (wo_h, wov),
    ]
    copies = [pltpu.make_async_copy(src, dst, loc.at[i]) for i, (src, dst) in enumerate(loads)]
    (
        in_x,
        in_wq,
        in_gain,
        in_wk,
        in_wv,
        in_tok,
        in_lens,
        in_accs,
        in_cum,
        in_parent,
        in_wft,
        in_bias,
        in_gpost,
        in_kc,
        in_vc,
        in_wo,
    ) = copies
    urgent = 5
    for c in copies[:urgent]:
        c.start()
    for e in range(1, everyone):
        pl.semaphore_signal(
            barrier,
            inc=1,
            device_id={"kv": kvs[e // nt], "tp": tps[e % nt]},
            device_id_type=MESH,
        )

    def send(kind, slot, device, src, dst):
        return pltpu.make_async_remote_copy(
            src_ref=src,
            dst_ref=dst,
            send_sem=ssem.at[kind],
            recv_sem=rsem.at[slot],
            device_id=device,
            device_id_type=MESH,
        )

    def to_kv(kind, slot, mask, src, dst):
        return send(kind, slot, {"kv": kvs[mask]}, src, dst)

    def rrow(i):
        return pl.ds(pl.multiple_of(i * R, R), R)

    def spread_to(kind, slot, mask, ref, rank):
        return to_kv(kind, slot, mask, ref.at[rrow(rank)], ref.at[rrow(rank)])

    def sent(kind, ref):
        to_kv(kind, 0, 1, ref, ref).wait_send()

    def received(slot, ref):
        to_kv(0, slot, 1, ref, ref).wait_recv()

    flat = [0]

    def slots(count):
        flat[0] += count
        return flat[0] - count

    on_qy, on_qz, on_ky, on_kz = slots(half), slots(1), slots(half), slots(2)
    on_qag, on_cand, on_stat, on_val = slots(n - 1), slots(1), slots(1), slots(n - 1)
    on_att, on_kvag, on_o, on_sq = slots(half + 1), slots(half), slots(2), slots(1)
    last = n - 1

    def q_yrs(m):
        return to_kv(0, on_qy + m // 2, 1, part_q.at[rrow(kvs[m + 1])], q_y.at[m // 2])

    def q_zrs(m):
        return to_kv(1, on_qz, m, q_zs.at[m // 2], q_zr.at[m // 2])

    def kv_yrs(m):
        src = part_kv.at[rrow(kvs[(m + 1) ^ last])]
        return to_kv(2, on_ky + m // 2, 1, src, kv_y.at[m // 2])

    def kv_near():
        return to_kv(3, on_kz, 2, kv_zs.at[pl.ds(0, 2)], kv_zr.at[pl.ds(0, 2)])

    def kv_far():
        return to_kv(4, on_kz + 1, half, kv_zs.at[2], kv_zr.at[2])

    def q_ag(m):
        if m % 2:
            return spread_to(5, on_qag + m - 1, 1, q_full, kvs[m - 1])
        return spread_to(5, on_qag + m - 1, m, q_full, me)

    def cand_copy(m):
        return to_kv(6, on_cand, m, cand_send, cand_recv.at[m])

    def stat_copy(m):
        return to_kv(7, on_stat, m, st_send.at[m], st_recv.at[m])

    def val_copy(m):
        return to_kv(8, on_val + m - 1, m, val_send.at[m], val_recv.at[m])

    def att_ag(m):
        if m % 2:
            return spread_to(9, on_att + half - 1 + m // half, 1, att, kvs[(m - 1) ^ last])
        return spread_to(9, on_att + m // 2 - 1, m, att, kvs[last])

    def kv_cross():
        return spread_to(10, on_kvag, half, kv_full, kvs[last])

    def kv_pass(m):
        return spread_to(10, on_kvag + 1 + m // half, half // 2, kv_full, kvs[(m - half // 2) ^ last])

    def kv_side(m):
        return spread_to(10, on_kvag + half - 1, 1, kv_full, kvs[(m - 1) ^ last])

    def each(count, fn):
        for d in range(1, count):
            fn(d)

    def each_far(count, fn):
        for d in range(count - 1, 0, -1):
            fn(d)

    def scaled(total, rank):
        inv = invv[rrow(rank)]
        return jnp.concatenate(
            [
                total[:, j * lanes : (j + 1) * lanes] * inv
                for j in range(total.shape[1] // lanes)
            ],
            axis=1,
        )

    zmasks = list(range(2, n, 2))
    nb = prop
    lanes = 128

    def sum_rows(i, c):
        sl = pl.ds(pl.multiple_of(i * nb, nb), nb)
        accs4 = [None] * 4
        for j in range(width // lanes):
            t = tokv[sl, j * lanes : (j + 1) * lanes].astype(F32)
            p = t * t
            accs4[j % 4] = p if accs4[j % 4] is None else accs4[j % 4] + p
        ssq[sl, :] = (accs4[0] + accs4[1]) + (accs4[2] + accs4[3])
        return c

    in_x.wait()
    in_gain.wait()
    xloc[...] = (xraw[...].astype(F32) * gain[:, mine]).astype(BF)
    in_wq.wait()
    part_q[...] = jnp.dot(xloc[...], wqkv[0], preferred_element_type=F32).astype(BF)
    pl.semaphore_wait(barrier, everyone - 1)
    for m in zmasks[::-1] + [0]:
        q_yrs(m).start()
    for c in copies[urgent:]:
        c.start()
    in_wk.wait()
    in_wv.wait()
    part_kv[:, 0:hw] = jnp.dot(xloc[...], wqkv[1], preferred_element_type=F32).astype(BF)
    part_kv[:, hw : 2 * hw] = jnp.dot(xloc[...], wqkv[2], preferred_element_type=F32).astype(BF)
    def kv_sum(m):
        return part_kv[rrow(kvs[m ^ last])].astype(F32) + kv_y[m // 2].astype(F32)
    for m in zmasks[::-1] + [0]:
        kv_yrs(m).start()
    in_lens.wait()
    in_accs.wait()
    in_cum.wait()
    r64 = num_seqs * heads
    c64 = cum[...]
    srow = iota((r64, span), 0) // heads
    lane = iota((r64, span), 1)
    rel64 = jnp.zeros((r64, span), jnp.int32)
    rel16 = jnp.zeros((num_seqs, cols), jnp.int32)
    s16 = iota((num_seqs, cols), 0)
    for s in range(num_seqs):
        rel_s = lens[s] + accs[s] - base
        at_out[s] = rel_s
        rel64 = jnp.where(srow == s, rel_s, rel64)
        rel16 = jnp.where(s16 == s, rel_s, rel16)
    cand = jnp.max(jnp.where(lane == rel64 - 1, c64, floor_value), axis=1, keepdims=True)
    diag = iota((r64, 128), 0) == iota((r64, 128), 1)
    cand_send[...] = jnp.sum(jnp.where(diag, cand, 0.0), axis=0, keepdims=True)
    each_far(n, lambda m: cand_copy(m).start())

    spread = hot(iota((span, cols), 1) // heads == iota((span, cols), 0))
    e1 = dot_hi(c64, spread)
    e1 = jnp.where(iota((r64, cols), 0) % heads == iota((r64, cols), 1) % heads, e1, 0.0)
    take = hot(iota((num_seqs, r64), 1) // heads == iota((num_seqs, r64), 0))
    cflat = dot_hi(take, e1)
    brow[...] = jnp.where(iota((num_seqs, cols), 1) // heads < rel16, -cflat, floor_value)
    for m in zmasks[::-1]:
        q_yrs(m).wait_recv()
        q_zs[m // 2] = (part_q[rrow(kvs[m])].astype(F32) + q_y[m // 2].astype(F32)).astype(BF)
        q_zrs(m).start()
    in_tok.wait()
    lax.fori_loop(0, rows // nb, sum_rows, 0)
    total = dot_left(ssq[...], jnp.ones((lanes, lanes), F32))
    invv[...] = lax.rsqrt(total / width + epsilon)
    in_parent.wait()
    ri = iota((rows, rows), 0)
    ci = iota((rows, rows), 1)
    pick = hot(iota((rows, num_seqs), 0) // prop == iota((rows, num_seqs), 1))
    pb = dot_hi(pick, parent[...].astype(F32))
    pcol = jnp.sum(
        jnp.where(iota((rows, prop), 1) == iota((rows, prop), 0) % prop, pb, 0.0),
        axis=1,
        keepdims=True,
    )
    target = jnp.where(pcol >= 0.0, (ri // prop * prop).astype(F32) + pcol, -1.0)
    a = jnp.where((ri == ci) | (ci.astype(F32) == target), 1.0, 0.0)
    for sweep in range(max(1, (prop - 1).bit_length())):
        low = a.astype(BF)
        a = jnp.minimum(jnp.dot(low, low, preferred_element_type=F32), 1.0)
    anc[...] = a
    q_yrs(0).wait_recv()
    own = part_q[rrow(me)].astype(F32) + q_y[0].astype(F32)
    received(on_qz, q_zr.at[pl.ds(1, half - 1)])
    for m in zmasks:
        own = own + q_zr[m // 2].astype(F32)
    q_full[rrow(me)] = scaled(own, me).astype(BF)
    for m in [1] + zmasks[::-1]:
        q_ag(m).start()
    same_head = iota((hp, cols), 0) // prop == iota((hp, cols), 1) % heads
    diag_l = iota((L, L), 0) == iota((L, L), 1)

    def heads_of(ref, s, first):
        block = ref[pl.ds(pl.multiple_of(s * prop, prop), prop), first : first + hw]
        return jnp.concatenate([block[:, h * hd : (h + 1) * hd] for h in range(heads)], axis=0)

    def block_part(src):
        maxes, totals, values = [], [], []
        for j in range(sp):
            s = src * sp + j
            q = heads_of(q_full, s, 0)
            sc = lax.dot_general(q, kcv[s], NT, preferred_element_type=F32) * scale
            sc = jnp.where(same_head, sc + brow[pl.ds(s, 1), :], floor_value)
            m = jnp.max(sc, axis=1, keepdims=True)
            w = jnp.exp(sc - m)
            maxes.append(m)
            totals.append(jnp.sum(w, axis=1, keepdims=True))
            values.append(
                jnp.dot(w.astype(BF), vcv[s], preferred_element_type=F32).astype(BF)
            )
        m = jnp.concatenate(maxes, axis=0)
        t = jnp.concatenate(totals, axis=0)
        m_lane = jnp.sum(jnp.where(diag_l, m, 0.0), axis=0, keepdims=True)
        t_lane = jnp.sum(jnp.where(diag_l, t, 0.0), axis=0, keepdims=True)
        stats = jnp.where(iota((2, L), 0) == 0, m_lane, t_lane)
        return stats, jnp.concatenate(values, axis=0)

    def blocks(masks):
        parts = [block_part(kvs[m]) for m in masks]
        for m, (stats, values) in zip(masks, parts):
            if m == last:
                st_recv[0] = stats
                val_recv[0] = values
            else:
                st_send[last - m] = stats
                val_send[last - m] = values
        for m in masks:
            if m != last:
                stat_copy(last - m).start()
                val_copy(last - m).start()
    def take_q(m):
        q_ag(m).wait_recv()
        if m % 2 == 0:
            q_ag(m + 1).start()
    in_kc.wait()
    in_vc.wait()
    blocks([0])
    for i, m in enumerate((2, 6)):
        kv_yrs(m).wait_recv()
        kv_zs[i] = kv_sum(m).astype(BF)
    kv_near().start()
    in_wft.wait()
    in_bias.wait()
    wscaled = wft[...].astype(F32) * gain[...]
    whigh = wscaled.astype(BF)
    wlow = (wscaled - whigh.astype(F32)).astype(BF)
    lf = lax.dot_general(
        jnp.concatenate([whigh, wlow], axis=0), tokv[...], NT, preferred_element_type=F32
    )
    lf = lf[0:heads_all] + lf[heads_all : 2 * heads_all]
    inv_lane = dot_right(jnp.full((8, lanes), 1.0 / lanes, F32), invv[...], NT)[0:1]
    bcol = jnp.zeros((heads_all, rows), F32)
    for h in range(heads_all):
        bcol = jnp.where(iota((heads_all, rows), 0) == h, bias[h], bcol)
    z = lf * inv_lane + bcol
    lf = jnp.minimum(z, 0.0) - jnp.log1p(jnp.exp(-jnp.abs(z)))
    path_t = dot_left(lf, a, NT)
    rep = hot(iota((r64, heads_all), 1) == mt * heads + iota((r64, heads_all), 0) % heads)
    pm = dot_right(rep, path_t)
    pm = jnp.where(iota((r64, rows), 1) // prop == iota((r64, rows), 0) // heads, pm, 0.0)
    fold = hot(iota((rows, 128), 0) % prop == iota((rows, 128), 1) % prop)
    pt = dot_left(pm, fold)
    ptile[...] = pt
    ptm = jnp.where((iota((r64, 128), 1) // prop) % heads == iota((r64, 128), 0) % heads, pt, 0.0)
    tpath[...] = dot_right(take, ptm)
    take_q(2)
    take_q(1)
    blocks([1, 2])
    take_q(4)
    take_q(6)
    blocks([4, 6])
    kv_yrs(4).wait_recv()
    kv_near().wait_recv()
    kv_zs[2] = (kv_sum(4) + kv_zr[1].astype(F32)).astype(BF)
    kv_far().start()
    take_q(3)
    take_q(5)
    blocks([3, 5])
    take_q(7)
    blocks([7])


    kv_yrs(0).wait_recv()
    kv_far().wait_recv()
    own = kv_sum(0) + kv_zr[0].astype(F32) + kv_zr[2].astype(F32)
    kv_full[rrow(kvs[last])] = scaled(own, kvs[last]).astype(BF)

    fold_h = iota((rows, hp), 0)
    tmax, ttot, tval = [], [], []
    for j in range(sp):
        s = kvs[last] * sp + j
        q = heads_of(q_full, s, 0)
        k = heads_of(kv_full, s, 0)
        v = heads_of(kv_full, s, hw)
        arows = anc[pl.ds(pl.multiple_of(s * prop, prop), prop), :]
        sel = hot(fold_h == s * prop + iota((rows, hp), 1) % prop).astype(BF)
        am = jnp.dot(arows.astype(BF), sel, preferred_element_type=F32)
        am = jnp.concatenate([am] * heads, axis=0)
        mask = (am > 0.5) & (iota((hp, hp), 0) // prop == iota((hp, hp), 1) // prop)
        sc = lax.dot_general(q, k, NT, preferred_element_type=F32) * scale
        sc = jnp.where(mask, sc - tpath[pl.ds(s, 1), 0:hp], floor_value)
        m = jnp.max(sc, axis=1, keepdims=True)
        w = jnp.where(mask, jnp.exp(sc - m), 0.0)
        tmax.append(m)
        ttot.append(jnp.sum(w, axis=1, keepdims=True))
        tval.append(jnp.dot(w.astype(BF), v, preferred_element_type=F32))
    tree_max = jnp.concatenate(tmax, axis=0)
    tree_tot = jnp.concatenate(ttot, axis=0)
    tree_val = jnp.concatenate(tval, axis=0)

    last_lane = cand_send[...]
    received(on_cand, cand_recv.at[pl.ds(1, n - 1)])
    for m in range(1, n):
        last_lane = jnp.maximum(last_lane, cand_recv[m])
    own_rows = iota((L, 128), 0)
    own_head = (kvs[last] * sp + own_rows // hp) * heads + (own_rows % hp) // prop
    own_pick = iota((L, 128), 1) == own_head
    last_own = jnp.sum(jnp.where(own_pick, last_lane, 0.0), axis=1, keepdims=True)

    received(on_stat, st_recv.at[pl.ds(1, n - 1)])
    top = st_recv[0, 0:1]
    for m in range(1, n):
        top = jnp.maximum(top, st_recv[m, 0:1])

    def col(x):
        return jnp.sum(jnp.where(diag_l, x, 0.0), axis=1, keepdims=True)

    cache_tot = jnp.zeros((1, L), F32)
    scales = []
    for m in range(n):
        sd = jnp.exp(st_recv[m, 0:1] - top)
        scales.append(col(sd))
        cache_tot = cache_tot + st_recv[m, 1:2] * sd
    shifted = col(top) + last_own
    both = jnp.maximum(shifted, tree_max)
    cscale = jnp.exp(shifted - both)
    tscale = jnp.exp(tree_max - both)
    denom = col(cache_tot) * cscale + tree_tot * tscale
    vals = val_recv[0].astype(F32) * scales[0]
    for m in range(1, n):
        val_copy(m).wait_recv()
        vals = vals + val_recv[m].astype(F32) * scales[m]
    attended = ((vals * cscale + tree_val * tscale) / denom).astype(BF)
    for j in range(sp):
        for h in range(heads):
            att[pl.ds(pl.multiple_of(kvs[last] * R + j * prop, prop), prop), h * hd : (h + 1) * hd] = (
                attended[j * hp + h * prop : j * hp + (h + 1) * prop]
            )
    for m in [1] + zmasks[::-1]:
        att_ag(m).start()

    upper = me >= half

    @pl.when(upper)
    def _():
        kv_pass(2).start()
        kv_side(1).start()

    @pl.when(jnp.logical_not(upper))
    def _():
        kv_cross().start()

    last_col = jnp.sum(jnp.where(diag, last_lane, 0.0), axis=1, keepdims=True)
    shifted_path = ptile[...]
    for b in range((span - 1).bit_length()):
        moved = pltpu.roll(shifted_path, 1 << b, 1)
        shifted_path = jnp.where((rel64 >> b) & 1 == 1, moved, shifted_path)
    off = lane - rel64
    cum_out[...] = jnp.where((off >= 0) & (off < prop), last_col + shifted_path, c64)

    in_wo.wait()
    oc = o_send.shape[2]
    near = half * R - lax.div(me, half) * (half * R)
    grows = [
        pl.ds(pl.multiple_of(first, half * R), half * R) for first in (near, half * R - near)
    ]

    def o_copy(g, d):
        return send(
            11,
            on_o + g,
            {"tp": tps[d]},
            o_send.at[tps[d], grows[g]],
            o_recv.at[d, grows[g]],
        )

    for m in zmasks:
        att_ag(m).wait_recv()
        att_ag(m + 1).start()
    for g in range(2):
        received(on_att + half - 1 + g, att.at[pl.ds(0, half // 2 * R)])
        full = jnp.dot(att[grows[g]], wov[...], preferred_element_type=F32).astype(BF)
        for t in range(nt):
            o_send[t, grows[g]] = full[:, t * oc : (t + 1) * oc]
        each_far(nt, lambda d: o_copy(g, d).start())

    @pl.when(upper)
    def _():
        kv_cross().wait_recv()
        kv_pass(6).start()
        kv_side(5).start()
        kv_pass(2).wait_recv()
        kv_side(3).start()

    mixed = o_send[mt].astype(F32)
    for g in range(2):
        received(on_o + g, o_recv.at[pl.ds(1, nt - 1), grows[g]])
    for d in range(1, nt):
        mixed = mixed + o_recv[d].astype(F32)
    ones = jnp.ones((8, oc), BF)
    sq = sum(
        lax.dot_general(ones, part, NT, preferred_element_type=F32)
        for part in thirds(mixed * mixed)
    )[0:1]
    sq_send[...] = sq

    def sq_copy(e):
        peer = {"kv": kvs[e // nt], "tp": tps[e % nt]}
        return send(12, on_sq, peer, sq_send, sq_recv.at[e])

    each_far(everyone, lambda e: sq_copy(e).start())

    order = hot(
        iota((hp, hp), 1) == iota((hp, hp), 0) % heads * prop + iota((hp, hp), 0) // heads
    ).astype(BF)

    unroll = 4

    @pl.when(upper)
    def _():
        kv_pass(6).wait_recv()
        kv_side(7).start()
        received(on_kvag + half - 1, kv_full.at[pl.ds(0, half * R)])

        def some(i, c):
            fresh = [
                heads_of(kv_full, i * unroll + j, first) for j in range(unroll) for first in (0, hw)
            ]
            placed = jnp.dot(
                order, jnp.concatenate(fresh, axis=1), preferred_element_type=F32
            ).astype(BF)
            for j in range(unroll):
                at = 2 * j * hd
                knew_out[i * unroll + j] = placed[:, at : at + hd]
                vnew_out[i * unroll + j] = placed[:, at + hd : at + 2 * hd]
            return c

        lax.fori_loop(0, num_seqs // unroll, some, 0)

    received(on_sq, sq_recv.at[pl.ds(1, everyone - 1)])
    for e in range(1, everyone):
        sq = sq + sq_recv[e]
    eighth = jnp.full((8, oc), 0.125, BF)
    ssum = sum(
        lax.dot_general(part, eighth, TN, preferred_element_type=F32)
        for part in thirds(jnp.broadcast_to(sq, (8, rows)))
    )
    in_gpost.wait()
    mixed_out[...] = (mixed * lax.rsqrt(ssum / width + epsilon) * gpost[...]).astype(BF)

    sent(0, q_y)
    sent(1, q_zr.at[pl.ds(1, half - 1)])
    sent(2, kv_y)
    sent(3, kv_zr.at[pl.ds(0, 2)])
    sent(4, kv_zr.at[2])
    sent(5, q_full.at[pl.ds(0, last * R)])
    sent(6, cand_recv.at[pl.ds(1, last)])
    sent(7, st_recv.at[pl.ds(1, last)])
    sent(8, val_recv.at[pl.ds(1, last)])
    sent(9, att.at[pl.ds(0, last * R)])

    @pl.when(upper)
    def _():
        sent(10, kv_full.at[pl.ds(0, (2 + half) * R)])

    @pl.when(jnp.logical_not(upper))
    def _():
        sent(10, kv_full.at[pl.ds(0, R)])

    sent(11, o_recv.at[pl.ds(1, nt - 1)])
    sent(12, sq_recv.at[pl.ds(1, everyone - 1)])


def patch_kernel(
    n,
    prop,
    k_in,
    v_in,
    knew,
    vnew,
    mixed,
    cum,
    starts,
    k_out,
    v_out,
    mixed_out,
    cum_out,
    k_buf,
    v_buf,
    sem,
):
    me = lax.axis_index("kv")
    num_seqs, span = k_out.shape[:2]
    out_m = pltpu.make_async_copy(mixed, mixed_out, sem.at[0])
    out_c = pltpu.make_async_copy(cum, cum_out, sem.at[1])
    out_m.start()
    out_c.start()

    def store(s):
        pltpu.make_async_copy(k_buf.at[s], k_out.at[s], sem.at[2]).start()
        pltpu.make_async_copy(v_buf.at[s], v_out.at[s], sem.at[3]).start()

    def place(s):
        at = starts[s]

        @pl.when((at >= 0) & (at <= span - prop))
        def _():
            k_buf[s, pl.ds(at, prop)] = knew[s]
            v_buf[s, pl.ds(at, prop)] = vnew[s]

        @pl.when(((at > -prop) & (at < 0)) | ((at > span - prop) & (at < span)))
        def _():
            def one(j, c):
                @pl.when((at + j >= 0) & (at + j < span))
                def _():
                    k_buf[s, pl.ds(at + j, 1)] = knew[s, pl.ds(j, 1)]
                    v_buf[s, pl.ds(at + j, 1)] = vnew[s, pl.ds(j, 1)]

                return c

            lax.fori_loop(0, prop, one, 0)

    @pl.when(me >= n // 2)
    def _():
        for s in range(num_seqs):
            place(s)
            if s > 0:
                store(s - 1)
        store(num_seqs - 1)

    @pl.when(me < n // 2)
    def _():
        for s in range(num_seqs):
            store(s)

    pltpu.make_async_copy(k_buf, k_out, sem.at[2]).wait()
    pltpu.make_async_copy(v_buf, v_out, sem.at[3]).wait()
    out_m.wait()
    out_c.wait()


def fast_device(
    n,
    nt,
    tokens,
    gain_pre,
    w_query,
    w_key,
    w_value,
    w_forget,
    b_forget,
    w_out,
    gain_post,
    key_cache,
    value_cache,
    cum_cache,
    lengths,
    accepted,
    parent,
):
    num_seqs, prop, width = tokens.shape
    span, heads, hd = key_cache.shape[1:]
    rows = num_seqs * prop
    hw = heads * hd
    cols = heads * span
    sp = num_seqs // n
    R = sp * prop
    L = sp * heads * prop
    oc = gain_post.shape[0]
    half = n // 2
    everyone = n * nt
    kc = key_cache.reshape(num_seqs, cols, hd)
    vc = value_cache.reshape(num_seqs, cols, hd)
    cum = jnp.swapaxes(cum_cache, 1, 2).reshape(num_seqs * heads, span)
    hbm = pl.BlockSpec(memory_space=pltpu.HBM)
    vmem = pl.BlockSpec(memory_space=pltpu.VMEM)
    smem = pl.BlockSpec(memory_space=pltpu.SMEM)
    V = pltpu.VMEM
    S = pltpu.SMEM
    D = pltpu.SemaphoreType.DMA
    mixed, cum_new, knew, vnew, kv, vv, starts = pl.pallas_call(
        functools.partial(layer_kernel, n, nt, num_seqs, prop, heads, hd, span),
        out_shape=(
            V((rows, oc), BF),
            V(cum.shape, F32),
            V((num_seqs, heads * prop, hd), BF),
            V((num_seqs, heads * prop, hd), BF),
            V(kc.shape, BF),
            V(vc.shape, BF),
            S(lengths.shape, jnp.int32),
        ),
        in_specs=[hbm] * 15,
        out_specs=(vmem,) * 6 + (smem,),
        scratch_shapes=[
            V((rows, width), BF),
            V((1, width), F32),
            V((3,) + w_query.shape, BF),
            V(w_forget.shape[::-1], BF),
            S(b_forget.shape, F32),
            V(w_out.shape, BF),
            V((1, oc), F32),
            V(cum.shape, F32),
            S(lengths.shape, jnp.int32),
            S(accepted.shape, jnp.int32),
            V(parent.shape, jnp.int32),
            V((rows, 128), F32),
            V((rows, 128), F32),
            V((rows, w_query.shape[0]), BF),
            V((rows, w_query.shape[0]), BF),
            V((rows, hw), BF),
            V((half, R, hw), BF),
            V((half, R, hw), BF),
            V((half, R, hw), BF),
            V((rows, hw), BF),
            V((rows, 2 * hw), BF),
            V((half, R, 2 * hw), BF),
            V((half - 1, R, 2 * hw), BF),
            V((half - 1, R, 2 * hw), BF),
            V((rows, 2 * hw), BF),
            V((n, 2, L), F32),
            V((n, L, hd), BF),
            V((n, 2, L), F32),
            V((n, L, hd), BF),
            V((1, 128), F32),
            V((n, 1, 128), F32),
            V((num_seqs, cols), F32),
            V((rows, rows), F32),
            V((num_seqs, 128), F32),
            V((num_seqs * heads, 128), F32),
            V((rows, hw), BF),
            V((nt, rows, oc), BF),
            V((nt, rows, oc), BF),
            V((1, rows), F32),
            V((everyone, 1, rows), F32),
            D((16,)),
            D((13,)),
            D((4 * half + 2 * n + 7,)),
        ],
        compiler_params=pltpu.CompilerParams(
            collective_id=0, has_side_effects=True, vmem_limit_bytes=50 * 1024 * 1024
        ),
        name="layer",
    )(
        *[
            pltpu.with_memory_space_constraint(operand, pltpu.HBM)
            for operand in (
                tokens.reshape(rows, width),
                gain_pre.reshape(1, width),
                w_query,
                w_key,
                w_value,
                w_forget.T,
                b_forget,
                w_out,
                gain_post.reshape(1, oc),
                kc,
                vc,
                cum,
                lengths,
                accepted,
                parent,
            )
        ]
    )
    fresh = (num_seqs, prop, heads, hd)
    key_out, value_out, mixed, cum_new, *unused = pl.pallas_call(
        functools.partial(patch_kernel, n, prop),
        out_shape=(
            pltpu.HBM(key_cache.shape, BF),
            pltpu.HBM(value_cache.shape, BF),
            pltpu.HBM(mixed.shape, BF),
            pltpu.HBM(cum.shape, F32),
            V(key_cache.shape, BF),
            V(key_cache.shape, BF),
        ),
        in_specs=[vmem, vmem, vmem, vmem, vmem, vmem, smem],
        out_specs=(hbm, hbm, hbm, hbm, vmem, vmem),
        input_output_aliases={0: 4, 1: 5},
        scratch_shapes=[D((4,))],
        compiler_params=pltpu.CompilerParams(
            has_side_effects=True, vmem_limit_bytes=4 * 1024 * 1024
        ),
        name="patch",
    )(
        *[
            pltpu.with_memory_space_constraint(operand, V)
            for operand in (kv.reshape(key_cache.shape), vv.reshape(key_cache.shape), knew.reshape(fresh), vnew.reshape(fresh), mixed, cum_new)
        ],
        starts,
    )
    cum_out = jnp.swapaxes(cum_new.reshape(num_seqs, heads, span), 1, 2)
    return (
        mixed.reshape(num_seqs, prop, oc),
        key_out.reshape(key_cache.shape),
        value_out.reshape(value_cache.shape),
        cum_out,
    )


def choose(mesh):
    n, nt = mesh.shape["kv"], mesh.shape["tp"]

    def body(*args):
        tokens, key_cache = args[0], args[9]
        num_seqs, prop = tokens.shape[:2]
        span, heads = key_cache.shape[1:3]
        fits = (
            num_seqs % n == 0
            and n == 8
            and nt & (nt - 1) == 0
            and num_seqs % 4 == 0
            and (num_seqs // n) * heads * prop == 128
            and span == 128
            and num_seqs * heads <= 128
            and prop % 16 == 0
        )
        if fits:
            return fast_device(n, nt, *args)
        return per_device(*args)

    return body


def solution(mesh):
    return jax.shard_map(
        choose(mesh),
        mesh=mesh,
        in_specs=(
            P(),
            P(),
            P("kv", "tp"),
            P("kv", "tp"),
            P("kv", "tp"),
            P(),
            P(),
            P("tp", "kv"),
            P(("kv", "tp")),
            P(None, "kv", "tp", None),
            P(None, "kv", "tp", None),
            P(None, "kv", "tp"),
            P(),
            P(),
            P(),
        ),
        out_specs=(
            P(None, None, ("kv", "tp")),
            P(None, "kv", "tp", None),
            P(None, "kv", "tp", None),
            P(None, "kv", "tp"),
        ),
        check_vma=False,
    )
```
